1024 devices in a mesh: sp: 256 (over z, x, core), tp: 4 (over y).
Axes of the slice: x: 4, y: 4, z: 32, core: 2. Of those that a mesh axis runs over, the one named last changes fastest.
Arguments:
- proj_value: bfloat16 [98304, 1024], P('sp', 'tp'), may hold values from -6 to 6
- proj_gate: bfloat16 [98304, 1024], P('sp', 'tp'), may hold values from -8 to 8
- out_cotangent: bfloat16 [98304, 2048], P('sp'), may hold values from -24 to 24
- out_weight: bfloat16 [1024, 2048], P('tp'), may hold values from -0.1875 to 0.1875
- conv_taps: bfloat16 [31, 1024], P(None, 'tp'), may hold values from -1 to 1
- norm_gain: float32 [1024], P('tp'), may hold values from 0.1 to 1.9
- row_mean: float32 [98304], P('sp'), may hold values from -2 to 2
- row_scale: float32 [98304], P('sp'), may hold values from 0.7 to 3
Outputs:
- value_grad: bfloat16 [98304, 1024], P('sp', 'tp')
- gate_grad: bfloat16 [98304, 1024], P('sp', 'tp')
- out_weight_grad: float32 [2048, 1024], P('sp', 'tp')
- taps_grad: float32 [31, 1024], P(None, 'tp')
- gain_grad: float32 [1024], P('tp')
The draws below stay inside these ranges and needn't reach their ends.
All inputs are finite; a program needn't handle non-finite values.
Results may differ from the reference program's by a relative error of at most 0.0047.
Values may be sent and summed in bfloat16 or wider, within the bound.
No kernel may reach another device: no remote copies, remote signals or barrier semaphores. Data moves between devices by JAX's collectives and lax.ppermute only.
A program may use at most 32 MiB of HBM per device.

```python
import math
import jax
import jax.numpy as jnp

D = 2048
CH = 1024
CONV_K = 31
TOKENS = 98304


def with_spikes(values, key, source, target, shards_of, factor):
    owner, partner = [(jnp.arange(values.shape[dim]) // (values.shape[dim] // shards_of)).reshape([-1 if axis == dim else 1 for axis in range(values.ndim)]) for dim in (source, target)]
    chosen = jax.random.permutation(key, shards_of)[partner]
    strong = (owner == chosen) | (owner == (partner + shards_of // 2) % shards_of)
    return jnp.where(strong, factor * values, values)


def level_of(rng, shape, pieces, least, top_value):
    def one(position, blocks):
        steps = jax.random.uniform(jax.random.fold_in(jax.random.fold_in(rng, 6), position), (blocks,), jnp.float32, least / len(pieces), top_value / len(pieces))
        return jnp.repeat(jnp.exp(steps), shape[position] // blocks).reshape((-1,) + (1,) * (len(shape) - position - 1))

    factor_of = one(*pieces[0])
    for cut in pieces[1:]:
        factor_of = factor_of * one(*cut)
    return factor_of


def noise(own_key, shape, scale, most, split=(), held_as=jnp.bfloat16):
    factor_of = level_of(own_key, shape, split, -0.22, 0.18) if split else 1.0
    result = jax.random.normal(own_key, shape, jnp.float32) * scale * factor_of
    return jnp.minimum(jnp.maximum(result, -most), most).astype(held_as)


def bell_draw_with(stream_key, extent, width, reach, shards, heavy, held_as=jnp.bfloat16):
    result = width * jax.random.normal(stream_key, extent, jnp.float32)
    if shards:
        result = result * level_of(stream_key, extent, shards, -0.22, 0.18)
    return jnp.clip(with_spikes(result, jax.random.fold_in(stream_key, 3), *heavy), -reach, reach).astype(held_as)


def setup_inputs(seed: int = 0) -> dict:
    key_list = jax.random.split(jax.random.key(seed), 9)
    proj_value = noise(key_list[0], (TOKENS, CH), 1.0, 6.0, ((0, 256), (1, 4)))
    proj_gate = noise(key_list[1], (TOKENS, CH), 1.5, 8.0, ((0, 256), (1, 4)))
    out_cotangent = bell_draw_with(key_list[2], (TOKENS, D), 1.0, 24.0, ((0, 256),), (0, 1, 256, 6.0))
    out_weight = noise(key_list[3], (CH, D), CH ** -0.5, 0.1875, ((0, 4),))
    conv_taps = noise(key_list[4], (CONV_K, CH), CONV_K ** -0.5, 1.0, ((1, 4),))
    norm_gain = jnp.clip(1.0 + 0.18 * jax.random.normal(key_list[5], (CH,), jnp.float32), 0.1, 1.9)
    row_mean = noise(key_list[6], (TOKENS,), 0.3, 2.0, ((0, 256),), jnp.float32)
    row_scale = jnp.clip(jnp.exp(math.log(3.0) - 1.4552872 * jax.random.uniform(key_list[7], (TOKENS,), jnp.float32) ** level_of(key_list[7], (TOKENS,), ((0, 256),), -0.2, 0.2)), 0.7, 3.0)
    return {"proj_value": proj_value, "proj_gate": proj_gate, "out_cotangent": out_cotangent, "out_weight": out_weight, "conv_taps": conv_taps, "norm_gain": norm_gain, "row_mean": row_mean, "row_scale": row_scale}


def reference(proj_value, proj_gate, out_cotangent, out_weight, conv_taps, norm_gain, row_mean, row_scale):
    kernel = conv_taps.shape[0]
    length = proj_value.shape[0]
    channels = proj_value.shape[1]
    gate_sig = jax.nn.sigmoid(proj_gate.astype(jnp.float32))
    gated = (proj_value.astype(jnp.float32) * gate_sig).astype(jnp.bfloat16)
    padded = jnp.concatenate([jnp.zeros((kernel - 1, channels), jnp.bfloat16), gated], 0).astype(jnp.float32)
    taps_wide = conv_taps.astype(jnp.float32)
    conv = jnp.zeros((length, channels), jnp.float32)
    for offset in range(kernel):
        conv = conv + taps_wide[offset][None, :] * padded[offset:offset + length]
    normed = (conv - row_mean[:, None]) * row_scale[:, None]
    gain_wide = norm_gain.astype(jnp.float32)
    active = normed * gain_wide[None, :]
    sig_act = jax.nn.sigmoid(active)
    hidden = (active * sig_act).astype(jnp.bfloat16)
    upstream = jnp.dot(out_cotangent, out_weight.T, preferred_element_type=jnp.float32)
    weight_grad = jnp.dot(out_cotangent.T, hidden, preferred_element_type=jnp.float32)
    d_active = upstream * sig_act * (1.0 + active * (1.0 - sig_act))
    gain_grad = jnp.sum(d_active * normed, 0)
    d_normed = d_active * gain_wide[None, :]
    first = jnp.mean(d_normed, 1)
    second = jnp.mean(d_normed * normed, 1)
    d_conv = row_scale[:, None] * (d_normed - first[:, None] - normed * second[:, None])
    taps_grad = jnp.stack([jnp.sum(d_conv * padded[offset:offset + length], 0) for offset in range(kernel)])
    extended = jnp.concatenate([d_conv, jnp.zeros((kernel - 1, channels), jnp.float32)], 0)
    d_gated = jnp.zeros((length, channels), jnp.float32)
    for offset in range(kernel):
        begin = kernel - 1 - offset
        d_gated = d_gated + taps_wide[offset][None, :] * extended[begin:begin + length]
    value_grad = (d_gated * gate_sig).astype(jnp.bfloat16)
    gate_grad = (d_gated * proj_value.astype(jnp.float32) * gate_sig * (1.0 - gate_sig)).astype(jnp.bfloat16)
    return value_grad, gate_grad, weight_grad, taps_grad, gain_grad
```

```python
import jax
import jax.numpy as jnp
from jax import lax
from jax.sharding import Mesh
from jax.sharding import PartitionSpec as P

SP = ("zh", "zl", "x", "c")
NEAR = ("zl", "x")
AXES = (("zh", 16), ("zl", 2), ("x", 4), ("c", 2))


def shifted(value, axis, steps):
    count = lax.axis_size(axis)
    first, last = (max(0, -steps), min(count, count - steps))
    return lax.ppermute(value, axis, [(source, source + steps) for source in range(first, last)])


def halves(value):
    high = lax.reduce_precision(value, 8, 7)
    return high.astype(jnp.bfloat16), (value - high).astype(jnp.bfloat16)


def exchange(pieces, axes):
    return lax.all_to_all(pieces, axes, 0, 0, tiled=True)


def shards(
    proj_value, proj_gate, out_cotangent, out_weight, conv_taps, norm_gain, row_mean, row_scale
):
    kernel = conv_taps.shape[0]
    margin = kernel - 1
    length = proj_value.shape[0]
    channels = proj_value.shape[1]
    near = lax.axis_size(NEAR)
    far = lax.axis_size("zh")
    wide = jnp.float32
    gate_sig = jax.nn.sigmoid(proj_gate.astype(wide))
    gated = (proj_value.astype(wide) * gate_sig).astype(jnp.bfloat16)
    before = shifted(gated[length - margin :], SP, 1)
    padded = jnp.concatenate([before, gated], 0).astype(wide)
    taps_wide = conv_taps.astype(wide)
    conv = jnp.zeros((length, channels), wide)
    for offset in range(kernel):
        conv = conv + taps_wide[offset][None, :] * padded[offset : offset + length]
    normed = (conv - row_mean[:, None]) * row_scale[:, None]
    active = normed * norm_gain[None, :]
    sig_act = jax.nn.sigmoid(active)
    hidden = (active * sig_act).astype(jnp.bfloat16)
    upstream = lax.dot_general(
        out_cotangent, out_weight, (((1,), (1,)), ((), ())), preferred_element_type=wide
    )
    d_active = upstream * sig_act * (1.0 + active * (1.0 - sig_act))
    gain_local = jnp.sum(d_active * normed, 0)
    d_normed = d_active * norm_gain[None, :]
    sums = jnp.stack([jnp.sum(d_normed, 1), jnp.sum(d_normed * normed, 1)])
    tp = lax.axis_size("tp")
    sums = exchange(jnp.broadcast_to(sums[None], (tp, *sums.shape)), "tp").sum(0)
    first, second = sums / (channels * tp)

    weight_part = lax.dot_general(
        out_cotangent, hidden, (((0,), (0,)), ((), ())), preferred_element_type=wide
    )
    model = weight_part.shape[0]
    own = model // (near * far * 2)
    core = lax.axis_index("c")
    by_core = weight_part.reshape(far * near, 2, own, channels)
    mine = lax.dynamic_index_in_dim(by_core, core, 1, keepdims=False)
    other = lax.dynamic_index_in_dim(by_core, 1 - core, 1, keepdims=False)
    other = lax.ppermute(other.astype(jnp.bfloat16), "c", [(0, 1), (1, 0)])
    chip = (mine + other.astype(wide)).astype(jnp.bfloat16)
    chip = chip.reshape(far, near, own, channels).transpose(1, 0, 2, 3)
    chip = chip.reshape(near, far * own, channels)

    d_conv = row_scale[:, None] * (d_normed - first[:, None] - normed * second[:, None])
    small = jnp.stack(
        [jnp.sum(d_conv * padded[offset : offset + length], 0) for offset in range(kernel)]
        + [gain_local]
    )
    rows = small.shape[0] // near
    small = small.reshape(near, rows, channels)
    arrived = exchange(jnp.concatenate([chip, *halves(small)], 1), NEAR).astype(wide).sum(0)
    chip, small = arrived[: far * own], arrived[far * own :]
    small = jnp.concatenate(halves(small[:rows] + small[rows:]), 0)
    pieces = jnp.concatenate(
        [
            chip.astype(jnp.bfloat16).reshape(far, own, channels),
            jnp.broadcast_to(small[None], (far, *small.shape)),
        ],
        1,
    )
    arrived = exchange(pieces, "zh").astype(wide).sum(0)
    weight_grad, small = arrived[:own], arrived[own:]
    small = small[:rows] + small[rows:]
    small = exchange(
        jnp.broadcast_to(small[None], (near * 2, *small.shape)), (*NEAR, "c")
    ).reshape(near, 2, rows, channels)
    small = small.sum(1).reshape(near * rows, channels)
    taps_grad, gain_grad = small[:kernel], small[kernel]

    spread = jnp.zeros((length + margin, channels), wide)
    for offset in range(kernel):
        placed = taps_wide[offset][None, :] * d_conv
        spread = spread + jnp.pad(placed, ((offset, margin - offset), (0, 0)))
    arrived = shifted(spread[:margin], SP, -1)
    tail_part = jnp.concatenate([jnp.zeros((length - margin, channels), wide), arrived], 0)
    d_gated = spread[margin:] + tail_part
    value_grad = (d_gated * gate_sig).astype(jnp.bfloat16)
    gate_grad = (d_gated * proj_value.astype(wide) * gate_sig * (1.0 - gate_sig)).astype(
        jnp.bfloat16
    )
    return (value_grad, gate_grad, weight_grad, taps_grad, gain_grad)


def solution(mesh):
    sizes = [size for _, size in AXES]
    split = Mesh(mesh.devices.reshape(*sizes, mesh.shape["tp"]), (*SP, "tp"))
    placed = (
        P(SP, "tp"),
        P(SP, "tp"),
        P(SP, None),
        P("tp", None),
        P(None, "tp"),
        P("tp"),
        P(SP),
        P(SP),
    )
    return jax.shard_map(
        shards,
        mesh=split,
        in_specs=placed,
        out_specs=(P(SP, "tp"), P(SP, "tp"), P(SP, "tp"), P(None, "tp"), P("tp")),
        check_vma=False,
    )
```

```python
import functools

import jax
import jax.numpy as jnp
from jax import lax
from jax.experimental import pallas as pl
from jax.experimental.pallas import tpu as pltpu
from jax.sharding import Mesh
from jax.sharding import PartitionSpec as P

SP = ("zh", "zl", "x", "c")
NEAR = ("zl", "x")
FAR = 16
CLOSE = 8
AXES = (("zh", FAR), ("zl", 2), ("x", 4), ("c", 2))
TP = 4
TAPS = 31
ROWS = 384
EDGE = 32
LANES = 128
HALVES = 2
WIDTH = HALVES * LANES
MODEL = 2048
OWN = 8
CHUNK = 64
WIDE = jnp.float32
NARROW = jnp.bfloat16


def shifted(value, axis, steps):
    count = lax.axis_size(axis)
    first, last = (max(0, -steps), min(count, count - steps))
    return lax.ppermute(value, axis, [(source, source + steps) for source in range(first, last)])


def exchange(pieces, axes):
    return lax.all_to_all(pieces, axes, 0, 0, tiled=True)


def lanes(half):
    return slice(half * LANES, (half + 1) * LANES)


def column(row):
    return jnp.transpose(jnp.broadcast_to(row, (LANES, LANES)))


def call(body, outs, *args, flops=0, limit=24):
    shapes = [jax.ShapeDtypeStruct(shape, dtype) for shape, dtype in outs]
    size = sum(a.size * a.dtype.itemsize for a in (*args, *shapes))
    return pl.pallas_call(
        body,
        out_shape=shapes,
        compiler_params=pltpu.CompilerParams(vmem_limit_bytes=limit << 20),
        cost_estimate=pl.CostEstimate(flops=flops, bytes_accessed=size, transcendentals=0),
        name=body.__name__,
    )(*args)


def gate_and_upstream(value, gate, cotangent, weight, body, upstream):
    for start in range(0, ROWS, CHUNK):
        rows = slice(start, start + CHUNK)
        for half in range(HALVES):
            sig = jax.nn.sigmoid(gate[rows, lanes(half)].astype(WIDE))
            gated = (value[rows, lanes(half)].astype(WIDE) * sig).astype(NARROW)
            body[half, rows, :] = gated.astype(WIDE)
    product = lax.dot_general(
        cotangent[...], weight[...], (((1,), (1,)), ((), ())), preferred_element_type=WIDE
    )
    for half in range(HALVES):
        upstream[half] = product[:, lanes(half)]


def forward(
    halo, body, upstream, taps, gain, mean, scale,
    padded, scaled, spread, hidden, message, gain_part,
    taps_wide, mean_columns, scale_columns, sum_first, sum_second,
):
    taps_wide[0:TAPS] = taps[...].astype(WIDE)
    for block in range(ROWS // LANES):
        rows = slice(block * LANES, (block + 1) * LANES)
        mean_columns[rows] = column(mean[rows].reshape(1, LANES))
        scale_columns[rows] = column(scale[rows].reshape(1, LANES))
    for half in range(HALVES):
        padded[half, 0:EDGE] = halo[:, lanes(half)].astype(WIDE)
        padded[half, EDGE:] = body[half]
    for half in range(HALVES):
        gain_row = gain[0:1, lanes(half)]
        gain_sum = jnp.zeros((8, LANES), WIDE)
        for start in range(0, ROWS, CHUNK):
            rows = slice(start, start + CHUNK)
            conv = jnp.zeros((CHUNK, LANES), WIDE)
            for tap in range(TAPS):
                begin = start + tap + EDGE - TAPS + 1
                conv = conv + taps_wide[tap : tap + 1, lanes(half)] * padded[half, begin : begin + CHUNK]
            factor = scale_columns[rows]
            normed = (conv - mean_columns[rows]) * factor
            active = normed * gain_row
            sig = jax.nn.sigmoid(active)
            hidden[rows, lanes(half)] = (active * sig).astype(NARROW)
            d_active = upstream[half, rows] * sig * (1.0 + active * (1.0 - sig))
            gain_sum = gain_sum + jnp.sum((d_active * normed).reshape(CHUNK // 8, 8, LANES), 0)
            d_normed = d_active * gain_row
            scaled[half, rows] = factor * d_normed
            spread[half, rows] = factor * normed
            weighted = d_normed * normed
            if half == 0:
                sum_first[rows] = d_normed
                sum_second[rows] = weighted
            else:
                sum_first[rows] = sum_first[rows] + d_normed
                sum_second[rows] = sum_second[rows] + weighted
        gain_part[half] = gain_sum
    found = []
    for source in (sum_first, sum_second):
        for block in range(ROWS // LANES):
            turned = jnp.transpose(source[block * LANES : (block + 1) * LANES])
            found.append(jnp.sum(turned, 0, keepdims=True))
    found.append(jnp.zeros((2, LANES), WIDE))
    sums = jnp.concatenate(found, 0)
    for peer in range(TP):
        message[peer] = sums


def weight_product(core, cotangent, hidden, mine, other):
    first = core[0] == 0
    for far in range(FAR):
        part = lax.dot_general(
            cotangent[:, lanes(far)], hidden[...], (((0,), (0,)), ((), ())),
            preferred_element_type=WIDE,
        )
        part = part.reshape(CLOSE, 2, OWN, WIDTH)
        low, high = part[:, 0], part[:, 1]
        mine[:, far] = jnp.where(first, low, high)
        other[:, far] = jnp.where(first, high, low).astype(NARROW)


def halves(value):
    high = value.astype(NARROW)
    return high, (value - high.astype(WIDE)).astype(NARROW)


def backward(
    sums, scaled, spread, padded, scale, gain_part, mine, other,
    pieces, extended,
    small,
):
    total = sums[0]
    for peer in range(1, TP):
        total = total + sums[peer]
    total = total * (1.0 / (TP * WIDTH))
    blocks = ROWS // LANES
    for half in range(HALVES):
        extended[half, 0:EDGE] = jnp.zeros((EDGE, LANES), WIDE)
        extended[half, EDGE + ROWS :] = jnp.zeros((EDGE, LANES), WIDE)
    for block in range(blocks):
        rows = slice(block * LANES, (block + 1) * LANES)
        first = column(total[block : block + 1] * scale[rows].reshape(1, LANES))
        second = column(total[blocks + block : blocks + block + 1])
        for half in range(HALVES):
            d_conv = scaled[half, rows] - first - spread[half, rows] * second
            extended[half, EDGE + block * LANES : EDGE + (block + 1) * LANES] = d_conv
    for half in range(HALVES):
        for group in range(0, TAPS, 8):
            members = range(group, min(group + 8, TAPS))
            found = [jnp.zeros((8, LANES), WIDE) for _ in members]
            for start in range(0, ROWS, 8):
                d_conv = extended[half, EDGE + start : EDGE + start + 8]
                for i, tap in enumerate(members):
                    begin = start + tap + EDGE - TAPS + 1
                    found[i] = found[i] + d_conv * padded[half, begin : begin + 8]
            for i, tap in enumerate(members):
                small[tap : tap + 1, lanes(half)] = jnp.sum(found[i], 0, keepdims=True)
        small[TAPS : TAPS + 1, lanes(half)] = jnp.sum(gain_part[half], 0, keepdims=True)
    for near in range(CLOSE):
        chip = mine[near] + other[near].astype(WIDE)
        pieces[near, 0 : FAR * OWN] = chip.reshape(FAR * OWN, WIDTH).astype(NARROW)
        high, low = halves(small[near * 4 : near * 4 + 4])
        pieces[near, FAR * OWN :] = jnp.concatenate([high.astype(WIDE), low.astype(WIDE)], 0).astype(NARROW)


def gated_gradient(extended, taps, d_gated, margin, taps_wide):
    taps_wide[0:TAPS] = taps[...].astype(WIDE)
    for half in range(HALVES):
        for start in range(0, EDGE + ROWS, EDGE):
            found = jnp.zeros((EDGE, LANES), WIDE)
            for tap in range(TAPS):
                begin = start + TAPS - 1 - tap
                found = found + taps_wide[tap : tap + 1, lanes(half)] * extended[half, begin : begin + EDGE]
            if start == 0:
                margin[half] = found
            else:
                d_gated[half, start - EDGE : start] = found


def outputs(d_gated, arrived, value, gate, value_grad, gate_grad):
    for half in range(HALVES):
        for start in range(0, ROWS, EDGE):
            rows = slice(start, start + EDGE)
            grad = d_gated[half, rows]
            if start == ROWS - EDGE:
                grad = grad + arrived[half]
            sig = jax.nn.sigmoid(gate[rows, lanes(half)].astype(WIDE))
            wide = value[rows, lanes(half)].astype(WIDE)
            value_grad[rows, lanes(half)] = (grad * sig).astype(NARROW)
            gate_grad[rows, lanes(half)] = (grad * wide * sig * (1.0 - sig)).astype(NARROW)


def fold_near(arrived, pieces):
    for far in range(FAR):
        rows = slice(far * OWN, (far + 1) * OWN)
        total = arrived[0, rows].astype(WIDE)
        for near in range(1, CLOSE):
            total = total + arrived[near, rows].astype(WIDE)
        pieces[far, :, 0:WIDTH] = total.astype(NARROW)
    both = arrived[0, FAR * OWN :].astype(WIDE)
    for near in range(1, CLOSE):
        both = both + arrived[near, FAR * OWN :].astype(WIDE)
    small = both[0:4] + both[4:8]
    small = jnp.concatenate([small[:, lanes(0)], small[:, lanes(1)]], 0).astype(NARROW)
    for far in range(FAR):
        pieces[far, :, WIDTH:] = small


def fold_far(arrived, weight_grad, message):
    total = arrived[0].astype(WIDE)
    for far in range(1, FAR):
        total = total + arrived[far].astype(WIDE)
    weight_grad[...] = total[:, 0:WIDTH]
    for peer in range(CLOSE * 2):
        message[peer] = total[:, WIDTH:]


def finish(arrived, taps_grad, gain_grad):
    for near in range(CLOSE):
        total = arrived[2 * near] + arrived[2 * near + 1]
        total = jnp.concatenate([total[0:4], total[4:8]], 1)
        if near < CLOSE - 1:
            taps_grad[near * 4 : near * 4 + 4] = total
        else:
            taps_grad[near * 4 : near * 4 + 3] = total[0:3]
            gain_grad[...] = total[3:4]


def shards(
    proj_value, proj_gate, out_cotangent, out_weight, conv_taps, norm_gain, row_mean, row_scale
):
    end_gate = jax.nn.sigmoid(proj_gate[ROWS - EDGE :].astype(WIDE))
    end = (proj_value[ROWS - EDGE :].astype(WIDE) * end_gate).astype(NARROW)
    halo = shifted(end, SP, 1)
    split = (HALVES, ROWS, LANES)
    body, upstream = call(
        gate_and_upstream, [(split, WIDE), (split, WIDE)],
        proj_value, proj_gate, out_cotangent, out_weight, flops=2 * ROWS * WIDTH * MODEL,
    )
    column_scratch = [pltpu.VMEM((ROWS, LANES), WIDE)] * 4
    taps_scratch = pltpu.VMEM((TAPS + 1, WIDTH), WIDE)
    padded, scaled, spread, hidden, message, gain_part = call_with(
        forward,
        [
            ((HALVES, EDGE + ROWS, LANES), WIDE), (split, WIDE), (split, WIDE),
            ((ROWS, WIDTH), NARROW), ((TP, 8, LANES), WIDE), ((HALVES, 8, LANES), WIDE),
        ],
        [taps_scratch, *column_scratch],
        halo, body, upstream, conv_taps, norm_gain.reshape(1, WIDTH), row_mean, row_scale,
        flops=100 * ROWS * WIDTH,
    )
    sums = exchange(message, "tp")
    core = lax.axis_index("c").reshape(1)
    grouped = (CLOSE, FAR, OWN, WIDTH)
    mine, other = weight_call(core, out_cotangent, hidden, [(grouped, WIDE), (grouped, NARROW)])
    other = lax.ppermute(other, "c", [(0, 1), (1, 0)])
    pieces, extended = call_with(
        backward,
        [((CLOSE, FAR * OWN + 8, WIDTH), NARROW), ((HALVES, ROWS + 2 * EDGE, LANES), WIDE)],
        [pltpu.VMEM((TAPS + 1, WIDTH), WIDE)],
        sums, scaled, spread, padded, row_scale, gain_part, mine, other,
        flops=100 * ROWS * WIDTH,
    )
    (pieces,) = call(
        fold_near, [((FAR, OWN, WIDTH + LANES), NARROW)], exchange(pieces, NEAR), flops=1 << 20
    )
    arrived = exchange(pieces, "zh")
    d_gated, margin = call_with(
        gated_gradient, [(split, WIDE), ((HALVES, EDGE, LANES), WIDE)], [taps_scratch],
        extended, conv_taps, flops=100 * ROWS * WIDTH,
    )
    late = shifted(margin, SP, -1)
    value_grad, gate_grad = call(
        outputs, [((ROWS, WIDTH), NARROW), ((ROWS, WIDTH), NARROW)],
        d_gated, late, proj_value, proj_gate, flops=10 * ROWS * WIDTH,
    )
    weight_grad, message = call(
        fold_far, [((OWN, WIDTH), WIDE), ((CLOSE * 2, 8, LANES), WIDE)], arrived, flops=1 << 16
    )
    taps_grad, gain_grad = call(
        finish, [((TAPS, WIDTH), WIDE), ((1, WIDTH), WIDE)],
        exchange(message, (*NEAR, "c")), flops=1 << 16,
    )
    return (value_grad, gate_grad, weight_grad, taps_grad, gain_grad.reshape(WIDTH))


def call_with(body, outs, scratch, *args, flops=0, limit=24):
    shapes = [jax.ShapeDtypeStruct(shape, dtype) for shape, dtype in outs]
    size = sum(a.size * a.dtype.itemsize for a in (*args, *shapes))
    return pl.pallas_call(
        body,
        out_shape=shapes,
        scratch_shapes=scratch,
        compiler_params=pltpu.CompilerParams(vmem_limit_bytes=limit << 20),
        cost_estimate=pl.CostEstimate(flops=flops, bytes_accessed=size, transcendentals=0),
        name=body.__name__,
    )(*args)


def weight_call(core, cotangent, hidden, outs):
    whole = pl.BlockSpec(memory_space=pltpu.VMEM)
    return pl.pallas_call(
        weight_product,
        out_shape=[jax.ShapeDtypeStruct(shape, dtype) for shape, dtype in outs],
        in_specs=[pl.BlockSpec(memory_space=pltpu.SMEM), whole, whole],
        out_specs=[whole, whole],
        compiler_params=pltpu.CompilerParams(vmem_limit_bytes=24 << 20),
        cost_estimate=pl.CostEstimate(
            flops=2 * ROWS * WIDTH * MODEL, bytes_accessed=4 << 20, transcendentals=0
        ),
        name="weight_product",
    )(core, cotangent, hidden)


def solution(mesh):
    sizes = [size for _, size in AXES]
    split = Mesh(mesh.devices.reshape(*sizes, mesh.shape["tp"]), (*SP, "tp"))
    placed = (
        P(SP, "tp"),
        P(SP, "tp"),
        P(SP, None),
        P("tp", None),
        P(None, "tp"),
        P("tp"),
        P(SP),
        P(SP),
    )
    return jax.shard_map(
        shards,
        mesh=split,
        in_specs=placed,
        out_specs=(P(SP, "tp"), P(SP, "tp"), P(SP, "tp"), P(None, "tp"), P("tp")),
        check_vma=False,
    )
```

```python
import jax
import jax.numpy as jnp
from jax import lax
from jax.experimental import pallas as pl
from jax.experimental.pallas import tpu as pltpu
from jax.sharding import Mesh
from jax.sharding import PartitionSpec as P


SP = ("zh", "zl", "x", "c")
NEAR = ("zl", "x")
FAR = 16
CLOSE = 8
AXES = (("zh", FAR), ("zl", 2), ("x", 4), ("c", 2))
TP = 4
TAPS = 31
ROWS = 384
EDGE = 32
LANES = 128
HALVES = 2
WIDTH = HALVES * LANES
MODEL = 2048
OWN = 8
CHUNK = 64
WIDE = jnp.float32
NARROW = jnp.bfloat16


def shifted(value, axis, steps):
    count = lax.axis_size(axis)
    first, last = (max(0, -steps), min(count, count - steps))
    return lax.ppermute(value, axis, [(source, source + steps) for source in range(first, last)])


def exchange(pieces, axes):
    return lax.all_to_all(pieces, axes, 0, 0, tiled=True)


def lanes(half):
    return slice(half * LANES, (half + 1) * LANES)


def column(row):
    return jnp.transpose(jnp.broadcast_to(row, (LANES, LANES)))


def call(body, outs, *args, flops=0, limit=6):
    shapes = [jax.ShapeDtypeStruct(shape, dtype) for shape, dtype in outs]
    size = sum(a.size * a.dtype.itemsize for a in (*args, *shapes))
    return pl.pallas_call(
        body,
        out_shape=shapes,
        compiler_params=pltpu.CompilerParams(vmem_limit_bytes=limit << 20),
        cost_estimate=pl.CostEstimate(flops=flops, bytes_accessed=size, transcendentals=0),
    )(*args)


def gate_and_upstream(
    value, gate, cotangent, weight, body, upstream, held, held_value, held_gate, held_weight, arrivals
):
    parts = ROWS // LANES
    copies = [
        pltpu.make_async_copy(value, held_value, arrivals.at[0]),
        pltpu.make_async_copy(gate, held_gate, arrivals.at[1]),
        pltpu.make_async_copy(weight, held_weight, arrivals.at[2]),
    ]
    for part in range(parts):
        rows = pl.ds(part * LANES, LANES)
        copies.append(
            pltpu.make_async_copy(cotangent.at[rows], held.at[rows], arrivals.at[3 + part])
        )
    for copy in copies:
        copy.start()
    copies[0].wait()
    copies[1].wait()
    for start in range(0, ROWS, CHUNK):
        rows = slice(start, start + CHUNK)
        for half in range(HALVES):
            sig = jax.nn.sigmoid(held_gate[rows, lanes(half)].astype(WIDE))
            gated = (held_value[rows, lanes(half)].astype(WIDE) * sig).astype(NARROW)
            body[half, rows, :] = gated.astype(WIDE)
    copies[2].wait()
    for part in range(parts):
        rows = slice(part * LANES, (part + 1) * LANES)
        copies[3 + part].wait()
        product = lax.dot_general(
            held[rows], held_weight[...], (((1,), (1,)), ((), ())), preferred_element_type=WIDE
        )
        for half in range(HALVES):
            upstream[half, rows] = product[:, lanes(half)]


def forward(
    halo, body, upstream, taps, gain, mean, scale,
    padded, scaled, spread, hidden, message, gain_part,
    taps_wide, mean_columns, scale_columns, sum_first, sum_second,
):
    taps_wide[0:TAPS] = taps[...].astype(WIDE)
    for block in range(ROWS // LANES):
        rows = slice(block * LANES, (block + 1) * LANES)
        mean_columns[rows] = column(mean[rows].reshape(1, LANES))
        scale_columns[rows] = column(scale[rows].reshape(1, LANES))
    for half in range(HALVES):
        padded[half, 0:EDGE] = halo[:, lanes(half)].astype(WIDE)
        padded[half, EDGE:] = body[half]
    for half in range(HALVES):
        gain_row = gain[0:1, lanes(half)]
        gain_sum = jnp.zeros((8, LANES), WIDE)
        for start in range(0, ROWS, CHUNK):
            rows = slice(start, start + CHUNK)
            conv = jnp.zeros((CHUNK, LANES), WIDE)
            for tap in range(TAPS):
                begin = start + tap + EDGE - TAPS + 1
                conv = conv + taps_wide[tap : tap + 1, lanes(half)] * padded[half, begin : begin + CHUNK]
            factor = scale_columns[rows]
            normed = (conv - mean_columns[rows]) * factor
            active = normed * gain_row
            sig = jax.nn.sigmoid(active)
            hidden[rows, lanes(half)] = (active * sig).astype(NARROW)
            d_active = upstream[half, rows] * sig * (1.0 + active * (1.0 - sig))
            gain_sum = gain_sum + jnp.sum((d_active * normed).reshape(CHUNK // 8, 8, LANES), 0)
            d_normed = d_active * gain_row
            scaled[half, rows] = factor * d_normed
            spread[half, rows] = factor * normed
            weighted = d_normed * normed
            if half == 0:
                sum_first[rows] = d_normed
                sum_second[rows] = weighted
            else:
                sum_first[rows] = sum_first[rows] + d_normed
                sum_second[rows] = sum_second[rows] + weighted
        gain_part[half] = gain_sum
    found = []
    for source in (sum_first, sum_second):
        for block in range(ROWS // LANES):
            turned = jnp.transpose(source[block * LANES : (block + 1) * LANES])
            found.append(jnp.sum(turned, 0, keepdims=True))
    found.append(jnp.zeros((2, LANES), WIDE))
    sums = jnp.concatenate(found, 0)
    for peer in range(TP):
        message[peer] = sums


def weight_product(core, cotangent, hidden, mine, other):
    first = core[0] == 0
    for far in range(FAR):
        part = lax.dot_general(
            cotangent[:, lanes(far)], hidden[...], (((0,), (0,)), ((), ())),
            preferred_element_type=WIDE,
        )
        part = part.reshape(CLOSE, 2, OWN, WIDTH)
        low, high = part[:, 0], part[:, 1]
        mine[:, far] = jnp.where(first, low, high)
        other[:, far] = jnp.where(first, high, low).astype(NARROW)


def halves(value):
    high = value.astype(NARROW)
    return high, (value - high.astype(WIDE)).astype(NARROW)


def backward(
    sums, scaled, spread, padded, scale, gain_part, mine, other,
    pieces, extended,
    small,
):
    total = sums[0]
    for peer in range(1, TP):
        total = total + sums[peer]
    total = total * (1.0 / (TP * WIDTH))
    blocks = ROWS // LANES
    for half in range(HALVES):
        extended[half, 0:EDGE] = jnp.zeros((EDGE, LANES), WIDE)
        extended[half, EDGE + ROWS :] = jnp.zeros((EDGE, LANES), WIDE)
    for block in range(blocks):
        rows = slice(block * LANES, (block + 1) * LANES)
        first = column(total[block : block + 1] * scale[rows].reshape(1, LANES))
        second = column(total[blocks + block : blocks + block + 1])
        for half in range(HALVES):
            d_conv = scaled[half, rows] - first - spread[half, rows] * second
            extended[half, EDGE + block * LANES : EDGE + (block + 1) * LANES] = d_conv
    for half in range(HALVES):
        for group in range(0, TAPS, 8):
            members = range(group, min(group + 8, TAPS))
            found = [jnp.zeros((8, LANES), WIDE) for _ in members]
            for start in range(0, ROWS, 8):
                d_conv = extended[half, EDGE + start : EDGE + start + 8]
                for i, tap in enumerate(members):
                    begin = start + tap + EDGE - TAPS + 1
                    found[i] = found[i] + d_conv * padded[half, begin : begin + 8]
            for i, tap in enumerate(members):
                small[tap : tap + 1, lanes(half)] = jnp.sum(found[i], 0, keepdims=True)
        small[TAPS : TAPS + 1, lanes(half)] = jnp.sum(gain_part[half], 0, keepdims=True)
    for near in range(CLOSE):
        chip = mine[near] + other[near].astype(WIDE)
        pieces[near, 0 : FAR * OWN] = chip.reshape(FAR * OWN, WIDTH).astype(NARROW)
        high, low = halves(small[near * 4 : near * 4 + 4])
        pieces[near, FAR * OWN :] = jnp.concatenate([high.astype(WIDE), low.astype(WIDE)], 0).astype(NARROW)


def gated_gradient(extended, taps, d_gated, margin, taps_wide):
    taps_wide[0:TAPS] = taps[...].astype(WIDE)
    for half in range(HALVES):
        for start in range(0, EDGE + ROWS, EDGE):
            found = jnp.zeros((EDGE, LANES), WIDE)
            for tap in range(TAPS):
                begin = start + TAPS - 1 - tap
                found = found + taps_wide[tap : tap + 1, lanes(half)] * extended[half, begin : begin + EDGE]
            if start == 0:
                margin[half] = found
            else:
                d_gated[half, start - EDGE : start] = found


def outputs(d_gated, arrived, value, gate, value_grad, gate_grad):
    for half in range(HALVES):
        for start in range(0, ROWS, EDGE):
            rows = slice(start, start + EDGE)
            grad = d_gated[half, rows]
            if start == ROWS - EDGE:
                grad = grad + arrived[half]
            sig = jax.nn.sigmoid(gate[rows, lanes(half)].astype(WIDE))
            wide = value[rows, lanes(half)].astype(WIDE)
            value_grad[rows, lanes(half)] = (grad * sig).astype(NARROW)
            gate_grad[rows, lanes(half)] = (grad * wide * sig * (1.0 - sig)).astype(NARROW)


def fold_near(arrived, pieces):
    for far in range(FAR):
        rows = slice(far * OWN, (far + 1) * OWN)
        total = arrived[0, rows].astype(WIDE)
        for near in range(1, CLOSE):
            total = total + arrived[near, rows].astype(WIDE)
        pieces[far, :, 0:WIDTH] = total.astype(NARROW)
    both = arrived[0, FAR * OWN :].astype(WIDE)
    for near in range(1, CLOSE):
        both = both + arrived[near, FAR * OWN :].astype(WIDE)
    small = both[0:4] + both[4:8]
    small = jnp.concatenate([small[:, lanes(0)], small[:, lanes(1)]], 0).astype(NARROW)
    for far in range(FAR):
        pieces[far, :, WIDTH:] = small


def fold_far(arrived, weight_grad, message):
    total = arrived[0].astype(WIDE)
    for far in range(1, FAR):
        total = total + arrived[far].astype(WIDE)
    weight_grad[...] = total[:, 0:WIDTH]
    for peer in range(CLOSE * 2):
        message[peer] = total[:, WIDTH:]


def finish(arrived, taps_grad, gain_grad):
    for near in range(CLOSE):
        total = arrived[2 * near] + arrived[2 * near + 1]
        total = jnp.concatenate([total[0:4], total[4:8]], 1)
        if near < CLOSE - 1:
            taps_grad[near * 4 : near * 4 + 4] = total
        else:
            taps_grad[near * 4 : near * 4 + 3] = total[0:3]
            gain_grad[...] = total[3:4]


def shards(
    proj_value, proj_gate, out_cotangent, out_weight, conv_taps, norm_gain, row_mean, row_scale
):
    end_gate = jax.nn.sigmoid(proj_gate[ROWS - EDGE :].astype(WIDE))
    end = (proj_value[ROWS - EDGE :].astype(WIDE) * end_gate).astype(NARROW)
    halo = shifted(end, SP, 1)
    split = (HALVES, ROWS, LANES)
    body, upstream, held = first_call(
        [(split, WIDE), (split, WIDE), ((ROWS, MODEL), NARROW)],
        proj_value, proj_gate, out_cotangent, out_weight,
    )
    column_scratch = [pltpu.VMEM((ROWS, LANES), WIDE)] * 4
    taps_scratch = pltpu.VMEM((TAPS + 1, WIDTH), WIDE)
    padded, scaled, spread, hidden, message, gain_part = call_with(
        forward,
        [
            ((HALVES, EDGE + ROWS, LANES), WIDE), (split, WIDE), (split, WIDE),
            ((ROWS, WIDTH), NARROW), ((TP, 8, LANES), WIDE), ((HALVES, 8, LANES), WIDE),
        ],
        [taps_scratch, *column_scratch],
        halo, body, upstream, conv_taps, norm_gain.reshape(1, WIDTH), row_mean, row_scale,
        flops=100 * ROWS * WIDTH,
    )
    sums = exchange(message, "tp")
    core = lax.axis_index("c").reshape(1)
    grouped = (CLOSE, FAR, OWN, WIDTH)
    mine, other = weight_call(core, held, hidden, [(grouped, WIDE), (grouped, NARROW)])
    other = lax.ppermute(other, "c", [(0, 1), (1, 0)])
    pieces, extended = call_with(
        backward,
        [((CLOSE, FAR * OWN + 8, WIDTH), NARROW), ((HALVES, ROWS + 2 * EDGE, LANES), WIDE)],
        [pltpu.VMEM((TAPS + 1, WIDTH), WIDE)],
        sums, scaled, spread, padded, row_scale, gain_part, mine, other,
        flops=100 * ROWS * WIDTH,
    )
    (pieces,) = call(
        fold_near, [((FAR, OWN, WIDTH + LANES), NARROW)], exchange(pieces, NEAR), flops=1 << 20
    )
    arrived = exchange(pieces, "zh")
    d_gated, margin = call_with(
        gated_gradient, [(split, WIDE), ((HALVES, EDGE, LANES), WIDE)], [taps_scratch],
        extended, conv_taps, flops=100 * ROWS * WIDTH,
    )
    late = shifted(margin, SP, -1)
    value_grad, gate_grad = call(
        outputs, [((ROWS, WIDTH), NARROW), ((ROWS, WIDTH), NARROW)],
        d_gated, late, proj_value, proj_gate, flops=10 * ROWS * WIDTH,
    )
    weight_grad, message = call(
        fold_far, [((OWN, WIDTH), WIDE), ((CLOSE * 2, 8, LANES), WIDE)], arrived, flops=1 << 16
    )
    taps_grad, gain_grad = call(
        finish, [((TAPS, WIDTH), WIDE), ((1, WIDTH), WIDE)],
        exchange(message, (*NEAR, "c")), flops=1 << 16,
    )
    return (value_grad, gate_grad, weight_grad, taps_grad, gain_grad.reshape(WIDTH))


def call_with(body, outs, scratch, *args, flops=0, limit=6):
    shapes = [jax.ShapeDtypeStruct(shape, dtype) for shape, dtype in outs]
    size = sum(a.size * a.dtype.itemsize for a in (*args, *shapes))
    return pl.pallas_call(
        body,
        out_shape=shapes,
        scratch_shapes=scratch,
        compiler_params=pltpu.CompilerParams(vmem_limit_bytes=limit << 20),
        cost_estimate=pl.CostEstimate(flops=flops, bytes_accessed=size, transcendentals=0),
    )(*args)


def first_call(outs, *args):
    narrow = (ROWS, WIDTH)
    return pl.pallas_call(
        gate_and_upstream,
        out_shape=[jax.ShapeDtypeStruct(shape, dtype) for shape, dtype in outs],
        in_specs=[pl.BlockSpec(memory_space=pltpu.HBM)] * 4,
        out_specs=[pl.BlockSpec(memory_space=pltpu.VMEM)] * 3,
        scratch_shapes=[
            pltpu.VMEM(narrow, NARROW),
            pltpu.VMEM(narrow, NARROW),
            pltpu.VMEM((WIDTH, MODEL), NARROW),
            pltpu.SemaphoreType.DMA((3 + ROWS // LANES,)),
        ],
        compiler_params=pltpu.CompilerParams(vmem_limit_bytes=6 << 20),
        cost_estimate=pl.CostEstimate(
            flops=2 * ROWS * WIDTH * MODEL, bytes_accessed=4 << 20, transcendentals=0
        ),
        name="gate_and_upstream",
    )(*(pltpu.with_memory_space_constraint(a, pltpu.HBM) for a in args))


def weight_call(core, cotangent, hidden, outs):
    whole = pl.BlockSpec(memory_space=pltpu.VMEM)
    return pl.pallas_call(
        weight_product,
        out_shape=[jax.ShapeDtypeStruct(shape, dtype) for shape, dtype in outs],
        in_specs=[pl.BlockSpec(memory_space=pltpu.SMEM), whole, whole],
        out_specs=[whole, whole],
        compiler_params=pltpu.CompilerParams(vmem_limit_bytes=6 << 20),
        cost_estimate=pl.CostEstimate(
            flops=2 * ROWS * WIDTH * MODEL, bytes_accessed=4 << 20, transcendentals=0
        ),
        name="weight_product",
    )(core, cotangent, hidden)


def solution(mesh):
    sizes = [size for _, size in AXES]
    split = Mesh(mesh.devices.reshape(*sizes, mesh.shape["tp"]), (*SP, "tp"))
    placed = (
        P(SP, "tp"),
        P(SP, "tp"),
        P(SP, None),
        P("tp", None),
        P(None, "tp"),
        P("tp"),
        P(SP),
        P(SP),
    )
    return jax.shard_map(
        shards,
        mesh=split,
        in_specs=placed,
        out_specs=(P(SP, "tp"), P(SP, "tp"), P(SP, "tp"), P(None, "tp"), P("tp")),
        check_vma=False,
    )
```

```python
import jax
import jax.numpy as jnp
from jax import lax
from jax.experimental import pallas as pl
from jax.experimental.pallas import tpu as pltpu
from jax.sharding import Mesh
from jax.sharding import PartitionSpec as P


SP = ("zh", "zl", "x", "c")
NEAR = ("zl", "x")
FAR = 16
CLOSE = 8
AXES = (("zh", FAR), ("zl", 2), ("x", 4), ("c", 2))
FAR_ORDER = [(place + 10) % FAR for place in range(FAR)]
TP = 4
TAPS = 31
ROWS = 384
EDGE = 32
LANES = 128
HALVES = 2
WIDTH = HALVES * LANES
MODEL = 2048
OWN = 8
CHUNK = 64
WIDE = jnp.float32
NARROW = jnp.bfloat16


def shifted(value, axis, steps):
    count = lax.axis_size(axis)
    first, last = (max(0, -steps), min(count, count - steps))
    return lax.ppermute(value, axis, [(source, source + steps) for source in range(first, last)])


def exchange(pieces, axes, order=None):
    groups = order and [order]
    return lax.all_to_all(pieces, axes, 0, 0, tiled=True, axis_index_groups=groups)


def lanes(half):
    return slice(half * LANES, (half + 1) * LANES)


def column(row):
    return jnp.transpose(jnp.broadcast_to(row, (LANES, LANES)))


def call(body, outs, *args, flops=0, limit=6):
    shapes = [jax.ShapeDtypeStruct(shape, dtype) for shape, dtype in outs]
    size = sum(a.size * a.dtype.itemsize for a in (*args, *shapes))
    return pl.pallas_call(
        body,
        out_shape=shapes,
        compiler_params=pltpu.CompilerParams(vmem_limit_bytes=limit << 20),
        cost_estimate=pl.CostEstimate(flops=flops, bytes_accessed=size, transcendentals=0),
    )(*args)


def forward(
    halo, value, gate, upstream, taps, gain, mean, scale,
    padded, scaled, spread, hidden, message, gain_part,
    taps_wide, mean_columns, scale_columns, sum_first, sum_second,
):
    taps_wide[0:TAPS] = taps[...].astype(WIDE)
    for block in range(ROWS // LANES):
        rows = slice(block * LANES, (block + 1) * LANES)
        mean_columns[rows] = column(mean[rows].reshape(1, LANES))
        scale_columns[rows] = column(scale[rows].reshape(1, LANES))
    for half in range(HALVES):
        padded[half, 0:EDGE] = halo[:, lanes(half)].astype(WIDE)
        for start in range(0, ROWS, CHUNK):
            rows = slice(start, start + CHUNK)
            sig = jax.nn.sigmoid(gate[rows, lanes(half)].astype(WIDE))
            gated = (value[rows, lanes(half)].astype(WIDE) * sig).astype(NARROW)
            padded[half, EDGE + start : EDGE + start + CHUNK] = gated.astype(WIDE)
    for half in range(HALVES):
        gain_row = gain[0:1, lanes(half)]
        gain_sum = jnp.zeros((8, LANES), WIDE)
        for start in range(0, ROWS, CHUNK):
            rows = slice(start, start + CHUNK)
            conv = jnp.zeros((CHUNK, LANES), WIDE)
            for tap in range(TAPS):
                begin = start + tap + EDGE - TAPS + 1
                conv = conv + taps_wide[tap : tap + 1, lanes(half)] * padded[half, begin : begin + CHUNK]
            factor = scale_columns[rows]
            normed = (conv - mean_columns[rows]) * factor
            active = normed * gain_row
            sig = jax.nn.sigmoid(active)
            hidden[rows, lanes(half)] = (active * sig).astype(NARROW)
            d_active = upstream[rows, lanes(half)] * sig * (1.0 + active * (1.0 - sig))
            gain_sum = gain_sum + jnp.sum((d_active * normed).reshape(CHUNK // 8, 8, LANES), 0)
            d_normed = d_active * gain_row
            scaled[half, rows] = factor * d_normed
            spread[half, rows] = factor * normed
            weighted = d_normed * normed
            if half == 0:
                sum_first[rows] = d_normed
                sum_second[rows] = weighted
            else:
                sum_first[rows] = sum_first[rows] + d_normed
                sum_second[rows] = sum_second[rows] + weighted
        gain_part[half] = gain_sum
    found = []
    for source in (sum_first, sum_second):
        for block in range(ROWS // LANES):
            turned = jnp.transpose(source[block * LANES : (block + 1) * LANES])
            found.append(jnp.sum(turned, 0, keepdims=True))
    found.append(jnp.zeros((2, LANES), WIDE))
    sums = jnp.concatenate(found, 0)
    for peer in range(TP):
        message[peer] = sums


def weight_product(core, cotangent, hidden, mine, other):
    first = core[0] == 0
    for far in range(FAR):
        part = lax.dot_general(
            cotangent[:, lanes(far)], hidden[...], (((0,), (0,)), ((), ())),
            preferred_element_type=WIDE,
        )
        part = part.reshape(CLOSE, 2, OWN, WIDTH)
        low, high = part[:, 0], part[:, 1]
        mine[:, far] = jnp.where(first, low, high)
        other[:, far] = jnp.where(first, high, low).astype(NARROW)


def halves(value):
    high = value.astype(NARROW)
    return high, (value - high.astype(WIDE)).astype(NARROW)


def backward(
    sums, scaled, spread, padded, scale, gain_part, mine, other,
    pieces, extended,
    small,
):
    total = sums[0]
    for peer in range(1, TP):
        total = total + sums[peer]
    total = total * (1.0 / (TP * WIDTH))
    blocks = ROWS // LANES
    for half in range(HALVES):
        extended[half, 0:EDGE] = jnp.zeros((EDGE, LANES), WIDE)
        extended[half, EDGE + ROWS :] = jnp.zeros((EDGE, LANES), WIDE)
    for block in range(blocks):
        rows = slice(block * LANES, (block + 1) * LANES)
        first = column(total[block : block + 1] * scale[rows].reshape(1, LANES))
        second = column(total[blocks + block : blocks + block + 1])
        for half in range(HALVES):
            d_conv = scaled[half, rows] - first - spread[half, rows] * second
            extended[half, EDGE + block * LANES : EDGE + (block + 1) * LANES] = d_conv
    for half in range(HALVES):
        for group in range(0, TAPS, 8):
            members = range(group, min(group + 8, TAPS))
            found = [jnp.zeros((8, LANES), WIDE) for _ in members]
            for start in range(0, ROWS, 8):
                d_conv = extended[half, EDGE + start : EDGE + start + 8]
                for i, tap in enumerate(members):
                    begin = start + tap + EDGE - TAPS + 1
                    found[i] = found[i] + d_conv * padded[half, begin : begin + 8]
            for i, tap in enumerate(members):
                small[tap : tap + 1, lanes(half)] = jnp.sum(found[i], 0, keepdims=True)
        small[TAPS : TAPS + 1, lanes(half)] = jnp.sum(gain_part[half], 0, keepdims=True)
    for near in range(CLOSE):
        chip = mine[near] + other[near].astype(WIDE)
        pieces[near, 0 : FAR * OWN] = chip.reshape(FAR * OWN, WIDTH).astype(NARROW)
        high, low = halves(small[near * 4 : near * 4 + 4])
        pieces[near, FAR * OWN :] = jnp.concatenate([high.astype(WIDE), low.astype(WIDE)], 0).astype(NARROW)


def gated_gradient(extended, taps, d_gated, margin, taps_wide):
    taps_wide[0:TAPS] = taps[...].astype(WIDE)
    for half in range(HALVES):
        for start in range(0, EDGE + ROWS, EDGE):
            found = jnp.zeros((EDGE, LANES), WIDE)
            for tap in range(TAPS):
                begin = start + TAPS - 1 - tap
                found = found + taps_wide[tap : tap + 1, lanes(half)] * extended[half, begin : begin + EDGE]
            if start == 0:
                margin[half] = found
            else:
                d_gated[half, start - EDGE : start] = found


def outputs(d_gated, arrived, value, gate, value_grad, gate_grad):
    for half in range(HALVES):
        for start in range(0, ROWS, EDGE):
            rows = slice(start, start + EDGE)
            grad = d_gated[half, rows]
            if start == ROWS - EDGE:
                grad = grad + arrived[half]
            sig = jax.nn.sigmoid(gate[rows, lanes(half)].astype(WIDE))
            wide = value[rows, lanes(half)].astype(WIDE)
            value_grad[rows, lanes(half)] = (grad * sig).astype(NARROW)
            gate_grad[rows, lanes(half)] = (grad * wide * sig * (1.0 - sig)).astype(NARROW)


def fold_near(arrived, pieces):
    for far in range(FAR):
        rows = slice(far * OWN, (far + 1) * OWN)
        total = arrived[0, rows].astype(WIDE)
        for near in range(1, CLOSE):
            total = total + arrived[near, rows].astype(WIDE)
        pieces[FAR_ORDER.index(far), :, 0:WIDTH] = total.astype(NARROW)
    both = arrived[0, FAR * OWN :].astype(WIDE)
    for near in range(1, CLOSE):
        both = both + arrived[near, FAR * OWN :].astype(WIDE)
    small = both[0:4] + both[4:8]
    small = jnp.concatenate([small[:, lanes(0)], small[:, lanes(1)]], 0).astype(NARROW)
    for far in range(FAR):
        pieces[far, :, WIDTH:] = small


def fold_far(arrived, weight_grad, message):
    total = arrived[0].astype(WIDE)
    for far in range(1, FAR):
        total = total + arrived[far].astype(WIDE)
    weight_grad[...] = total[:, 0:WIDTH]
    for peer in range(CLOSE * 2):
        message[peer] = total[:, WIDTH:]


def finish(arrived, taps_grad, gain_grad):
    for near in range(CLOSE):
        total = arrived[2 * near] + arrived[2 * near + 1]
        total = jnp.concatenate([total[0:4], total[4:8]], 1)
        if near < CLOSE - 1:
            taps_grad[near * 4 : near * 4 + 4] = total
        else:
            taps_grad[near * 4 : near * 4 + 3] = total[0:3]
            gain_grad[...] = total[3:4]


def shards(
    proj_value, proj_gate, out_cotangent, out_weight, conv_taps, norm_gain, row_mean, row_scale
):
    end_gate = jax.nn.sigmoid(proj_gate[ROWS - EDGE :].astype(WIDE))
    end = (proj_value[ROWS - EDGE :].astype(WIDE) * end_gate).astype(NARROW)
    halo = shifted(end, SP, 1)
    split = (HALVES, ROWS, LANES)
    upstream = lax.dot_general(
        out_cotangent, out_weight, (((1,), (1,)), ((), ())), preferred_element_type=WIDE
    )
    column_scratch = [pltpu.VMEM((ROWS, LANES), WIDE)] * 4
    taps_scratch = pltpu.VMEM((TAPS + 1, WIDTH), WIDE)
    padded, scaled, spread, hidden, message, gain_part = call_with(
        forward,
        [
            ((HALVES, EDGE + ROWS, LANES), WIDE), (split, WIDE), (split, WIDE),
            ((ROWS, WIDTH), NARROW), ((TP, 8, LANES), WIDE), ((HALVES, 8, LANES), WIDE),
        ],
        [taps_scratch, *column_scratch],
        halo, proj_value, proj_gate, upstream, conv_taps, norm_gain.reshape(1, WIDTH), row_mean, row_scale,
        flops=100 * ROWS * WIDTH,
    )
    sums = exchange(message, "tp")
    core = lax.axis_index("c").reshape(1)
    grouped = (CLOSE, FAR, OWN, WIDTH)
    mine, other = weight_call(core, out_cotangent, hidden, [(grouped, WIDE), (grouped, NARROW)])
    other = lax.ppermute(other, "c", [(0, 1), (1, 0)])
    pieces, extended = call_with(
        backward,
        [((CLOSE, FAR * OWN + 8, WIDTH), NARROW), ((HALVES, ROWS + 2 * EDGE, LANES), WIDE)],
        [pltpu.VMEM((TAPS + 1, WIDTH), WIDE)],
        sums, scaled, spread, padded, row_scale, gain_part, mine, other,
        flops=100 * ROWS * WIDTH,
    )
    (pieces,) = call(
        fold_near, [((FAR, OWN, WIDTH + LANES), NARROW)], exchange(pieces, NEAR), flops=1 << 20
    )
    arrived = exchange(pieces, "zh", FAR_ORDER)
    d_gated, margin = call_with(
        gated_gradient, [(split, WIDE), ((HALVES, EDGE, LANES), WIDE)], [taps_scratch],
        extended, conv_taps, flops=100 * ROWS * WIDTH,
    )
    late = shifted(margin, SP, -1)
    value_grad, gate_grad = call(
        outputs, [((ROWS, WIDTH), NARROW), ((ROWS, WIDTH), NARROW)],
        d_gated, late, proj_value, proj_gate, flops=10 * ROWS * WIDTH,
    )
    weight_grad, message = call(
        fold_far, [((OWN, WIDTH), WIDE), ((CLOSE * 2, 8, LANES), WIDE)], arrived, flops=1 << 16
    )
    taps_grad, gain_grad = call(
        finish, [((TAPS, WIDTH), WIDE), ((1, WIDTH), WIDE)],
        exchange(message, (*NEAR, "c")), flops=1 << 16,
    )
    return (value_grad, gate_grad, weight_grad, taps_grad, gain_grad.reshape(WIDTH))


def call_with(body, outs, scratch, *args, flops=0, limit=6):
    shapes = [jax.ShapeDtypeStruct(shape, dtype) for shape, dtype in outs]
    size = sum(a.size * a.dtype.itemsize for a in (*args, *shapes))
    return pl.pallas_call(
        body,
        out_shape=shapes,
        scratch_shapes=scratch,
        compiler_params=pltpu.CompilerParams(vmem_limit_bytes=limit << 20),
        cost_estimate=pl.CostEstimate(flops=flops, bytes_accessed=size, transcendentals=0),
    )(*args)


def weight_call(core, cotangent, hidden, outs):
    whole = pl.BlockSpec(memory_space=pltpu.VMEM)
    return pl.pallas_call(
        weight_product,
        out_shape=[jax.ShapeDtypeStruct(shape, dtype) for shape, dtype in outs],
        in_specs=[pl.BlockSpec(memory_space=pltpu.SMEM), whole, whole],
        out_specs=[whole, whole],
        compiler_params=pltpu.CompilerParams(vmem_limit_bytes=6 << 20),
        cost_estimate=pl.CostEstimate(
            flops=2 * ROWS * WIDTH * MODEL, bytes_accessed=4 << 20, transcendentals=0
        ),
        name="weight_product",
    )(core, cotangent, hidden)


def solution(mesh):
    sizes = [size for _, size in AXES]
    split = Mesh(mesh.devices.reshape(*sizes, mesh.shape["tp"]), (*SP, "tp"))
    placed = (
        P(SP, "tp"),
        P(SP, "tp"),
        P(SP, None),
        P("tp", None),
        P(None, "tp"),
        P("tp"),
        P(SP),
        P(SP),
    )
    return jax.shard_map(
        shards,
        mesh=split,
        in_specs=placed,
        out_specs=(P(SP, "tp"), P(SP, "tp"), P(SP, "tp"), P(None, "tp"), P("tp")),
        check_vma=False,
    )
```

```python
import jax
import jax.numpy as jnp
from jax import lax
from jax.experimental import pallas as pl
from jax.experimental.pallas import tpu as pltpu
from jax.sharding import Mesh
from jax.sharding import PartitionSpec as P


SP = ("zh", "zl", "x", "c")
NEAR = ("zl", "x")
FAR = 16
CLOSE = 8
AXES = (("zh", FAR), ("zl", 2), ("x", 4), ("c", 2))
FAR_ORDER = [(place + 10) % FAR for place in range(FAR)]
GATHER_ORDER = [place ^ 1 for place in range(CLOSE * 2)]
TP = 4
TAPS = 31
ROWS = 384
EDGE = 32
LANES = 128
HALVES = 2
WIDTH = HALVES * LANES
MODEL = 2048
OWN = 8
CHUNK = 64
WIDE = jnp.float32
NARROW = jnp.bfloat16


def shifted(value, axis, steps):
    count = lax.axis_size(axis)
    first, last = (max(0, -steps), min(count, count - steps))
    return lax.ppermute(value, axis, [(source, source + steps) for source in range(first, last)])


def exchange(pieces, axes, order=None):
    groups = order and [order]
    return lax.all_to_all(pieces, axes, 0, 0, tiled=True, axis_index_groups=groups)


def lanes(half):
    return slice(half * LANES, (half + 1) * LANES)


def column(row):
    return jnp.transpose(jnp.broadcast_to(row, (LANES, LANES)))


def call(body, outs, *args, flops=0, limit=6):
    shapes = [jax.ShapeDtypeStruct(shape, dtype) for shape, dtype in outs]
    size = sum(a.size * a.dtype.itemsize for a in (*args, *shapes))
    return pl.pallas_call(
        body,
        out_shape=shapes,
        compiler_params=pltpu.CompilerParams(vmem_limit_bytes=limit << 20),
        cost_estimate=pl.CostEstimate(flops=flops, bytes_accessed=size, transcendentals=0),
    )(*args)


def forward(
    halo, value, gate, upstream, taps, gain, mean, scale,
    padded, scaled, spread, hidden, message, gain_part,
    taps_wide, mean_columns, scale_columns, sum_first, sum_second,
):
    taps_wide[0:TAPS] = taps[...].astype(WIDE)
    for block in range(ROWS // LANES):
        rows = slice(block * LANES, (block + 1) * LANES)
        mean_columns[rows] = column(mean[rows].reshape(1, LANES))
        scale_columns[rows] = column(scale[rows].reshape(1, LANES))
    for half in range(HALVES):
        padded[half, 0:EDGE] = halo[:, lanes(half)].astype(WIDE)
        for start in range(0, ROWS, CHUNK):
            rows = slice(start, start + CHUNK)
            sig = jax.nn.sigmoid(gate[rows, lanes(half)].astype(WIDE))
            gated = (value[rows, lanes(half)].astype(WIDE) * sig).astype(NARROW)
            padded[half, EDGE + start : EDGE + start + CHUNK] = gated.astype(WIDE)
    for half in range(HALVES):
        gain_row = gain[0:1, lanes(half)]
        gain_sum = jnp.zeros((8, LANES), WIDE)
        for start in range(0, ROWS, CHUNK):
            rows = slice(start, start + CHUNK)
            conv = jnp.zeros((CHUNK, LANES), WIDE)
            for tap in range(TAPS):
                begin = start + tap + EDGE - TAPS + 1
                conv = conv + taps_wide[tap : tap + 1, lanes(half)] * padded[half, begin : begin + CHUNK]
            factor = scale_columns[rows]
            normed = (conv - mean_columns[rows]) * factor
            active = normed * gain_row
            sig = jax.nn.sigmoid(active)
            hidden[rows, lanes(half)] = (active * sig).astype(NARROW)
            d_active = upstream[rows, lanes(half)] * sig * (1.0 + active * (1.0 - sig))
            gain_sum = gain_sum + jnp.sum((d_active * normed).reshape(CHUNK // 8, 8, LANES), 0)
            d_normed = d_active * gain_row
            scaled[half, rows] = factor * d_normed
            spread[half, rows] = factor * normed
            weighted = d_normed * normed
            if half == 0:
                sum_first[rows] = d_normed
                sum_second[rows] = weighted
            else:
                sum_first[rows] = sum_first[rows] + d_normed
                sum_second[rows] = sum_second[rows] + weighted
        gain_part[half] = gain_sum
    found = []
    for source in (sum_first, sum_second):
        for block in range(ROWS // LANES):
            turned = jnp.transpose(source[block * LANES : (block + 1) * LANES])
            found.append(jnp.sum(turned, 0, keepdims=True))
    found.append(jnp.zeros((2, LANES), WIDE))
    message[...] = jnp.concatenate(found, 0)


def weight_product(core, cotangent, hidden, mine, other):
    first = core[0] == 0
    for far in range(FAR):
        part = lax.dot_general(
            cotangent[:, lanes(far)], hidden[...], (((0,), (0,)), ((), ())),
            preferred_element_type=WIDE,
        )
        part = part.reshape(CLOSE, 2, OWN, WIDTH)
        low, high = part[:, 0], part[:, 1]
        mine[:, far] = jnp.where(first, low, high)
        other[:, far] = jnp.where(first, high, low).astype(NARROW)


def halves(value):
    high = value.astype(NARROW)
    return high, (value - high.astype(WIDE)).astype(NARROW)


def backward(
    sums_0, sums_1, sums_2, sums_3, scaled, spread, padded, scale, gain_part, mine, other,
    pieces, extended,
    small,
):
    total = (sums_0[...] + sums_1[...]) + (sums_2[...] + sums_3[...])
    total = total * (1.0 / (TP * WIDTH))
    blocks = ROWS // LANES
    for half in range(HALVES):
        extended[half, 0:EDGE] = jnp.zeros((EDGE, LANES), WIDE)
        extended[half, EDGE + ROWS :] = jnp.zeros((EDGE, LANES), WIDE)
    for block in range(blocks):
        rows = slice(block * LANES, (block + 1) * LANES)
        first = column(total[block : block + 1] * scale[rows].reshape(1, LANES))
        second = column(total[blocks + block : blocks + block + 1])
        for half in range(HALVES):
            d_conv = scaled[half, rows] - first - spread[half, rows] * second
            extended[half, EDGE + block * LANES : EDGE + (block + 1) * LANES] = d_conv
    for half in range(HALVES):
        for group in range(0, TAPS, 8):
            members = range(group, min(group + 8, TAPS))
            found = [jnp.zeros((8, LANES), WIDE) for _ in members]
            for start in range(0, ROWS, 8):
                d_conv = extended[half, EDGE + start : EDGE + start + 8]
                for i, tap in enumerate(members):
                    begin = start + tap + EDGE - TAPS + 1
                    found[i] = found[i] + d_conv * padded[half, begin : begin + 8]
            for i, tap in enumerate(members):
                small[tap : tap + 1, lanes(half)] = jnp.sum(found[i], 0, keepdims=True)
        small[TAPS : TAPS + 1, lanes(half)] = jnp.sum(gain_part[half], 0, keepdims=True)
    for near in range(CLOSE):
        chip = mine[near] + other[near].astype(WIDE)
        pieces[near, 0 : FAR * OWN] = chip.reshape(FAR * OWN, WIDTH).astype(NARROW)
        high, low = halves(small[near * 4 : near * 4 + 4])
        pieces[near, FAR * OWN :] = jnp.concatenate([high.astype(WIDE), low.astype(WIDE)], 0).astype(NARROW)


def gated_gradient(extended, taps, d_gated, margin, taps_wide):
    taps_wide[0:TAPS] = taps[...].astype(WIDE)
    for half in range(HALVES):
        for start in range(0, EDGE + ROWS, EDGE):
            found = jnp.zeros((EDGE, LANES), WIDE)
            for tap in range(TAPS):
                begin = start + TAPS - 1 - tap
                found = found + taps_wide[tap : tap + 1, lanes(half)] * extended[half, begin : begin + EDGE]
            if start == 0:
                margin[half] = found
            else:
                d_gated[half, start - EDGE : start] = found


def outputs(d_gated, arrived, value, gate, value_grad, gate_grad):
    for half in range(HALVES):
        for start in range(0, ROWS, EDGE):
            rows = slice(start, start + EDGE)
            grad = d_gated[half, rows]
            if start == ROWS - EDGE:
                grad = grad + arrived[half]
            sig = jax.nn.sigmoid(gate[rows, lanes(half)].astype(WIDE))
            wide = value[rows, lanes(half)].astype(WIDE)
            value_grad[rows, lanes(half)] = (grad * sig).astype(NARROW)
            gate_grad[rows, lanes(half)] = (grad * wide * sig * (1.0 - sig)).astype(NARROW)


def fold_near(arrived, pieces):
    for far in range(FAR):
        rows = slice(far * OWN, (far + 1) * OWN)
        total = arrived[0, rows].astype(WIDE)
        for near in range(1, CLOSE):
            total = total + arrived[near, rows].astype(WIDE)
        pieces[FAR_ORDER.index(far), :, 0:WIDTH] = total.astype(NARROW)
    both = arrived[0, FAR * OWN :].astype(WIDE)
    for near in range(1, CLOSE):
        both = both + arrived[near, FAR * OWN :].astype(WIDE)
    small = both[0:4] + both[4:8]
    small = jnp.concatenate([small[:, lanes(0)], small[:, lanes(1)]], 0).astype(NARROW)
    for far in range(FAR):
        pieces[far, :, WIDTH:] = small


def fold_far(arrived, message):
    total = arrived[0, :, WIDTH:].astype(WIDE)
    for far in range(1, FAR):
        total = total + arrived[far, :, WIDTH:].astype(WIDE)
    for peer in range(CLOSE * 2):
        message[peer] = total


def finish(arrived, weights, taps_grad, gain_grad, weight_grad):
    total = weights[0, :, 0:WIDTH].astype(WIDE)
    for far in range(1, FAR):
        total = total + weights[far, :, 0:WIDTH].astype(WIDE)
    weight_grad[...] = total
    for near in range(CLOSE):
        total = arrived[2 * near] + arrived[2 * near + 1]
        total = jnp.concatenate([total[0:4], total[4:8]], 1)
        if near < CLOSE - 1:
            taps_grad[near * 4 : near * 4 + 4] = total
        else:
            taps_grad[near * 4 : near * 4 + 3] = total[0:3]
            gain_grad[...] = total[3:4]


def shards(
    proj_value, proj_gate, out_cotangent, out_weight, conv_taps, norm_gain, row_mean, row_scale
):
    end_gate = jax.nn.sigmoid(proj_gate[ROWS - EDGE :].astype(WIDE))
    end = (proj_value[ROWS - EDGE :].astype(WIDE) * end_gate).astype(NARROW)
    halo = shifted(end, SP, 1)
    split = (HALVES, ROWS, LANES)
    upstream = lax.dot_general(
        out_cotangent, out_weight, (((1,), (1,)), ((), ())), preferred_element_type=WIDE
    )
    column_scratch = [pltpu.VMEM((ROWS, LANES), WIDE)] * 4
    taps_scratch = pltpu.VMEM((TAPS + 1, WIDTH), WIDE)
    padded, scaled, spread, hidden, message, gain_part = call_with(
        forward,
        [
            ((HALVES, EDGE + ROWS, LANES), WIDE), (split, WIDE), (split, WIDE),
            ((ROWS, WIDTH), NARROW), ((8, LANES), WIDE), ((HALVES, 8, LANES), WIDE),
        ],
        [taps_scratch, *column_scratch],
        halo, proj_value, proj_gate, upstream, conv_taps, norm_gain.reshape(1, WIDTH), row_mean, row_scale,
        flops=100 * ROWS * WIDTH,
    )
    sums = [message]
    for step in range(1, TP):
        pairs = [(place, (place + step) % TP) for place in range(TP)]
        sums.append(lax.ppermute(message, "tp", pairs))
    core = lax.axis_index("c").reshape(1)
    grouped = (CLOSE, FAR, OWN, WIDTH)
    mine, other = weight_call(core, out_cotangent, hidden, [(grouped, WIDE), (grouped, NARROW)])
    other = lax.ppermute(other, "c", [(0, 1), (1, 0)])
    pieces, extended = call_with(
        backward,
        [((CLOSE, FAR * OWN + 8, WIDTH), NARROW), ((HALVES, ROWS + 2 * EDGE, LANES), WIDE)],
        [pltpu.VMEM((TAPS + 1, WIDTH), WIDE)],
        *sums, scaled, spread, padded, row_scale, gain_part, mine, other,
        flops=100 * ROWS * WIDTH,
    )
    (pieces,) = call(
        fold_near, [((FAR, OWN, WIDTH + LANES), NARROW)], exchange(pieces, NEAR), flops=1 << 20
    )
    arrived = exchange(pieces, "zh", FAR_ORDER)
    d_gated, margin = call_with(
        gated_gradient, [(split, WIDE), ((HALVES, EDGE, LANES), WIDE)], [taps_scratch],
        extended, conv_taps, flops=100 * ROWS * WIDTH,
    )
    late = shifted(margin, SP, -1)
    value_grad, gate_grad = call(
        outputs, [((ROWS, WIDTH), NARROW), ((ROWS, WIDTH), NARROW)],
        d_gated, late, proj_value, proj_gate, flops=10 * ROWS * WIDTH,
    )
    (message,) = call(
        fold_far, [((CLOSE * 2, 8, LANES), WIDE)], arrived, flops=1 << 16
    )
    taps_grad, gain_grad, weight_grad = call(
        finish, [((TAPS, WIDTH), WIDE), ((1, WIDTH), WIDE), ((OWN, WIDTH), WIDE)],
        exchange(message, (*NEAR, "c"), GATHER_ORDER), arrived, flops=1 << 16,
    )
    return (value_grad, gate_grad, weight_grad, taps_grad, gain_grad.reshape(WIDTH))


def call_with(body, outs, scratch, *args, flops=0, limit=6):
    shapes = [jax.ShapeDtypeStruct(shape, dtype) for shape, dtype in outs]
    size = sum(a.size * a.dtype.itemsize for a in (*args, *shapes))
    return pl.pallas_call(
        body,
        out_shape=shapes,
        scratch_shapes=scratch,
        compiler_params=pltpu.CompilerParams(vmem_limit_bytes=limit << 20),
        cost_estimate=pl.CostEstimate(flops=flops, bytes_accessed=size, transcendentals=0),
    )(*args)


def weight_call(core, cotangent, hidden, outs):
    whole = pl.BlockSpec(memory_space=pltpu.VMEM)
    return pl.pallas_call(
        weight_product,
        out_shape=[jax.ShapeDtypeStruct(shape, dtype) for shape, dtype in outs],
        in_specs=[pl.BlockSpec(memory_space=pltpu.SMEM), whole, whole],
        out_specs=[whole, whole],
        compiler_params=pltpu.CompilerParams(vmem_limit_bytes=6 << 20),
        cost_estimate=pl.CostEstimate(
            flops=2 * ROWS * WIDTH * MODEL, bytes_accessed=4 << 20, transcendentals=0
        ),
        name="weight_product",
    )(core, cotangent, hidden)


def solution(mesh):
    sizes = [size for _, size in AXES]
    split = Mesh(mesh.devices.reshape(*sizes, mesh.shape["tp"]), (*SP, "tp"))
    placed = (
        P(SP, "tp"),
        P(SP, "tp"),
        P(SP, None),
        P("tp", None),
        P(None, "tp"),
        P("tp"),
        P(SP),
        P(SP),
    )
    return jax.shard_map(
        shards,
        mesh=split,
        in_specs=placed,
        out_specs=(P(SP, "tp"), P(SP, "tp"), P(SP, "tp"), P(None, "tp"), P("tp")),
        check_vma=False,
    )
```

```python
import jax
import jax.numpy as jnp
from jax import lax
from jax.experimental import pallas as pl
from jax.experimental.pallas import tpu as pltpu
from jax.sharding import Mesh
from jax.sharding import PartitionSpec as P


SP = ("zh", "zl", "x", "c")
NEAR = ("zl", "x")
FAR = 16
CLOSE = 8
AXES = (("zh", FAR), ("zl", 2), ("x", 4), ("c", 2))
FAR_ORDER = [(place + 10) % FAR for place in range(FAR)]
TP = 4
PARTS = 4
TAPS = 31
ROWS = 384
EDGE = 32
LANES = 128
HALVES = 2
WIDTH = HALVES * LANES
MODEL = 2048
OWN = 8
CHUNK = 64
WIDE = jnp.float32
NARROW = jnp.bfloat16


def shifted(value, axis, steps):
    count = lax.axis_size(axis)
    first, last = (max(0, -steps), min(count, count - steps))
    return lax.ppermute(value, axis, [(source, source + steps) for source in range(first, last)])


def exchange(pieces, axes, order=None):
    groups = order and [order]
    return lax.all_to_all(pieces, axes, 0, 0, tiled=True, axis_index_groups=groups)


def lanes(half):
    return slice(half * LANES, (half + 1) * LANES)


def column(row):
    return jnp.transpose(jnp.broadcast_to(row, (LANES, LANES)))


def call(body, outs, *args, flops=0, limit=6):
    shapes = [jax.ShapeDtypeStruct(shape, dtype) for shape, dtype in outs]
    size = sum(a.size * a.dtype.itemsize for a in (*args, *shapes))
    return pl.pallas_call(
        body,
        out_shape=shapes,
        compiler_params=pltpu.CompilerParams(vmem_limit_bytes=limit << 20),
        cost_estimate=pl.CostEstimate(flops=flops, bytes_accessed=size, transcendentals=0),
    )(*args)


def norm_backward(conv, mean, factor, gain_row, upstream):
    normed = (conv - mean) * factor
    active = normed * gain_row
    sig = jax.nn.sigmoid(active)
    hidden = (active * sig).astype(NARROW)
    d_active = upstream * sig * (1.0 + active * (1.0 - sig))
    d_normed = d_active * gain_row
    gain_part = jnp.sum((d_active * normed).reshape(conv.shape[0] // 8, 8, LANES), 0)
    return hidden, factor * d_normed, factor * normed, d_normed, d_normed * normed, gain_part


def convolve(source, half, taps_wide, start, size):
    conv = jnp.zeros((size, LANES), WIDE)
    for tap in range(TAPS):
        begin = start + tap + EDGE - TAPS + 1
        conv = conv + taps_wide[tap : tap + 1, lanes(half)] * source[half, begin : begin + size]
    return conv


def column_sums(source):
    return jnp.sum(jnp.transpose(source), 0, keepdims=True)


def forward(
    value, gate, upstream, taps, gain, mean, scale,
    gated, scaled, spread, hidden, sums, gain_part,
    padded, taps_wide, mean_columns, scale_columns, sum_first, sum_second,
):
    taps_wide[0:TAPS] = taps[...].astype(WIDE)
    for block in range(ROWS // LANES):
        rows = slice(block * LANES, (block + 1) * LANES)
        mean_columns[rows] = column(mean[rows].reshape(1, LANES))
        scale_columns[rows] = column(scale[rows].reshape(1, LANES))
    for half in range(HALVES):
        for start in range(0, ROWS, CHUNK):
            rows = slice(start, start + CHUNK)
            sig = jax.nn.sigmoid(gate[rows, lanes(half)].astype(WIDE))
            product = (value[rows, lanes(half)].astype(WIDE) * sig).astype(NARROW)
            gated[rows, lanes(half)] = product
            padded[half, EDGE + start : EDGE + start + CHUNK] = product.astype(WIDE)
    sum_first[0:EDGE] = jnp.zeros((EDGE, LANES), WIDE)
    sum_second[0:EDGE] = jnp.zeros((EDGE, LANES), WIDE)
    for half in range(HALVES):
        gain_row = gain[0:1, lanes(half)]
        gain_sum = jnp.zeros((8, LANES), WIDE)
        for start in range(EDGE, ROWS, EDGE):
            rows = slice(start, start + EDGE)
            conv = convolve(padded, half, taps_wide, start, EDGE)
            narrow, own_scaled, own_spread, first, second, part = norm_backward(
                conv, mean_columns[rows], scale_columns[rows], gain_row, upstream[rows, lanes(half)]
            )
            hidden[start - EDGE : start, lanes(half)] = narrow
            scaled[half, start - EDGE : start] = own_scaled
            spread[half, start - EDGE : start] = own_spread
            gain_sum = gain_sum + part
            if half == 0:
                sum_first[rows] = first
                sum_second[rows] = second
            else:
                sum_first[rows] = sum_first[rows] + first
                sum_second[rows] = sum_second[rows] + second
        gain_part[half] = gain_sum
    found = [
        column_sums(source[block * LANES : (block + 1) * LANES])
        for source in (sum_first, sum_second)
        for block in range(ROWS // LANES)
    ]
    sums[...] = jnp.concatenate([*found, jnp.zeros((2, LANES), WIDE)], 0)


def head(
    halo, gated, upstream, taps, gain, mean, scale, sums, gain_part,
    scaled, spread, hidden, message, gain_total,
    padded, taps_wide, turned,
):
    taps_wide[0:TAPS] = taps[...].astype(WIDE)
    rows = slice(0, EDGE)
    mean_columns = column(mean[0:LANES].reshape(1, LANES))[rows]
    scale_columns = column(scale[0:LANES].reshape(1, LANES))[rows]
    turned[...] = jnp.zeros((2, LANES, LANES), WIDE)
    for half in range(HALVES):
        padded[half, rows] = halo[:, lanes(half)].astype(WIDE)
        padded[half, EDGE:] = gated[rows, lanes(half)].astype(WIDE)
    for half in range(HALVES):
        conv = convolve(padded, half, taps_wide, 0, EDGE)
        narrow, own_scaled, own_spread, first, second, part = norm_backward(
            conv, mean_columns, scale_columns, gain[0:1, lanes(half)], upstream[rows, lanes(half)]
        )
        hidden[:, lanes(half)] = narrow
        scaled[half] = own_scaled
        spread[half] = own_spread
        gain_total[half] = gain_part[half] + part
        turned[0, rows] = turned[0, rows] + first
        turned[1, rows] = turned[1, rows] + second
    blocks = ROWS // LANES
    total = sums[...]
    extra = [column_sums(turned[0]), column_sums(turned[1])]
    none = jnp.zeros((blocks - 1, LANES), WIDE)
    last = jnp.zeros((2, LANES), WIDE)
    total = total + jnp.concatenate([extra[0], none, extra[1], none, last], 0)
    for peer in range(TP):
        message[peer] = total


def weight_product(
    core, cotangent, hidden, first_hidden, mine, other, held, whole, kept, arrivals, departure
):
    copies = []
    for part in range(PARTS):
        columns = pl.ds(part * (MODEL // PARTS), MODEL // PARTS)
        copies.append(
            pltpu.make_async_copy(
                cotangent.at[:, columns], held.at[:, columns], arrivals.at[part]
            )
        )
        copies[-1].start()
    whole[0:EDGE] = first_hidden[...]
    whole[EDGE:] = hidden[...]
    first = core[0] == 0
    for far in range(FAR):
        if far % (FAR // PARTS) == 0:
            copies[far // (FAR // PARTS)].wait()
        part = lax.dot_general(
            held[:, lanes(far)], whole[...], (((0,), (0,)), ((), ())),
            preferred_element_type=WIDE,
        )
        part = part.reshape(CLOSE, 2, OWN, WIDTH)
        low, high = part[:, 0], part[:, 1]
        kept[:, far] = jnp.where(first, low, high)
        other[:, far] = jnp.where(first, high, low).astype(NARROW)
    leaving = pltpu.make_async_copy(kept, mine, departure)
    leaving.start()
    leaving.wait()


def halves(value):
    high = value.astype(NARROW)
    return high, (value - high.astype(WIDE)).astype(NARROW)


def backward(
    mine, other, sums, scaled, spread, first_scaled, first_spread, halo, gated, scale, gain_part,
    pieces, extended,
    small, padded, held_mine, held_other, arrivals,
):
    copies = [
        pltpu.make_async_copy(mine, held_mine, arrivals.at[0]),
        pltpu.make_async_copy(other, held_other, arrivals.at[1]),
    ]
    for copy in copies:
        copy.start()
    for half in range(HALVES):
        padded[half, 0:EDGE] = halo[:, lanes(half)].astype(WIDE)
        padded[half, EDGE:] = gated[:, lanes(half)].astype(WIDE)
    total = (sums[0] + sums[1]) + (sums[2] + sums[3])
    total = total * (1.0 / (TP * WIDTH))
    blocks = ROWS // LANES
    for half in range(HALVES):
        extended[half, 0:EDGE] = jnp.zeros((EDGE, LANES), WIDE)
        extended[half, EDGE + ROWS :] = jnp.zeros((EDGE, LANES), WIDE)
    for block in range(blocks):
        rows = slice(block * LANES, (block + 1) * LANES)
        first = column(total[block : block + 1] * scale[rows].reshape(1, LANES))
        second = column(total[blocks + block : blocks + block + 1])
        for half in range(HALVES):
            cut = 0
            if block == 0:
                cut = EDGE
                d_conv = first_scaled[half] - first[0:cut] - first_spread[half] * second[0:cut]
                extended[half, EDGE : EDGE + cut] = d_conv
            rows = slice(block * LANES + cut - EDGE, (block + 1) * LANES - EDGE)
            d_conv = scaled[half, rows] - first[cut:] - spread[half, rows] * second[cut:]
            extended[half, EDGE + block * LANES + cut : EDGE + (block + 1) * LANES] = d_conv
    lead = EDGE - TAPS + 1
    groups = ROWS // 8
    for offset in range(8):
        steps = [q for q in range(5) if 0 <= 8 * q + offset - lead < TAPS]
        found = {(half, q): jnp.zeros((8, LANES), WIDE) for half in range(HALVES) for q in steps}
        loaded = {}
        for m in range(groups + steps[-1]):
            for half in range(HALVES):
                if m < groups:
                    begin = EDGE + 8 * m
                    loaded[half, m] = extended[half, begin : begin + 8]
                moved = padded[half, 8 * m + offset : 8 * m + offset + 8]
                for q in steps:
                    if 0 <= m - q < groups:
                        found[half, q] = found[half, q] + loaded[half, m - q] * moved
        for half in range(HALVES):
            for q in steps:
                tap = 8 * q + offset - lead
                small[tap : tap + 1, lanes(half)] = jnp.sum(found[half, q], 0, keepdims=True)
    for half in range(HALVES):
        small[TAPS : TAPS + 1, lanes(half)] = jnp.sum(gain_part[half], 0, keepdims=True)
    for copy in copies:
        copy.wait()
    for near in range(CLOSE):
        chip = held_mine[near] + held_other[near].astype(WIDE)
        pieces[near, 0 : FAR * OWN] = chip.reshape(FAR * OWN, WIDTH).astype(NARROW)
        high, low = halves(small[near * 4 : near * 4 + 4])
        pieces[near, FAR * OWN :] = jnp.concatenate([high.astype(WIDE), low.astype(WIDE)], 0).astype(NARROW)


def gated_gradient(extended, taps, d_gated, margin, taps_wide):
    taps_wide[0:TAPS] = taps[...].astype(WIDE)
    for half in range(HALVES):
        for start in range(0, EDGE + ROWS, EDGE):
            found = jnp.zeros((EDGE, LANES), WIDE)
            for tap in range(TAPS):
                begin = start + TAPS - 1 - tap
                found = found + taps_wide[tap : tap + 1, lanes(half)] * extended[half, begin : begin + EDGE]
            if start == 0:
                margin[half] = found
            else:
                d_gated[half, start - EDGE : start] = found


def outputs(d_gated, arrived, value, gate, value_grad, gate_grad):
    for half in range(HALVES):
        for start in range(0, ROWS, EDGE):
            rows = slice(start, start + EDGE)
            grad = d_gated[half, rows]
            if start == ROWS - EDGE:
                grad = grad + arrived[half]
            sig = jax.nn.sigmoid(gate[rows, lanes(half)].astype(WIDE))
            wide = value[rows, lanes(half)].astype(WIDE)
            value_grad[rows, lanes(half)] = (grad * sig).astype(NARROW)
            gate_grad[rows, lanes(half)] = (grad * wide * sig * (1.0 - sig)).astype(NARROW)


def fold_near(arrived, pieces):
    for far in range(FAR):
        rows = slice(far * OWN, (far + 1) * OWN)
        total = arrived[0, rows].astype(WIDE)
        for near in range(1, CLOSE):
            total = total + arrived[near, rows].astype(WIDE)
        pieces[FAR_ORDER.index(far), :, 0:WIDTH] = total.astype(NARROW)
    both = arrived[0, FAR * OWN :].astype(WIDE)
    for near in range(1, CLOSE):
        both = both + arrived[near, FAR * OWN :].astype(WIDE)
    small = both[0:4] + both[4:8]
    small = jnp.concatenate([small[:, lanes(0)], small[:, lanes(1)]], 0).astype(NARROW)
    for far in range(FAR):
        pieces[far, :, WIDTH:] = small


def fold_far(arrived, message):
    total = arrived[0, :, WIDTH:].astype(WIDE)
    for far in range(1, FAR):
        total = total + arrived[far, :, WIDTH:].astype(WIDE)
    for peer in range(CLOSE * 2):
        message[peer] = total


def finish(arrived, weights, taps_grad, gain_grad, weight_grad):
    total = weights[0, :, 0:WIDTH].astype(WIDE)
    for far in range(1, FAR):
        total = total + weights[far, :, 0:WIDTH].astype(WIDE)
    weight_grad[...] = total
    for near in range(CLOSE):
        total = arrived[2 * near] + arrived[2 * near + 1]
        total = jnp.concatenate([total[0:4], total[4:8]], 1)
        if near < CLOSE - 1:
            taps_grad[near * 4 : near * 4 + 4] = total
        else:
            taps_grad[near * 4 : near * 4 + 3] = total[0:3]
            gain_grad[...] = total[3:4]


def shards(
    proj_value, proj_gate, out_cotangent, out_weight, conv_taps, norm_gain, row_mean, row_scale
):
    end_gate = jax.nn.sigmoid(proj_gate[ROWS - EDGE :].astype(WIDE))
    end = (proj_value[ROWS - EDGE :].astype(WIDE) * end_gate).astype(NARROW)
    halo = shifted(end, SP, 1)
    split = (HALVES, ROWS, LANES)
    upstream = lax.dot_general(
        out_cotangent, out_weight, (((1,), (1,)), ((), ())), preferred_element_type=WIDE
    )
    rest = (HALVES, ROWS - EDGE, LANES)
    row_gain = norm_gain.reshape(1, WIDTH)
    sides = pltpu.VMEM((HALVES, EDGE + ROWS, LANES), WIDE)
    taps_scratch = pltpu.VMEM((TAPS + 1, WIDTH), WIDE)
    gated, scaled, spread, hidden, sums, gain_part = call_with(
        forward,
        [
            ((ROWS, WIDTH), NARROW), (rest, WIDE), (rest, WIDE),
            ((ROWS - EDGE, WIDTH), NARROW), ((8, LANES), WIDE), ((HALVES, 8, LANES), WIDE),
        ],
        [sides, taps_scratch, *([pltpu.VMEM((ROWS, LANES), WIDE)] * 4)],
        proj_value, proj_gate, upstream, conv_taps, row_gain, row_mean, row_scale,
        flops=100 * ROWS * WIDTH,
    )
    edge = (HALVES, EDGE, LANES)
    first_scaled, first_spread, first_hidden, message, gain_part = call_with(
        head,
        [
            (edge, WIDE), (edge, WIDE), ((EDGE, WIDTH), NARROW),
            ((TP, 8, LANES), WIDE), ((HALVES, 8, LANES), WIDE),
        ],
        [
            pltpu.VMEM((HALVES, 2 * EDGE, LANES), WIDE),
            taps_scratch,
            pltpu.VMEM((2, LANES, LANES), WIDE),
        ],
        halo, gated, upstream, conv_taps, row_gain, row_mean, row_scale, sums, gain_part,
        flops=10 * ROWS * WIDTH,
    )
    sums = exchange(message, "tp")
    core = lax.axis_index("c").reshape(1)
    grouped = (CLOSE, FAR, OWN, WIDTH)
    mine, other = weight_call(core, out_cotangent, hidden, first_hidden, [(grouped, WIDE), (grouped, NARROW)])
    other = lax.ppermute(other, "c", [(0, 1), (1, 0)])
    pieces, extended = call_with(
        backward,
        [((CLOSE, FAR * OWN + 8, WIDTH), NARROW), ((HALVES, ROWS + 2 * EDGE, LANES), WIDE)],
        [
            taps_scratch, sides, pltpu.VMEM(grouped, WIDE), pltpu.VMEM(grouped, NARROW),
            pltpu.SemaphoreType.DMA((2,)),
        ],
        mine, other,
        sums, scaled, spread, first_scaled, first_spread, halo, gated, row_scale, gain_part,
        in_hbm=2,
        flops=100 * ROWS * WIDTH,
    )
    (pieces,) = call(
        fold_near, [((FAR, OWN, WIDTH + LANES), NARROW)], exchange(pieces, NEAR), flops=1 << 20
    )
    arrived = exchange(pieces, "zh", FAR_ORDER)
    d_gated, margin = call_with(
        gated_gradient, [(split, WIDE), ((HALVES, EDGE, LANES), WIDE)], [taps_scratch],
        extended, conv_taps, flops=100 * ROWS * WIDTH,
    )
    late = shifted(margin, SP, -1)
    value_grad, gate_grad = call(
        outputs, [((ROWS, WIDTH), NARROW), ((ROWS, WIDTH), NARROW)],
        d_gated, late, proj_value, proj_gate, flops=10 * ROWS * WIDTH,
    )
    (message,) = call(
        fold_far, [((CLOSE * 2, 8, LANES), WIDE)], arrived, flops=1 << 16
    )
    taps_grad, gain_grad, weight_grad = call(
        finish, [((TAPS, WIDTH), WIDE), ((1, WIDTH), WIDE), ((OWN, WIDTH), WIDE)],
        exchange(message, (*NEAR, "c")), arrived, flops=1 << 16,
    )
    return (value_grad, gate_grad, weight_grad, taps_grad, gain_grad.reshape(WIDTH))


def call_with(body, outs, scratch, *args, flops=0, limit=6, in_hbm=0):
    shapes = [jax.ShapeDtypeStruct(shape, dtype) for shape, dtype in outs]
    size = sum(a.size * a.dtype.itemsize for a in (*args, *shapes))
    far = [pltpu.with_memory_space_constraint(a, pltpu.HBM) for a in args[:in_hbm]]
    specs = [pl.BlockSpec(memory_space=pltpu.HBM)] * in_hbm
    specs += [pl.BlockSpec(memory_space=pltpu.VMEM)] * (len(args) - in_hbm)
    return pl.pallas_call(
        body,
        out_shape=shapes,
        in_specs=specs,
        scratch_shapes=scratch,
        compiler_params=pltpu.CompilerParams(vmem_limit_bytes=limit << 20),
        cost_estimate=pl.CostEstimate(flops=flops, bytes_accessed=size, transcendentals=0),
    )(*far, *args[in_hbm:])


def weight_call(core, cotangent, hidden, first_hidden, outs):
    whole = pl.BlockSpec(memory_space=pltpu.VMEM)
    cotangent = pltpu.with_memory_space_constraint(cotangent, pltpu.HBM)
    return pl.pallas_call(
        weight_product,
        out_shape=[pltpu.HBM(*outs[0]), jax.ShapeDtypeStruct(*outs[1])],
        in_specs=[
            pl.BlockSpec(memory_space=pltpu.SMEM),
            pl.BlockSpec(memory_space=pltpu.HBM),
            whole,
            whole,
        ],
        out_specs=[pl.BlockSpec(memory_space=pltpu.HBM), whole],
        scratch_shapes=[
            pltpu.VMEM((ROWS, MODEL), NARROW),
            pltpu.VMEM((ROWS, WIDTH), NARROW),
            pltpu.VMEM(*outs[0]),
            pltpu.SemaphoreType.DMA((PARTS,)),
            pltpu.SemaphoreType.DMA,
        ],
        compiler_params=pltpu.CompilerParams(vmem_limit_bytes=6 << 20),
        cost_estimate=pl.CostEstimate(
            flops=2 * ROWS * WIDTH * MODEL, bytes_accessed=4 << 20, transcendentals=0
        ),
        name="weight_product",
    )(core, cotangent, hidden, first_hidden)


def solution(mesh):
    sizes = [size for _, size in AXES]
    split = Mesh(mesh.devices.reshape(*sizes, mesh.shape["tp"]), (*SP, "tp"))
    placed = (
        P(SP, "tp"),
        P(SP, "tp"),
        P(SP, None),
        P("tp", None),
        P(None, "tp"),
        P("tp"),
        P(SP),
        P(SP),
    )
    return jax.shard_map(
        shards,
        mesh=split,
        in_specs=placed,
        out_specs=(P(SP, "tp"), P(SP, "tp"), P(SP, "tp"), P(None, "tp"), P("tp")),
        check_vma=False,
    )
```

```python
import jax
import jax.numpy as jnp
from jax import lax
from jax.experimental import pallas as pl
from jax.experimental.pallas import tpu as pltpu
from jax.sharding import Mesh
from jax.sharding import PartitionSpec as P


SP = ("zh", "zl", "x", "c")
NEAR = ("zl", "x")
FAR = 16
CLOSE = 8
AXES = (("zh", FAR), ("zl", 2), ("x", 4), ("c", 2))
FAR_ORDER = [(place + 10) % FAR for place in range(FAR)]
TP = 4
TAPS = 31
ROWS = 384
EDGE = 32
LANES = 128
HALVES = 2
WIDTH = HALVES * LANES
MODEL = 2048
OWN = 8
CHUNK = 64
WIDE = jnp.float32
NARROW = jnp.bfloat16


def shifted(value, axis, steps):
    count = lax.axis_size(axis)
    first, last = (max(0, -steps), min(count, count - steps))
    return lax.ppermute(value, axis, [(source, source + steps) for source in range(first, last)])


def exchange(pieces, axes, order=None):
    groups = order and [order]
    return lax.all_to_all(pieces, axes, 0, 0, tiled=True, axis_index_groups=groups)


def lanes(half):
    return slice(half * LANES, (half + 1) * LANES)


def column(row):
    return jnp.transpose(jnp.broadcast_to(row, (LANES, LANES)))


def call(body, outs, *args, flops=0, limit=6):
    shapes = [jax.ShapeDtypeStruct(shape, dtype) for shape, dtype in outs]
    size = sum(a.size * a.dtype.itemsize for a in (*args, *shapes))
    return pl.pallas_call(
        body,
        out_shape=shapes,
        compiler_params=pltpu.CompilerParams(vmem_limit_bytes=limit << 20),
        cost_estimate=pl.CostEstimate(flops=flops, bytes_accessed=size, transcendentals=0),
    )(*args)


def norm_backward(conv, mean, factor, gain_row, upstream):
    normed = (conv - mean) * factor
    active = normed * gain_row
    sig = jax.nn.sigmoid(active)
    hidden = (active * sig).astype(NARROW)
    d_active = upstream * sig * (1.0 + active * (1.0 - sig))
    d_normed = d_active * gain_row
    gain_part = jnp.sum((d_active * normed).reshape(conv.shape[0] // 8, 8, LANES), 0)
    return hidden, factor * d_normed, factor * normed, d_normed, d_normed * normed, gain_part


def convolve(source, half, taps_wide, start, size):
    conv = jnp.zeros((size, LANES), WIDE)
    for tap in range(TAPS):
        begin = start + tap + EDGE - TAPS + 1
        conv = conv + taps_wide[tap : tap + 1, lanes(half)] * source[half, begin : begin + size]
    return conv


def column_sums(source):
    return jnp.sum(jnp.transpose(source), 0, keepdims=True)


def forward(
    value, gate, upstream, taps, gain, mean, scale,
    gated, scaled, spread, hidden, sums, gain_part,
    padded, taps_wide, mean_columns, scale_columns, sum_first, sum_second,
):
    taps_wide[0:TAPS] = taps[...].astype(WIDE)
    for block in range(ROWS // LANES):
        rows = slice(block * LANES, (block + 1) * LANES)
        mean_columns[rows] = column(mean[rows].reshape(1, LANES))
        scale_columns[rows] = column(scale[rows].reshape(1, LANES))
    for half in range(HALVES):
        for start in range(0, ROWS, CHUNK):
            rows = slice(start, start + CHUNK)
            sig = jax.nn.sigmoid(gate[rows, lanes(half)].astype(WIDE))
            product = (value[rows, lanes(half)].astype(WIDE) * sig).astype(NARROW)
            gated[rows, lanes(half)] = product
            padded[half, EDGE + start : EDGE + start + CHUNK] = product.astype(WIDE)
    sum_first[0:EDGE] = jnp.zeros((EDGE, LANES), WIDE)
    sum_second[0:EDGE] = jnp.zeros((EDGE, LANES), WIDE)
    for half in range(HALVES):
        gain_row = gain[0:1, lanes(half)]
        gain_sum = jnp.zeros((8, LANES), WIDE)
        for start in range(EDGE, ROWS, EDGE):
            rows = slice(start, start + EDGE)
            conv = convolve(padded, half, taps_wide, start, EDGE)
            narrow, own_scaled, own_spread, first, second, part = norm_backward(
                conv, mean_columns[rows], scale_columns[rows], gain_row, upstream[rows, lanes(half)]
            )
            hidden[start - EDGE : start, lanes(half)] = narrow
            scaled[half, start - EDGE : start] = own_scaled
            spread[half, start - EDGE : start] = own_spread
            gain_sum = gain_sum + part
            if half == 0:
                sum_first[rows] = first
                sum_second[rows] = second
            else:
                sum_first[rows] = sum_first[rows] + first
                sum_second[rows] = sum_second[rows] + second
        gain_part[half] = gain_sum
    found = [
        column_sums(source[block * LANES : (block + 1) * LANES])
        for source in (sum_first, sum_second)
        for block in range(ROWS // LANES)
    ]
    sums[...] = jnp.concatenate([*found, jnp.zeros((2, LANES), WIDE)], 0)


def head(
    halo, gated, upstream, taps, gain, mean, scale, sums, gain_part,
    scaled, spread, hidden, message, gain_total,
    padded, taps_wide, turned,
):
    taps_wide[0:TAPS] = taps[...].astype(WIDE)
    rows = slice(0, EDGE)
    mean_columns = column(mean[0:LANES].reshape(1, LANES))[rows]
    scale_columns = column(scale[0:LANES].reshape(1, LANES))[rows]
    turned[...] = jnp.zeros((2, LANES, LANES), WIDE)
    for half in range(HALVES):
        padded[half, rows] = halo[:, lanes(half)].astype(WIDE)
        padded[half, EDGE:] = gated[rows, lanes(half)].astype(WIDE)
    for half in range(HALVES):
        conv = convolve(padded, half, taps_wide, 0, EDGE)
        narrow, own_scaled, own_spread, first, second, part = norm_backward(
            conv, mean_columns, scale_columns, gain[0:1, lanes(half)], upstream[rows, lanes(half)]
        )
        hidden[:, lanes(half)] = narrow
        scaled[half] = own_scaled
        spread[half] = own_spread
        gain_total[half] = gain_part[half] + part
        turned[0, rows] = turned[0, rows] + first
        turned[1, rows] = turned[1, rows] + second
    blocks = ROWS // LANES
    total = sums[...]
    extra = [column_sums(turned[0]), column_sums(turned[1])]
    none = jnp.zeros((blocks - 1, LANES), WIDE)
    last = jnp.zeros((2, LANES), WIDE)
    total = total + jnp.concatenate([extra[0], none, extra[1], none, last], 0)
    for peer in range(TP):
        message[peer] = total


def weight_product(core, cotangent, hidden, first_hidden, mine, other, whole):
    whole[0:EDGE] = first_hidden[...]
    whole[EDGE:] = hidden[...]
    first = core[0] == 0
    for far in range(FAR):
        part = lax.dot_general(
            cotangent[:, lanes(far)], whole[...], (((0,), (0,)), ((), ())),
            preferred_element_type=WIDE,
        )
        part = part.reshape(CLOSE, 2, OWN, WIDTH)
        low, high = part[:, 0], part[:, 1]
        mine[:, far] = jnp.where(first, low, high)
        other[:, far] = jnp.where(first, high, low).astype(NARROW)


def halves(value):
    high = value.astype(NARROW)
    return high, (value - high.astype(WIDE)).astype(NARROW)


def backward(
    sums, scaled, spread, first_scaled, first_spread, halo, gated, scale, gain_part, mine, other,
    pieces, extended,
    small, padded,
):
    for half in range(HALVES):
        padded[half, 0:EDGE] = halo[:, lanes(half)].astype(WIDE)
        padded[half, EDGE:] = gated[:, lanes(half)].astype(WIDE)
    total = (sums[0] + sums[1]) + (sums[2] + sums[3])
    total = total * (1.0 / (TP * WIDTH))
    blocks = ROWS // LANES
    for half in range(HALVES):
        extended[half, 0:EDGE] = jnp.zeros((EDGE, LANES), WIDE)
        extended[half, EDGE + ROWS :] = jnp.zeros((EDGE, LANES), WIDE)
    for block in range(blocks):
        rows = slice(block * LANES, (block + 1) * LANES)
        first = column(total[block : block + 1] * scale[rows].reshape(1, LANES))
        second = column(total[blocks + block : blocks + block + 1])
        for half in range(HALVES):
            cut = 0
            if block == 0:
                cut = EDGE
                d_conv = first_scaled[half] - first[0:cut] - first_spread[half] * second[0:cut]
                extended[half, EDGE : EDGE + cut] = d_conv
            rows = slice(block * LANES + cut - EDGE, (block + 1) * LANES - EDGE)
            d_conv = scaled[half, rows] - first[cut:] - spread[half, rows] * second[cut:]
            extended[half, EDGE + block * LANES + cut : EDGE + (block + 1) * LANES] = d_conv
    lead = EDGE - TAPS + 1
    groups = ROWS // 8
    for offset in range(8):
        steps = [q for q in range(5) if 0 <= 8 * q + offset - lead < TAPS]
        found = {(half, q): jnp.zeros((8, LANES), WIDE) for half in range(HALVES) for q in steps}
        loaded = {}
        for m in range(groups + steps[-1]):
            for half in range(HALVES):
                if m < groups:
                    begin = EDGE + 8 * m
                    loaded[half, m] = extended[half, begin : begin + 8]
                moved = padded[half, 8 * m + offset : 8 * m + offset + 8]
                for q in steps:
                    if 0 <= m - q < groups:
                        found[half, q] = found[half, q] + loaded[half, m - q] * moved
        for half in range(HALVES):
            for q in steps:
                tap = 8 * q + offset - lead
                small[tap : tap + 1, lanes(half)] = jnp.sum(found[half, q], 0, keepdims=True)
    for half in range(HALVES):
        small[TAPS : TAPS + 1, lanes(half)] = jnp.sum(gain_part[half], 0, keepdims=True)
    for near in range(CLOSE):
        chip = mine[near] + other[near].astype(WIDE)
        pieces[near, 0 : FAR * OWN] = chip.reshape(FAR * OWN, WIDTH).astype(NARROW)
        high, low = halves(small[near * 4 : near * 4 + 4])
        pieces[near, FAR * OWN :] = jnp.concatenate([high.astype(WIDE), low.astype(WIDE)], 0).astype(NARROW)


def gated_gradient(extended, taps, d_gated, margin, taps_wide):
    taps_wide[0:TAPS] = taps[...].astype(WIDE)
    for half in range(HALVES):
        for start in range(0, EDGE + ROWS, EDGE):
            found = jnp.zeros((EDGE, LANES), WIDE)
            for tap in range(TAPS):
                begin = start + TAPS - 1 - tap
                found = found + taps_wide[tap : tap + 1, lanes(half)] * extended[half, begin : begin + EDGE]
            if start == 0:
                margin[half] = found
            else:
                d_gated[half, start - EDGE : start] = found


def outputs(d_gated, arrived, value, gate, value_grad, gate_grad):
    for half in range(HALVES):
        for start in range(0, ROWS, EDGE):
            rows = slice(start, start + EDGE)
            grad = d_gated[half, rows]
            if start == ROWS - EDGE:
                grad = grad + arrived[half]
            sig = jax.nn.sigmoid(gate[rows, lanes(half)].astype(WIDE))
            wide = value[rows, lanes(half)].astype(WIDE)
            value_grad[rows, lanes(half)] = (grad * sig).astype(NARROW)
            gate_grad[rows, lanes(half)] = (grad * wide * sig * (1.0 - sig)).astype(NARROW)


def fold_near(arrived, pieces):
    for far in range(FAR):
        rows = slice(far * OWN, (far + 1) * OWN)
        total = arrived[0, rows].astype(WIDE)
        for near in range(1, CLOSE):
            total = total + arrived[near, rows].astype(WIDE)
        pieces[FAR_ORDER.index(far), :, 0:WIDTH] = total.astype(NARROW)
    both = arrived[0, FAR * OWN :].astype(WIDE)
    for near in range(1, CLOSE):
        both = both + arrived[near, FAR * OWN :].astype(WIDE)
    small = both[0:4] + both[4:8]
    small = jnp.concatenate([small[:, lanes(0)], small[:, lanes(1)]], 0).astype(NARROW)
    for far in range(FAR):
        pieces[far, :, WIDTH:] = small


def fold_far(arrived, message):
    total = arrived[0, :, WIDTH:].astype(WIDE)
    for far in range(1, FAR):
        total = total + arrived[far, :, WIDTH:].astype(WIDE)
    for peer in range(CLOSE * 2):
        message[peer] = total


def finish(arrived, weights, taps_grad, gain_grad, weight_grad):
    total = weights[0, :, 0:WIDTH].astype(WIDE)
    for far in range(1, FAR):
        total = total + weights[far, :, 0:WIDTH].astype(WIDE)
    weight_grad[...] = total
    for near in range(CLOSE):
        total = arrived[2 * near] + arrived[2 * near + 1]
        total = jnp.concatenate([total[0:4], total[4:8]], 1)
        if near < CLOSE - 1:
            taps_grad[near * 4 : near * 4 + 4] = total
        else:
            taps_grad[near * 4 : near * 4 + 3] = total[0:3]
            gain_grad[...] = total[3:4]


def shards(
    proj_value, proj_gate, out_cotangent, out_weight, conv_taps, norm_gain, row_mean, row_scale
):
    end_gate = jax.nn.sigmoid(proj_gate[ROWS - EDGE :].astype(WIDE))
    end = (proj_value[ROWS - EDGE :].astype(WIDE) * end_gate).astype(NARROW)
    halo = shifted(end, SP, 1)
    split = (HALVES, ROWS, LANES)
    upstream = lax.dot_general(
        out_cotangent, out_weight, (((1,), (1,)), ((), ())), preferred_element_type=WIDE
    )
    rest = (HALVES, ROWS - EDGE, LANES)
    row_gain = norm_gain.reshape(1, WIDTH)
    sides = pltpu.VMEM((HALVES, EDGE + ROWS, LANES), WIDE)
    taps_scratch = pltpu.VMEM((TAPS + 1, WIDTH), WIDE)
    gated, scaled, spread, hidden, sums, gain_part = call_with(
        forward,
        [
            ((ROWS, WIDTH), NARROW), (rest, WIDE), (rest, WIDE),
            ((ROWS - EDGE, WIDTH), NARROW), ((8, LANES), WIDE), ((HALVES, 8, LANES), WIDE),
        ],
        [sides, taps_scratch, *([pltpu.VMEM((ROWS, LANES), WIDE)] * 4)],
        proj_value, proj_gate, upstream, conv_taps, row_gain, row_mean, row_scale,
        flops=100 * ROWS * WIDTH,
    )
    edge = (HALVES, EDGE, LANES)
    first_scaled, first_spread, first_hidden, message, gain_part = call_with(
        head,
        [
            (edge, WIDE), (edge, WIDE), ((EDGE, WIDTH), NARROW),
            ((TP, 8, LANES), WIDE), ((HALVES, 8, LANES), WIDE),
        ],
        [
            pltpu.VMEM((HALVES, 2 * EDGE, LANES), WIDE),
            taps_scratch,
            pltpu.VMEM((2, LANES, LANES), WIDE),
        ],
        halo, gated, upstream, conv_taps, row_gain, row_mean, row_scale, sums, gain_part,
        flops=10 * ROWS * WIDTH,
    )
    sums = exchange(message, "tp")
    core = lax.axis_index("c").reshape(1)
    grouped = (CLOSE, FAR, OWN, WIDTH)
    mine, other = weight_call(core, out_cotangent, hidden, first_hidden, [(grouped, WIDE), (grouped, NARROW)])
    other = lax.ppermute(other, "c", [(0, 1), (1, 0)])
    pieces, extended = call_with(
        backward,
        [((CLOSE, FAR * OWN + 8, WIDTH), NARROW), ((HALVES, ROWS + 2 * EDGE, LANES), WIDE)],
        [taps_scratch, sides],
        sums, scaled, spread, first_scaled, first_spread, halo, gated, row_scale, gain_part,
        mine, other,
        flops=100 * ROWS * WIDTH,
    )
    (pieces,) = call(
        fold_near, [((FAR, OWN, WIDTH + LANES), NARROW)], exchange(pieces, NEAR), flops=1 << 20
    )
    arrived = exchange(pieces, "zh", FAR_ORDER)
    d_gated, margin = call_with(
        gated_gradient, [(split, WIDE), ((HALVES, EDGE, LANES), WIDE)], [taps_scratch],
        extended, conv_taps, flops=100 * ROWS * WIDTH,
    )
    late = shifted(margin, SP, -1)
    value_grad, gate_grad = call(
        outputs, [((ROWS, WIDTH), NARROW), ((ROWS, WIDTH), NARROW)],
        d_gated, late, proj_value, proj_gate, flops=10 * ROWS * WIDTH,
    )
    (message,) = call(
        fold_far, [((CLOSE * 2, 8, LANES), WIDE)], arrived, flops=1 << 16
    )
    taps_grad, gain_grad, weight_grad = call(
        finish, [((TAPS, WIDTH), WIDE), ((1, WIDTH), WIDE), ((OWN, WIDTH), WIDE)],
        exchange(message, (*NEAR, "c")), arrived, flops=1 << 16,
    )
    return (value_grad, gate_grad, weight_grad, taps_grad, gain_grad.reshape(WIDTH))


def call_with(body, outs, scratch, *args, flops=0, limit=6):
    shapes = [jax.ShapeDtypeStruct(shape, dtype) for shape, dtype in outs]
    size = sum(a.size * a.dtype.itemsize for a in (*args, *shapes))
    return pl.pallas_call(
        body,
        out_shape=shapes,
        scratch_shapes=scratch,
        compiler_params=pltpu.CompilerParams(vmem_limit_bytes=limit << 20),
        cost_estimate=pl.CostEstimate(flops=flops, bytes_accessed=size, transcendentals=0),
    )(*args)


def weight_call(core, cotangent, hidden, first_hidden, outs):
    whole = pl.BlockSpec(memory_space=pltpu.VMEM)
    return pl.pallas_call(
        weight_product,
        out_shape=[jax.ShapeDtypeStruct(shape, dtype) for shape, dtype in outs],
        in_specs=[pl.BlockSpec(memory_space=pltpu.SMEM), whole, whole, whole],
        out_specs=[whole, whole],
        scratch_shapes=[pltpu.VMEM((ROWS, WIDTH), NARROW)],
        compiler_params=pltpu.CompilerParams(vmem_limit_bytes=6 << 20),
        cost_estimate=pl.CostEstimate(
            flops=2 * ROWS * WIDTH * MODEL, bytes_accessed=4 << 20, transcendentals=0
        ),
        name="weight_product",
    )(core, cotangent, hidden, first_hidden)


def solution(mesh):
    sizes = [size for _, size in AXES]
    split = Mesh(mesh.devices.reshape(*sizes, mesh.shape["tp"]), (*SP, "tp"))
    placed = (
        P(SP, "tp"),
        P(SP, "tp"),
        P(SP, None),
        P("tp", None),
        P(None, "tp"),
        P("tp"),
        P(SP),
        P(SP),
    )
    return jax.shard_map(
        shards,
        mesh=split,
        in_specs=placed,
        out_specs=(P(SP, "tp"), P(SP, "tp"), P(SP, "tp"), P(None, "tp"), P("tp")),
        check_vma=False,
    )
```

```python
import jax
import jax.numpy as jnp
from jax import lax
from jax.experimental import pallas as pl
from jax.experimental.pallas import tpu as pltpu
from jax.sharding import Mesh
from jax.sharding import PartitionSpec as P


SP = ("zh", "zl", "x", "c")
NEAR = ("zl", "x")
FAR = 16
CLOSE = 8
AXES = (("zh", FAR), ("zl", 2), ("x", 4), ("c", 2))
TP = 4
BLOCK = CLOSE * 8
GATHER_ORDER = [(place + 1) % (2 * CLOSE) for place in range(2 * CLOSE)]
TAPS = 31
ROWS = 384
EDGE = 32
LANES = 128
HALVES = 2
WIDTH = HALVES * LANES
MODEL = 2048
OWN = 8
CHUNK = 64
WIDE = jnp.float32
NARROW = jnp.bfloat16


def shifted(value, axis, steps):
    count = lax.axis_size(axis)
    first, last = (max(0, -steps), min(count, count - steps))
    return lax.ppermute(value, axis, [(source, source + steps) for source in range(first, last)])


def exchange(pieces, axes, order=None):
    groups = order and [order]
    return lax.all_to_all(pieces, axes, 0, 0, tiled=True, axis_index_groups=groups)


def lanes(half):
    return slice(half * LANES, (half + 1) * LANES)


def column(row):
    return jnp.transpose(jnp.broadcast_to(row, (LANES, LANES)))


def call(body, outs, *args, flops=0, limit=6):
    shapes = [jax.ShapeDtypeStruct(shape, dtype) for shape, dtype in outs]
    size = sum(a.size * a.dtype.itemsize for a in (*args, *shapes))
    return pl.pallas_call(
        body,
        out_shape=shapes,
        compiler_params=pltpu.CompilerParams(vmem_limit_bytes=limit << 20),
        cost_estimate=pl.CostEstimate(flops=flops, bytes_accessed=size, transcendentals=0),
    )(*args)


def norm_backward(conv, mean, factor, gain_row, upstream):
    normed = (conv - mean) * factor
    active = normed * gain_row
    sig = jax.nn.sigmoid(active)
    hidden = (active * sig).astype(NARROW)
    d_active = upstream * sig * (1.0 + active * (1.0 - sig))
    d_normed = d_active * gain_row
    gain_part = jnp.sum((d_active * normed).reshape(conv.shape[0] // 8, 8, LANES), 0)
    return hidden, factor * d_normed, factor * normed, d_normed, d_normed * normed, gain_part


def convolve(source, half, taps_wide, start, size):
    conv = jnp.zeros((size, LANES), WIDE)
    for tap in range(TAPS):
        begin = start + tap + EDGE - TAPS + 1
        conv = conv + taps_wide[tap : tap + 1, lanes(half)] * source[half, begin : begin + size]
    return conv


def column_sums(source):
    return jnp.sum(jnp.transpose(source), 0, keepdims=True)


def forward(
    value, gate, upstream, taps, gain, mean, scale,
    gated, scaled, spread, hidden, sums, gain_part,
    padded, taps_wide, mean_columns, scale_columns, sum_first, sum_second,
):
    taps_wide[0:TAPS] = taps[...].astype(WIDE)
    for block in range(ROWS // LANES):
        rows = slice(block * LANES, (block + 1) * LANES)
        mean_columns[rows] = column(mean[rows].reshape(1, LANES))
        scale_columns[rows] = column(scale[rows].reshape(1, LANES))
    for half in range(HALVES):
        for start in range(0, ROWS, CHUNK):
            rows = slice(start, start + CHUNK)
            sig = jax.nn.sigmoid(gate[rows, lanes(half)].astype(WIDE))
            product = (value[rows, lanes(half)].astype(WIDE) * sig).astype(NARROW)
            gated[rows, lanes(half)] = product
            padded[half, EDGE + start : EDGE + start + CHUNK] = product.astype(WIDE)
    sum_first[0:EDGE] = jnp.zeros((EDGE, LANES), WIDE)
    sum_second[0:EDGE] = jnp.zeros((EDGE, LANES), WIDE)
    for half in range(HALVES):
        gain_row = gain[0:1, lanes(half)]
        gain_sum = jnp.zeros((8, LANES), WIDE)
        for start in range(EDGE, ROWS, EDGE):
            rows = slice(start, start + EDGE)
            conv = convolve(padded, half, taps_wide, start, EDGE)
            narrow, own_scaled, own_spread, first, second, part = norm_backward(
                conv, mean_columns[rows], scale_columns[rows], gain_row, upstream[rows, lanes(half)]
            )
            hidden[start - EDGE : start, lanes(half)] = narrow
            scaled[half, start - EDGE : start] = own_scaled
            spread[half, start - EDGE : start] = own_spread
            gain_sum = gain_sum + part
            if half == 0:
                sum_first[rows] = first
                sum_second[rows] = second
            else:
                sum_first[rows] = sum_first[rows] + first
                sum_second[rows] = sum_second[rows] + second
        gain_part[half] = gain_sum
    found = [
        column_sums(source[block * LANES : (block + 1) * LANES])
        for source in (sum_first, sum_second)
        for block in range(ROWS // LANES)
    ]
    sums[...] = jnp.concatenate([*found, jnp.zeros((2, LANES), WIDE)], 0)


def head(
    halo, gated, upstream, taps, gain, mean, scale, sums, gain_part,
    scaled, spread, hidden, message, gain_total,
    padded, taps_wide, turned,
):
    taps_wide[0:TAPS] = taps[...].astype(WIDE)
    rows = slice(0, EDGE)
    mean_columns = column(mean[0:LANES].reshape(1, LANES))[rows]
    scale_columns = column(scale[0:LANES].reshape(1, LANES))[rows]
    turned[...] = jnp.zeros((2, LANES, LANES), WIDE)
    for half in range(HALVES):
        padded[half, rows] = halo[:, lanes(half)].astype(WIDE)
        padded[half, EDGE:] = gated[rows, lanes(half)].astype(WIDE)
    for half in range(HALVES):
        conv = convolve(padded, half, taps_wide, 0, EDGE)
        narrow, own_scaled, own_spread, first, second, part = norm_backward(
            conv, mean_columns, scale_columns, gain[0:1, lanes(half)], upstream[rows, lanes(half)]
        )
        hidden[:, lanes(half)] = narrow
        scaled[half] = own_scaled
        spread[half] = own_spread
        gain_total[half] = gain_part[half] + part
        turned[0, rows] = turned[0, rows] + first
        turned[1, rows] = turned[1, rows] + second
    blocks = ROWS // LANES
    total = sums[...]
    extra = [column_sums(turned[0]), column_sums(turned[1])]
    none = jnp.zeros((blocks - 1, LANES), WIDE)
    last = jnp.zeros((2, LANES), WIDE)
    total = total + jnp.concatenate([extra[0], none, extra[1], none, last], 0)
    for peer in range(TP):
        message[peer] = total


def weight_product(place, cotangent, hidden, first_hidden, mine, other, whole):
    whole[0:EDGE] = first_hidden[...]
    whole[EDGE:] = hidden[...]
    first = place[0] % 2 == 0
    for far in range(FAR):
        part = lax.dot_general(
            cotangent[:, lanes(far)], whole[...], (((0,), (0,)), ((), ())),
            preferred_element_type=WIDE,
        )
        part = part.reshape(CLOSE, 2, OWN, WIDTH)
        low = part[:, 0].reshape(CLOSE * OWN, WIDTH)
        high = part[:, 1].reshape(CLOSE * OWN, WIDTH)
        mine[far] = jnp.where(first, low, high)
        other[far] = jnp.where(first, high, low).astype(NARROW)


def backward(
    place, sums, scaled, spread, first_scaled, first_spread, halo, gated, scale, gain_part, mine, other,
    pieces, extended,
    small, padded,
):
    for half in range(HALVES):
        padded[half, 0:EDGE] = halo[:, lanes(half)].astype(WIDE)
        padded[half, EDGE:] = gated[:, lanes(half)].astype(WIDE)
    total = (sums[0] + sums[1]) + (sums[2] + sums[3])
    total = total * (1.0 / (TP * WIDTH))
    blocks = ROWS // LANES
    for half in range(HALVES):
        extended[half, 0:EDGE] = jnp.zeros((EDGE, LANES), WIDE)
        extended[half, EDGE + ROWS :] = jnp.zeros((EDGE, LANES), WIDE)
    for block in range(blocks):
        rows = slice(block * LANES, (block + 1) * LANES)
        first = column(total[block : block + 1] * scale[rows].reshape(1, LANES))
        second = column(total[blocks + block : blocks + block + 1])
        for half in range(HALVES):
            cut = 0
            if block == 0:
                cut = EDGE
                d_conv = first_scaled[half] - first[0:cut] - first_spread[half] * second[0:cut]
                extended[half, EDGE : EDGE + cut] = d_conv
            rows = slice(block * LANES + cut - EDGE, (block + 1) * LANES - EDGE)
            d_conv = scaled[half, rows] - first[cut:] - spread[half, rows] * second[cut:]
            extended[half, EDGE + block * LANES + cut : EDGE + (block + 1) * LANES] = d_conv
    lead = EDGE - TAPS + 1
    groups = ROWS // 8
    for offset in range(8):
        steps = [q for q in range(5) if 0 <= 8 * q + offset - lead < TAPS]
        found = {(half, q): jnp.zeros((8, LANES), WIDE) for half in range(HALVES) for q in steps}
        loaded = {}
        for m in range(groups + steps[-1]):
            for half in range(HALVES):
                if m < groups:
                    begin = EDGE + 8 * m
                    loaded[half, m] = extended[half, begin : begin + 8]
                moved = padded[half, 8 * m + offset : 8 * m + offset + 8]
                for q in steps:
                    if 0 <= m - q < groups:
                        found[half, q] = found[half, q] + loaded[half, m - q] * moved
        for half in range(HALVES):
            for q in steps:
                tap = 8 * q + offset - lead
                small[tap : tap + 1, lanes(half)] = jnp.sum(found[half, q], 0, keepdims=True)
    for half in range(HALVES):
        small[TAPS : TAPS + 1, lanes(half)] = jnp.sum(gain_part[half], 0, keepdims=True)
    taps_rows = small[...].astype(NARROW)
    for near in range(CLOSE):
        for turn, rows in ((0, slice(0, BLOCK)), (CLOSE, slice(BLOCK, 2 * BLOCK))):
            far = lax.rem(place[0] // (2 * CLOSE) + near + turn, FAR)
            pieces[near, rows] = (mine[far] + other[far].astype(WIDE)).astype(NARROW)
        pieces[near, 2 * BLOCK :] = taps_rows


def gated_gradient(extended, taps, d_gated, margin, taps_wide):
    taps_wide[0:TAPS] = taps[...].astype(WIDE)
    for half in range(HALVES):
        for start in range(0, EDGE + ROWS, EDGE):
            found = jnp.zeros((EDGE, LANES), WIDE)
            for tap in range(TAPS):
                begin = start + TAPS - 1 - tap
                found = found + taps_wide[tap : tap + 1, lanes(half)] * extended[half, begin : begin + EDGE]
            if start == 0:
                margin[half] = found
            else:
                d_gated[half, start - EDGE : start] = found


def fold_near(arrived, to_first, to_second):
    for start in range(0, 2 * BLOCK + 32, 32):
        rows = slice(start, start + 32)
        total = arrived[0, rows].astype(WIDE)
        for near in range(1, CLOSE):
            total = total + arrived[near, rows].astype(WIDE)
        total = total.astype(NARROW)
        if start < BLOCK:
            to_first[rows] = total
        elif start < 2 * BLOCK:
            to_second[start - BLOCK : start - BLOCK + 32] = total
        else:
            to_first[BLOCK:] = total
            to_second[BLOCK:] = total


def fold_far(place, kept, first, second, message):
    own = place[0] // 2 % CLOSE == 0
    for start in range(BLOCK, -1, -8):
        size = 32 if start == BLOCK else 8
        rows = slice(start, start + size)
        here = jnp.where(own, kept[rows].astype(WIDE), first[rows].astype(WIDE))
        total = (here + second[rows].astype(WIDE)).astype(NARROW)
        if start == BLOCK:
            for position in range(2 * CLOSE):
                message[position, OWN:] = total
        else:
            for position in range(2 * CLOSE):
                if GATHER_ORDER[position] // 2 == start // 8:
                    message[position, 0:OWN] = total


def finish(
    place, arrived, d_gated, late, value, gate,
    value_grad, gate_grad, weight_grad, taps_grad, gain_grad,
):
    for half in range(HALVES):
        for start in range(0, ROWS, EDGE):
            rows = slice(start, start + EDGE)
            grad = d_gated[half, rows]
            if start == ROWS - EDGE:
                grad = grad + late[half]
            sig = jax.nn.sigmoid(gate[rows, lanes(half)].astype(WIDE))
            wide = value[rows, lanes(half)].astype(WIDE)
            value_grad[rows, lanes(half)] = (grad * sig).astype(NARROW)
            gate_grad[rows, lanes(half)] = (grad * wide * sig * (1.0 - sig)).astype(NARROW)
    by_core = []
    for side in range(2):
        positions = [p for p in range(2 * CLOSE) if GATHER_ORDER[p] % 2 == side]
        total = arrived[positions[0], 0:OWN].astype(WIDE)
        for position in positions[1:]:
            total = total + arrived[position, 0:OWN].astype(WIDE)
        by_core.append(total)
    weight_grad[...] = jnp.where(place[0] % 2 == 0, by_core[0], by_core[1])
    total = arrived[0, OWN:].astype(WIDE)
    for position in range(1, 2 * CLOSE):
        total = total + arrived[position, OWN:].astype(WIDE)
    taps_grad[...] = total[0:TAPS]
    gain_grad[...] = total[TAPS : TAPS + 1]


def to_block(value, turn):
    pairs = []
    for far in range(FAR):
        for near in range(CLOSE):
            step = (near + turn) % FAR
            if step:
                pairs.append((far * CLOSE + near, (far + step) % FAR * CLOSE + near))
    return lax.ppermute(value, ("zh", *NEAR), pairs)


def shards(
    proj_value, proj_gate, out_cotangent, out_weight, conv_taps, norm_gain, row_mean, row_scale
):
    end_gate = jax.nn.sigmoid(proj_gate[ROWS - EDGE :].astype(WIDE))
    end = (proj_value[ROWS - EDGE :].astype(WIDE) * end_gate).astype(NARROW)
    halo = shifted(end, SP, 1)
    split = (HALVES, ROWS, LANES)
    upstream = lax.dot_general(
        out_cotangent, out_weight, (((1,), (1,)), ((), ())), preferred_element_type=WIDE
    )
    rest = (HALVES, ROWS - EDGE, LANES)
    row_gain = norm_gain.reshape(1, WIDTH)
    sides = pltpu.VMEM((HALVES, EDGE + ROWS, LANES), WIDE)
    taps_scratch = pltpu.VMEM((TAPS + 1, WIDTH), WIDE)
    gated, scaled, spread, hidden, sums, gain_part = call_with(
        forward,
        [
            ((ROWS, WIDTH), NARROW), (rest, WIDE), (rest, WIDE),
            ((ROWS - EDGE, WIDTH), NARROW), ((8, LANES), WIDE), ((HALVES, 8, LANES), WIDE),
        ],
        [sides, taps_scratch, *([pltpu.VMEM((ROWS, LANES), WIDE)] * 4)],
        proj_value, proj_gate, upstream, conv_taps, row_gain, row_mean, row_scale,
        flops=100 * ROWS * WIDTH,
    )
    edge = (HALVES, EDGE, LANES)
    first_scaled, first_spread, first_hidden, message, gain_part = call_with(
        head,
        [
            (edge, WIDE), (edge, WIDE), ((EDGE, WIDTH), NARROW),
            ((TP, 8, LANES), WIDE), ((HALVES, 8, LANES), WIDE),
        ],
        [
            pltpu.VMEM((HALVES, 2 * EDGE, LANES), WIDE),
            taps_scratch,
            pltpu.VMEM((2, LANES, LANES), WIDE),
        ],
        halo, gated, upstream, conv_taps, row_gain, row_mean, row_scale, sums, gain_part,
        flops=10 * ROWS * WIDTH,
    )
    sums = exchange(message, "tp")
    place = lax.axis_index(SP).reshape(1)
    grouped = (FAR, CLOSE * OWN, WIDTH)
    mine, other = scalar_call(
        weight_product, [(grouped, WIDE), (grouped, NARROW)],
        place, out_cotangent, hidden, first_hidden,
        scratch=[pltpu.VMEM((ROWS, WIDTH), NARROW)], flops=2 * ROWS * WIDTH * MODEL,
    )
    other = lax.ppermute(other, "c", [(0, 1), (1, 0)])
    pieces, extended = scalar_call(
        backward,
        [((CLOSE, 2 * BLOCK + TAPS + 1, WIDTH), NARROW), ((HALVES, ROWS + 2 * EDGE, LANES), WIDE)],
        place, sums, scaled, spread, first_scaled, first_spread, halo, gated, row_scale,
        gain_part, mine, other, scratch=[taps_scratch, sides],
        flops=100 * ROWS * WIDTH,
    )
    arrived = exchange(pieces, NEAR)
    payload = ((BLOCK + TAPS + 1, WIDTH), NARROW)
    to_first, to_second = call(fold_near, [payload, payload], arrived, flops=1 << 20)
    first = to_block(to_first, 0)
    second = to_block(to_second, CLOSE)
    d_gated, margin = call_with(
        gated_gradient, [(split, WIDE), ((HALVES, EDGE, LANES), WIDE)], [taps_scratch],
        extended, conv_taps, flops=100 * ROWS * WIDTH,
    )
    late = shifted(margin, SP, -1)
    (message,) = scalar_call(
        fold_far, [((2 * CLOSE, OWN + TAPS + 1, WIDTH), NARROW)],
        place, to_first, first, second,
    )
    arrived = exchange(message, (*NEAR, "c"), GATHER_ORDER)
    narrow = ((ROWS, WIDTH), NARROW)
    value_grad, gate_grad, weight_grad, taps_grad, gain_grad = scalar_call(
        finish,
        [narrow, narrow, ((OWN, WIDTH), WIDE), ((TAPS, WIDTH), WIDE), ((1, WIDTH), WIDE)],
        place, arrived, d_gated, late, proj_value, proj_gate,
    )
    return (value_grad, gate_grad, weight_grad, taps_grad, gain_grad.reshape(WIDTH))


def call_with(body, outs, scratch, *args, flops=0, limit=6):
    shapes = [jax.ShapeDtypeStruct(shape, dtype) for shape, dtype in outs]
    size = sum(a.size * a.dtype.itemsize for a in (*args, *shapes))
    return pl.pallas_call(
        body,
        out_shape=shapes,
        scratch_shapes=scratch,
        compiler_params=pltpu.CompilerParams(vmem_limit_bytes=limit << 20),
        cost_estimate=pl.CostEstimate(flops=flops, bytes_accessed=size, transcendentals=0),
    )(*args)


def scalar_call(body, outs, scalar, *args, scratch=(), flops=1 << 20, limit=6):
    shapes = [jax.ShapeDtypeStruct(shape, dtype) for shape, dtype in outs]
    size = sum(a.size * a.dtype.itemsize for a in (*args, *shapes))
    whole = pl.BlockSpec(memory_space=pltpu.VMEM)
    return pl.pallas_call(
        body,
        out_shape=shapes,
        in_specs=[pl.BlockSpec(memory_space=pltpu.SMEM), *([whole] * len(args))],
        out_specs=[whole] * len(shapes),
        scratch_shapes=scratch,
        compiler_params=pltpu.CompilerParams(vmem_limit_bytes=limit << 20),
        cost_estimate=pl.CostEstimate(flops=flops, bytes_accessed=size, transcendentals=0),
    )(scalar, *args)


def solution(mesh):
    sizes = [size for _, size in AXES]
    split = Mesh(mesh.devices.reshape(*sizes, mesh.shape["tp"]), (*SP, "tp"))
    placed = (
        P(SP, "tp"),
        P(SP, "tp"),
        P(SP, None),
        P("tp", None),
        P(None, "tp"),
        P("tp"),
        P(SP),
        P(SP),
    )
    return jax.shard_map(
        shards,
        mesh=split,
        in_specs=placed,
        out_specs=(P(SP, "tp"), P(SP, "tp"), P(SP, "tp"), P(None, "tp"), P("tp")),
        check_vma=False,
    )
```

```python
import jax
import jax.numpy as jnp
from jax import lax
from jax.experimental import pallas as pl
from jax.experimental.pallas import tpu as pltpu
from jax.sharding import Mesh
from jax.sharding import PartitionSpec as P


SP = ("zh", "zl", "x", "c")
NEAR = ("zl", "x")
FAR = 16
CLOSE = 8
AXES = (("zh", FAR), ("zl", 2), ("x", 4), ("c", 2))
TP = 4
OFFSETS = ((0, -1, -2, -3, 1, 2, 3, -4), (8, 7, 6, 5, -7, -6, -5, 4))
BLOCK = CLOSE * 2 * 8
GATHER_ORDER = [(place + 1) % (2 * CLOSE) for place in range(2 * CLOSE)]
TAPS = 31
SMALL = TAPS + 1
ROWS = 384
EDGE = 32
LANES = 128
HALVES = 2
WIDTH = HALVES * LANES
MODEL = 2048
OWN = 8
CHUNK = 64
WIDE = jnp.float32
NARROW = jnp.bfloat16


def shifted(value, axis, steps):
    count = lax.axis_size(axis)
    first, last = (max(0, -steps), min(count, count - steps))
    return lax.ppermute(value, axis, [(source, source + steps) for source in range(first, last)])


def exchange(pieces, axes, order=None):
    groups = order and [order]
    return lax.all_to_all(pieces, axes, 0, 0, tiled=True, axis_index_groups=groups)


def lanes(half):
    return slice(half * LANES, (half + 1) * LANES)


def column(row):
    return jnp.transpose(jnp.broadcast_to(row, (LANES, LANES)))


def call(body, outs, *args, flops=0, limit=6):
    shapes = [jax.ShapeDtypeStruct(shape, dtype) for shape, dtype in outs]
    size = sum(a.size * a.dtype.itemsize for a in (*args, *shapes))
    return pl.pallas_call(
        body,
        out_shape=shapes,
        compiler_params=pltpu.CompilerParams(vmem_limit_bytes=limit << 20),
        cost_estimate=pl.CostEstimate(flops=flops, bytes_accessed=size, transcendentals=0),
    )(*args)


def norm_backward(conv, mean, factor, gain_row, upstream):
    normed = (conv - mean) * factor
    active = normed * gain_row
    sig = jax.nn.sigmoid(active)
    hidden = (active * sig).astype(NARROW)
    d_active = upstream * sig * (1.0 + active * (1.0 - sig))
    d_normed = d_active * gain_row
    gain_part = jnp.sum((d_active * normed).reshape(conv.shape[0] // 8, 8, LANES), 0)
    return hidden, factor * d_normed, factor * normed, d_normed, d_normed * normed, gain_part


def convolve(source, half, taps_wide, start, size):
    conv = jnp.zeros((size, LANES), WIDE)
    for tap in range(TAPS):
        begin = start + tap + EDGE - TAPS + 1
        conv = conv + taps_wide[tap : tap + 1, lanes(half)] * source[half, begin : begin + size]
    return conv


def column_sums(source):
    return jnp.sum(jnp.transpose(source), 0, keepdims=True)


def forward(
    value, gate, upstream, taps, gain, mean, scale,
    gated, scaled, spread, hidden, sums, gain_part,
    padded, taps_wide, mean_columns, scale_columns, sum_first, sum_second,
):
    taps_wide[0:TAPS] = taps[...].astype(WIDE)
    for block in range(ROWS // LANES):
        rows = slice(block * LANES, (block + 1) * LANES)
        mean_columns[rows] = column(mean[rows].reshape(1, LANES))
        scale_columns[rows] = column(scale[rows].reshape(1, LANES))
    for half in range(HALVES):
        for start in range(0, ROWS, CHUNK):
            rows = slice(start, start + CHUNK)
            sig = jax.nn.sigmoid(gate[rows, lanes(half)].astype(WIDE))
            product = (value[rows, lanes(half)].astype(WIDE) * sig).astype(NARROW)
            gated[rows, lanes(half)] = product
            padded[half, EDGE + start : EDGE + start + CHUNK] = product.astype(WIDE)
    sum_first[0:EDGE] = jnp.zeros((EDGE, LANES), WIDE)
    sum_second[0:EDGE] = jnp.zeros((EDGE, LANES), WIDE)
    for half in range(HALVES):
        gain_row = gain[0:1, lanes(half)]
        gain_sum = jnp.zeros((8, LANES), WIDE)
        for start in range(EDGE, ROWS, EDGE):
            rows = slice(start, start + EDGE)
            conv = convolve(padded, half, taps_wide, start, EDGE)
            narrow, own_scaled, own_spread, first, second, part = norm_backward(
                conv, mean_columns[rows], scale_columns[rows], gain_row, upstream[rows, lanes(half)]
            )
            hidden[start - EDGE : start, lanes(half)] = narrow
            scaled[half, start - EDGE : start] = own_scaled
            spread[half, start - EDGE : start] = own_spread
            gain_sum = gain_sum + part
            if half == 0:
                sum_first[rows] = first
                sum_second[rows] = second
            else:
                sum_first[rows] = sum_first[rows] + first
                sum_second[rows] = sum_second[rows] + second
        gain_part[half] = gain_sum
    found = [
        column_sums(source[block * LANES : (block + 1) * LANES])
        for source in (sum_first, sum_second)
        for block in range(ROWS // LANES)
    ]
    sums[...] = jnp.concatenate([*found, jnp.zeros((2, LANES), WIDE)], 0)


def head(
    _, halo, gated, upstream, taps, gain, mean, scale, sums, gain_part,
    scaled, spread, hidden, message, gain_total,
    padded, taps_wide, turned,
):
    taps_wide[0:TAPS] = taps[...].astype(WIDE)
    rows = slice(0, EDGE)
    mean_columns = column(mean[0:LANES].reshape(1, LANES))[rows]
    scale_columns = column(scale[0:LANES].reshape(1, LANES))[rows]
    turned[...] = jnp.zeros((2, LANES, LANES), WIDE)
    for half in range(HALVES):
        padded[half, rows] = halo[:, lanes(half)].astype(WIDE)
        padded[half, EDGE:] = gated[rows, lanes(half)].astype(WIDE)
    for half in range(HALVES):
        conv = convolve(padded, half, taps_wide, 0, EDGE)
        narrow, own_scaled, own_spread, first, second, part = norm_backward(
            conv, mean_columns, scale_columns, gain[0:1, lanes(half)], upstream[rows, lanes(half)]
        )
        hidden[:, lanes(half)] = narrow
        scaled[half] = own_scaled
        spread[half] = own_spread
        gain_total[half] = gain_part[half] + part
        turned[0, rows] = turned[0, rows] + first
        turned[1, rows] = turned[1, rows] + second
    blocks = ROWS // LANES
    total = sums[...]
    extra = [column_sums(turned[0]), column_sums(turned[1])]
    none = jnp.zeros((blocks - 1, LANES), WIDE)
    last = jnp.zeros((2, LANES), WIDE)
    total = total + jnp.concatenate([extra[0], none, extra[1], none, last], 0)
    for peer in range(TP):
        message[peer] = total


def block_rows(cotangent, hidden, far):
    columns = pl.ds(pl.multiple_of(far * BLOCK, BLOCK), BLOCK)
    return lax.dot_general(
        cotangent[:, columns], hidden[...], (((0,), (0,)), ((), ())), preferred_element_type=WIDE
    )


def backward(
    place, sums, scaled, spread, first_scaled, first_spread, halo, gated, scale, gain_part,
    cotangent, hidden, first_hidden,
    mine, other, small, extended,
    padded, whole,
):
    far, core = place[0] // (2 * CLOSE), place[0] % 2
    whole[0:EDGE] = first_hidden[...]
    whole[EDGE:] = hidden[...]
    for half in range(HALVES):
        padded[half, 0:EDGE] = halo[:, lanes(half)].astype(WIDE)
        padded[half, EDGE:] = gated[:, lanes(half)].astype(WIDE)
    total = (sums[0] + sums[1]) + (sums[2] + sums[3])
    total = total * (1.0 / (TP * WIDTH))
    blocks = ROWS // LANES
    for half in range(HALVES):
        extended[half, 0:EDGE] = jnp.zeros((EDGE, LANES), WIDE)
        extended[half, EDGE + ROWS :] = jnp.zeros((EDGE, LANES), WIDE)
    for block in range(blocks):
        rows = slice(block * LANES, (block + 1) * LANES)
        first = column(total[block : block + 1] * scale[rows].reshape(1, LANES))
        second = column(total[blocks + block : blocks + block + 1])
        for half in range(HALVES):
            cut = 0
            if block == 0:
                cut = EDGE
                d_conv = first_scaled[half] - first[0:cut] - first_spread[half] * second[0:cut]
                extended[half, EDGE : EDGE + cut] = d_conv
            rows = slice(block * LANES + cut - EDGE, (block + 1) * LANES - EDGE)
            d_conv = scaled[half, rows] - first[cut:] - spread[half, rows] * second[cut:]
            extended[half, EDGE + block * LANES + cut : EDGE + (block + 1) * LANES] = d_conv
    lead = EDGE - TAPS + 1
    groups = ROWS // 8
    for offset in range(8):
        steps = [q for q in range(5) if 0 <= 8 * q + offset - lead < TAPS]
        found = {(half, q): jnp.zeros((8, LANES), WIDE) for half in range(HALVES) for q in steps}
        loaded = {}
        for m in range(groups + steps[-1]):
            for half in range(HALVES):
                if m < groups:
                    begin = EDGE + 8 * m
                    loaded[half, m] = extended[half, begin : begin + 8]
                moved = padded[half, 8 * m + offset : 8 * m + offset + 8]
                for q in steps:
                    if 0 <= m - q < groups:
                        found[half, q] = found[half, q] + loaded[half, m - q] * moved
        for half in range(HALVES):
            for q in steps:
                tap = 8 * q + offset - lead
                small[tap : tap + 1, lanes(half)] = jnp.sum(found[half, q], 0, keepdims=True)
        near = offset
        low, high = OFFSETS[0][near], OFFSETS[1][near]
        own = lax.rem(far + jnp.where(core == 0, low, high) + FAR, FAR)
        theirs = lax.rem(far + jnp.where(core == 0, high, low) + FAR, FAR)
        mine[near] = block_rows(cotangent, whole, own)
        other[near * BLOCK : (near + 1) * BLOCK] = block_rows(cotangent, whole, theirs).astype(NARROW)
    for half in range(HALVES):
        small[TAPS:SMALL, lanes(half)] = jnp.sum(gain_part[half], 0, keepdims=True)
    value = small[...]
    top = value.astype(NARROW)
    other[CLOSE * BLOCK : CLOSE * BLOCK + SMALL] = top
    other[CLOSE * BLOCK + SMALL :] = (value - top.astype(WIDE)).astype(NARROW)


def pack(mine, small, other, pieces):
    end = CLOSE * BLOCK
    top = other[end : end + SMALL].astype(WIDE)
    both = small[...] + (top + other[end + SMALL :].astype(WIDE))
    both = both.astype(NARROW)
    for near in range(CLOSE):
        for start in range(0, BLOCK, 32):
            rows = slice(start, start + 32)
            there = other[near * BLOCK + start : near * BLOCK + start + 32].astype(WIDE)
            pieces[near, rows] = (mine[near, rows] + there).astype(NARROW)
        pieces[near, BLOCK:] = both


def gated_gradient(extended, taps, d_gated, margin, taps_wide):
    taps_wide[0:TAPS] = taps[...].astype(WIDE)
    for half in range(HALVES):
        for start in range(0, EDGE + ROWS, EDGE):
            found = jnp.zeros((EDGE, LANES), WIDE)
            for tap in range(TAPS):
                begin = start + TAPS - 1 - tap
                found = found + taps_wide[tap : tap + 1, lanes(half)] * extended[half, begin : begin + EDGE]
            if start == 0:
                margin[half] = found
            else:
                d_gated[half, start - EDGE : start] = found


def fold_near(arrived, payload):
    for start in range(0, BLOCK + SMALL, 32):
        rows = slice(start, start + 32)
        total = arrived[0, rows].astype(WIDE)
        for near in range(1, CLOSE):
            total = total + arrived[near, rows].astype(WIDE)
        payload[rows] = total.astype(NARROW)


def hand_out(payload, message):
    for position, member in enumerate(GATHER_ORDER):
        message[position, 0:OWN] = payload[member * OWN : (member + 1) * OWN]
        message[position, OWN:] = payload[BLOCK:]


def finish(
    arrived, d_gated, late, value, gate,
    value_grad, gate_grad, weight_grad, taps_grad, gain_grad,
):
    for half in range(HALVES):
        for start in range(0, ROWS, EDGE):
            rows = slice(start, start + EDGE)
            grad = d_gated[half, rows]
            if start == ROWS - EDGE:
                grad = grad + late[half]
            sig = jax.nn.sigmoid(gate[rows, lanes(half)].astype(WIDE))
            wide = value[rows, lanes(half)].astype(WIDE)
            value_grad[rows, lanes(half)] = (grad * sig).astype(NARROW)
            gate_grad[rows, lanes(half)] = (grad * wide * sig * (1.0 - sig)).astype(NARROW)
    total = arrived[0].astype(WIDE)
    for position in range(1, 2 * CLOSE):
        total = total + arrived[position].astype(WIDE)
    weight_grad[...] = total[0:OWN]
    taps_grad[...] = total[OWN : OWN + TAPS]
    gain_grad[...] = total[OWN + TAPS :]


def to_block(value):
    pairs = []
    for far in range(FAR):
        for near in range(CLOSE):
            for core in range(2):
                target = (far + OFFSETS[core][near]) % FAR
                pairs.append(((far * CLOSE + near) * 2 + core, (target * CLOSE + near) * 2 + core))
    return lax.ppermute(value, SP, pairs)


def shards(
    proj_value, proj_gate, out_cotangent, out_weight, conv_taps, norm_gain, row_mean, row_scale
):
    end_gate = jax.nn.sigmoid(proj_gate[ROWS - EDGE :].astype(WIDE))
    end = (proj_value[ROWS - EDGE :].astype(WIDE) * end_gate).astype(NARROW)
    halo = shifted(end, SP, 1)
    split = (HALVES, ROWS, LANES)
    upstream = lax.dot_general(
        out_cotangent, out_weight, (((1,), (1,)), ((), ())), preferred_element_type=WIDE
    )
    rest = (HALVES, ROWS - EDGE, LANES)
    row_gain = norm_gain.reshape(1, WIDTH)
    sides = pltpu.VMEM((HALVES, EDGE + ROWS, LANES), WIDE)
    taps_scratch = pltpu.VMEM((TAPS + 1, WIDTH), WIDE)
    gated, scaled, spread, hidden, sums, gain_part = call_with(
        forward,
        [
            ((ROWS, WIDTH), NARROW), (rest, WIDE), (rest, WIDE),
            ((ROWS - EDGE, WIDTH), NARROW), ((8, LANES), WIDE), ((HALVES, 8, LANES), WIDE),
        ],
        [sides, taps_scratch, *([pltpu.VMEM((ROWS, LANES), WIDE)] * 4)],
        proj_value, proj_gate, upstream, conv_taps, row_gain, row_mean, row_scale,
        flops=100 * ROWS * WIDTH,
    )
    edge = (HALVES, EDGE, LANES)
    place = lax.axis_index(SP).reshape(1)
    first_scaled, first_spread, first_hidden, message, gain_part = scalar_call(
        head,
        [
            (edge, WIDE), (edge, WIDE), ((EDGE, WIDTH), NARROW),
            ((TP, 8, LANES), WIDE), ((HALVES, 8, LANES), WIDE),
        ],
        place, halo, gated, upstream, conv_taps, row_gain, row_mean, row_scale, sums,
        gain_part,
        scratch=[
            pltpu.VMEM((HALVES, 2 * EDGE, LANES), WIDE),
            taps_scratch,
            pltpu.VMEM((2, LANES, LANES), WIDE),
        ],
        flops=10 * ROWS * WIDTH,
    )
    sums = exchange(message, "tp")
    rows = CLOSE * BLOCK + 2 * SMALL
    mine, other, small, extended = scalar_call(
        backward,
        [
            ((CLOSE, BLOCK, WIDTH), WIDE), ((rows, WIDTH), NARROW), ((SMALL, WIDTH), WIDE),
            ((HALVES, ROWS + 2 * EDGE, LANES), WIDE),
        ],
        place, sums, scaled, spread, first_scaled, first_spread, halo, gated, row_scale, gain_part,
        out_cotangent, hidden, first_hidden,
        scratch=[sides, pltpu.VMEM((ROWS, WIDTH), NARROW)], flops=2 * ROWS * WIDTH * MODEL,
    )
    other = lax.ppermute(other, "c", [(0, 1), (1, 0)])
    d_gated, margin = call_with(
        gated_gradient, [(split, WIDE), ((HALVES, EDGE, LANES), WIDE)], [taps_scratch],
        extended, conv_taps, flops=100 * ROWS * WIDTH,
    )
    (pieces,) = call(
        pack, [((CLOSE, BLOCK + SMALL, WIDTH), NARROW)], mine, small, other, flops=1 << 20
    )
    arrived = exchange(pieces, NEAR)
    (payload,) = call(fold_near, [((BLOCK + SMALL, WIDTH), NARROW)], arrived, flops=1 << 20)
    payload = to_block(payload)
    late = shifted(margin, SP, -1)
    (message,) = call(hand_out, [((2 * CLOSE, OWN + SMALL, WIDTH), NARROW)], payload, flops=1 << 16)
    arrived = exchange(message, (*NEAR, "c"), GATHER_ORDER)
    narrow = ((ROWS, WIDTH), NARROW)
    value_grad, gate_grad, weight_grad, taps_grad, gain_grad = call(
        finish,
        [narrow, narrow, ((OWN, WIDTH), WIDE), ((TAPS, WIDTH), WIDE), ((1, WIDTH), WIDE)],
        arrived, d_gated, late, proj_value, proj_gate, flops=10 * ROWS * WIDTH,
    )
    return (value_grad, gate_grad, weight_grad, taps_grad, gain_grad.reshape(WIDTH))


def call_with(body, outs, scratch, *args, flops=0, limit=6):
    shapes = [jax.ShapeDtypeStruct(shape, dtype) for shape, dtype in outs]
    size = sum(a.size * a.dtype.itemsize for a in (*args, *shapes))
    return pl.pallas_call(
        body,
        out_shape=shapes,
        scratch_shapes=scratch,
        compiler_params=pltpu.CompilerParams(vmem_limit_bytes=limit << 20),
        cost_estimate=pl.CostEstimate(flops=flops, bytes_accessed=size, transcendentals=0),
    )(*args)


def scalar_call(body, outs, scalar, *args, scratch=(), flops=1 << 20, limit=6):
    shapes = [jax.ShapeDtypeStruct(shape, dtype) for shape, dtype in outs]
    size = sum(a.size * a.dtype.itemsize for a in (*args, *shapes))
    whole = pl.BlockSpec(memory_space=pltpu.VMEM)
    return pl.pallas_call(
        body,
        out_shape=shapes,
        in_specs=[pl.BlockSpec(memory_space=pltpu.SMEM), *([whole] * len(args))],
        out_specs=[whole] * len(shapes),
        scratch_shapes=scratch,
        compiler_params=pltpu.CompilerParams(vmem_limit_bytes=limit << 20),
        cost_estimate=pl.CostEstimate(flops=flops, bytes_accessed=size, transcendentals=0),
    )(scalar, *args)


def solution(mesh):
    sizes = [size for _, size in AXES]
    split = Mesh(mesh.devices.reshape(*sizes, mesh.shape["tp"]), (*SP, "tp"))
    placed = (
        P(SP, "tp"),
        P(SP, "tp"),
        P(SP, None),
        P("tp", None),
        P(None, "tp"),
        P("tp"),
        P(SP),
        P(SP),
    )
    return jax.shard_map(
        shards,
        mesh=split,
        in_specs=placed,
        out_specs=(P(SP, "tp"), P(SP, "tp"), P(SP, "tp"), P(None, "tp"), P("tp")),
        check_vma=False,
    )
```

```python
import jax
import jax.numpy as jnp
from jax import lax
from jax.experimental import pallas as pl
from jax.experimental.pallas import tpu as pltpu
from jax.sharding import Mesh
from jax.sharding import PartitionSpec as P


SP = ("zh", "zl", "x", "c")
NEAR = ("zl", "x")
FAR = 16
CLOSE = 8
AXES = (("zh", FAR), ("zl", 2), ("x", 4), ("c", 2))
TP = 4
SUMS_ORDER = [1, 2, 3, 0]
OFFSETS = ((0, -1, -2, -3, 1, 2, 3, -4), (8, 7, 6, 5, -7, -6, -5, 4))
BLOCK = CLOSE * 2 * 8
GATHER_ORDER = [(place + 1) % (2 * CLOSE) for place in range(2 * CLOSE)]
TAPS = 31
SMALL = TAPS + 1
ROWS = 384
EDGE = 32
LANES = 128
HALVES = 2
WIDTH = HALVES * LANES
MODEL = 2048
OWN = 8
CHUNK = 64
WIDE = jnp.float32
NARROW = jnp.bfloat16


def shifted(value, axis, steps):
    count = lax.axis_size(axis)
    first, last = (max(0, -steps), min(count, count - steps))
    return lax.ppermute(value, axis, [(source, source + steps) for source in range(first, last)])


def exchange(pieces, axes, order=None):
    groups = order and [order]
    return lax.all_to_all(pieces, axes, 0, 0, tiled=True, axis_index_groups=groups)


def lanes(half):
    return slice(half * LANES, (half + 1) * LANES)


def column(row):
    return jnp.transpose(jnp.broadcast_to(row, (LANES, LANES)))


def call(body, outs, *args, flops=0, limit=6):
    shapes = [jax.ShapeDtypeStruct(shape, dtype) for shape, dtype in outs]
    size = sum(a.size * a.dtype.itemsize for a in (*args, *shapes))
    return pl.pallas_call(
        body,
        out_shape=shapes,
        compiler_params=pltpu.CompilerParams(vmem_limit_bytes=limit << 20),
        cost_estimate=pl.CostEstimate(flops=flops, bytes_accessed=size, transcendentals=0),
    )(*args)


def norm_backward(conv, mean, factor, gain_row, upstream):
    normed = (conv - mean) * factor
    active = normed * gain_row
    sig = jax.nn.sigmoid(active)
    hidden = (active * sig).astype(NARROW)
    d_active = upstream * sig * (1.0 + active * (1.0 - sig))
    d_normed = d_active * gain_row
    gain_part = jnp.sum((d_active * normed).reshape(conv.shape[0] // 8, 8, LANES), 0)
    return hidden, factor * d_normed, factor * normed, d_normed, d_normed * normed, gain_part


def convolve(source, half, taps_wide, start, size):
    conv = jnp.zeros((size, LANES), WIDE)
    for tap in range(TAPS):
        begin = start + tap + EDGE - TAPS + 1
        conv = conv + taps_wide[tap : tap + 1, lanes(half)] * source[half, begin : begin + size]
    return conv


def column_sums(source):
    return jnp.sum(jnp.transpose(source), 0, keepdims=True)


def forward(
    value, gate, upstream, taps, gain, mean, scale,
    gated, scaled, spread, hidden, sums, gain_part,
    padded, taps_wide, mean_columns, scale_columns, sum_first, sum_second,
):
    taps_wide[0:TAPS] = taps[...].astype(WIDE)
    for block in range(ROWS // LANES):
        rows = slice(block * LANES, (block + 1) * LANES)
        mean_columns[rows] = column(mean[rows].reshape(1, LANES))
        scale_columns[rows] = column(scale[rows].reshape(1, LANES))
    for half in range(HALVES):
        for start in range(0, ROWS, CHUNK):
            rows = slice(start, start + CHUNK)
            sig = jax.nn.sigmoid(gate[rows, lanes(half)].astype(WIDE))
            product = (value[rows, lanes(half)].astype(WIDE) * sig).astype(NARROW)
            gated[rows, lanes(half)] = product
            padded[half, EDGE + start : EDGE + start + CHUNK] = product.astype(WIDE)
    sum_first[0:EDGE] = jnp.zeros((EDGE, LANES), WIDE)
    sum_second[0:EDGE] = jnp.zeros((EDGE, LANES), WIDE)
    for half in range(HALVES):
        gain_row = gain[0:1, lanes(half)]
        gain_sum = jnp.zeros((8, LANES), WIDE)
        for start in range(EDGE, ROWS, EDGE):
            rows = slice(start, start + EDGE)
            conv = convolve(padded, half, taps_wide, start, EDGE)
            narrow, own_scaled, own_spread, first, second, part = norm_backward(
                conv, mean_columns[rows], scale_columns[rows], gain_row, upstream[rows, lanes(half)]
            )
            hidden[start - EDGE : start, lanes(half)] = narrow
            scaled[half, start - EDGE : start] = own_scaled
            spread[half, start - EDGE : start] = own_spread
            gain_sum = gain_sum + part
            if half == 0:
                sum_first[rows] = first
                sum_second[rows] = second
            else:
                sum_first[rows] = sum_first[rows] + first
                sum_second[rows] = sum_second[rows] + second
        gain_part[half] = gain_sum
    found = [
        column_sums(source[block * LANES : (block + 1) * LANES])
        for source in (sum_first, sum_second)
        for block in range(ROWS // LANES)
    ]
    sums[...] = jnp.concatenate([*found, jnp.zeros((2, LANES), WIDE)], 0)


def head(
    _, halo, gated, upstream, taps, gain, mean, scale, sums, gain_part,
    scaled, spread, hidden, message, gain_total,
    padded, taps_wide, turned,
):
    taps_wide[0:TAPS] = taps[...].astype(WIDE)
    rows = slice(0, EDGE)
    mean_columns = column(mean[0:LANES].reshape(1, LANES))[rows]
    scale_columns = column(scale[0:LANES].reshape(1, LANES))[rows]
    turned[...] = jnp.zeros((2, LANES, LANES), WIDE)
    for half in range(HALVES):
        padded[half, rows] = halo[:, lanes(half)].astype(WIDE)
        padded[half, EDGE:] = gated[rows, lanes(half)].astype(WIDE)
    for half in range(HALVES):
        conv = convolve(padded, half, taps_wide, 0, EDGE)
        narrow, own_scaled, own_spread, first, second, part = norm_backward(
            conv, mean_columns, scale_columns, gain[0:1, lanes(half)], upstream[rows, lanes(half)]
        )
        hidden[:, lanes(half)] = narrow
        scaled[half] = own_scaled
        spread[half] = own_spread
        gain_total[half] = gain_part[half] + part
        turned[0, rows] = turned[0, rows] + first
        turned[1, rows] = turned[1, rows] + second
    blocks = ROWS // LANES
    total = sums[...]
    extra = [column_sums(turned[0]), column_sums(turned[1])]
    none = jnp.zeros((blocks - 1, LANES), WIDE)
    last = jnp.zeros((2, LANES), WIDE)
    total = total + jnp.concatenate([extra[0], none, extra[1], none, last], 0)
    for peer in range(TP):
        message[peer] = total


def block_rows(cotangent, hidden, far):
    columns = pl.ds(pl.multiple_of(far * BLOCK, BLOCK), BLOCK)
    return lax.dot_general(
        cotangent[:, columns], hidden[...], (((0,), (0,)), ((), ())), preferred_element_type=WIDE
    )


def backward(
    place, sums, scaled, spread, first_scaled, first_spread, halo, gated, scale, gain_part,
    cotangent, hidden, first_hidden,
    mine, other, small, extended,
    padded, whole,
):
    far, core = place[0] // (2 * CLOSE), place[0] % 2
    whole[0:EDGE] = first_hidden[...]
    whole[EDGE:] = hidden[...]
    for half in range(HALVES):
        padded[half, 0:EDGE] = halo[:, lanes(half)].astype(WIDE)
        padded[half, EDGE:] = gated[:, lanes(half)].astype(WIDE)
    total = (sums[0] + sums[1]) + (sums[2] + sums[3])
    total = total * (1.0 / (TP * WIDTH))
    blocks = ROWS // LANES
    for half in range(HALVES):
        extended[half, 0:EDGE] = jnp.zeros((EDGE, LANES), WIDE)
        extended[half, EDGE + ROWS :] = jnp.zeros((EDGE, LANES), WIDE)
    for block in range(blocks):
        rows = slice(block * LANES, (block + 1) * LANES)
        first = column(total[block : block + 1] * scale[rows].reshape(1, LANES))
        second = column(total[blocks + block : blocks + block + 1])
        for half in range(HALVES):
            cut = 0
            if block == 0:
                cut = EDGE
                d_conv = first_scaled[half] - first[0:cut] - first_spread[half] * second[0:cut]
                extended[half, EDGE : EDGE + cut] = d_conv
            rows = slice(block * LANES + cut - EDGE, (block + 1) * LANES - EDGE)
            d_conv = scaled[half, rows] - first[cut:] - spread[half, rows] * second[cut:]
            extended[half, EDGE + block * LANES + cut : EDGE + (block + 1) * LANES] = d_conv
    lead = EDGE - TAPS + 1
    groups = ROWS // 8
    for offset in range(8):
        steps = [q for q in range(5) if 0 <= 8 * q + offset - lead < TAPS]
        found = {(half, q): jnp.zeros((8, LANES), WIDE) for half in range(HALVES) for q in steps}
        loaded = {}
        for m in range(groups + steps[-1]):
            for half in range(HALVES):
                if m < groups:
                    begin = EDGE + 8 * m
                    loaded[half, m] = extended[half, begin : begin + 8]
                moved = padded[half, 8 * m + offset : 8 * m + offset + 8]
                for q in steps:
                    if 0 <= m - q < groups:
                        found[half, q] = found[half, q] + loaded[half, m - q] * moved
        for half in range(HALVES):
            for q in steps:
                tap = 8 * q + offset - lead
                small[tap : tap + 1, lanes(half)] = jnp.sum(found[half, q], 0, keepdims=True)
        near = offset
        low, high = OFFSETS[0][near], OFFSETS[1][near]
        own = lax.rem(far + jnp.where(core == 0, low, high) + FAR, FAR)
        theirs = lax.rem(far + jnp.where(core == 0, high, low) + FAR, FAR)
        mine[near] = block_rows(cotangent, whole, own)
        other[near * BLOCK : (near + 1) * BLOCK] = block_rows(cotangent, whole, theirs).astype(NARROW)
    for half in range(HALVES):
        small[TAPS:SMALL, lanes(half)] = jnp.sum(gain_part[half], 0, keepdims=True)
    value = small[...]
    top = value.astype(NARROW)
    other[CLOSE * BLOCK : CLOSE * BLOCK + SMALL] = top
    other[CLOSE * BLOCK + SMALL :] = (value - top.astype(WIDE)).astype(NARROW)


def pack(mine, small, other, pieces):
    end = CLOSE * BLOCK
    top = other[end : end + SMALL].astype(WIDE)
    both = small[...] + (top + other[end + SMALL :].astype(WIDE))
    both = both.astype(NARROW)
    for near in range(CLOSE):
        for start in range(0, BLOCK, 32):
            rows = slice(start, start + 32)
            there = other[near * BLOCK + start : near * BLOCK + start + 32].astype(WIDE)
            pieces[near, rows] = (mine[near, rows] + there).astype(NARROW)
        pieces[near, BLOCK:] = both


def gated_gradient(extended, taps, d_gated, margin, taps_wide):
    taps_wide[0:TAPS] = taps[...].astype(WIDE)
    for half in range(HALVES):
        for start in range(0, EDGE + ROWS, EDGE):
            found = jnp.zeros((EDGE, LANES), WIDE)
            for tap in range(TAPS):
                begin = start + TAPS - 1 - tap
                found = found + taps_wide[tap : tap + 1, lanes(half)] * extended[half, begin : begin + EDGE]
            if start == 0:
                margin[half] = found
            else:
                d_gated[half, start - EDGE : start] = found


def fold_near(arrived, payload):
    for start in range(0, BLOCK + SMALL, 32):
        rows = slice(start, start + 32)
        total = arrived[0, rows].astype(WIDE)
        for near in range(1, CLOSE):
            total = total + arrived[near, rows].astype(WIDE)
        payload[rows] = total.astype(NARROW)


def hand_out(payload, message):
    for position, member in enumerate(GATHER_ORDER):
        message[position, 0:OWN] = payload[member * OWN : (member + 1) * OWN]
        message[position, OWN:] = payload[BLOCK:]


def totals(arrived, total):
    for start in range(0, OWN + SMALL, 8):
        rows = slice(start, start + 8)
        found = arrived[0, rows].astype(WIDE)
        for position in range(1, 2 * CLOSE):
            found = found + arrived[position, rows].astype(WIDE)
        total[rows] = found


def finish(
    total, d_gated, late, value, gate,
    value_grad, gate_grad, weight_grad, taps_grad, gain_grad,
):
    for half in range(HALVES):
        for start in range(0, ROWS, EDGE):
            rows = slice(start, start + EDGE)
            grad = d_gated[half, rows]
            if start == ROWS - EDGE:
                grad = grad + late[half]
            sig = jax.nn.sigmoid(gate[rows, lanes(half)].astype(WIDE))
            wide = value[rows, lanes(half)].astype(WIDE)
            value_grad[rows, lanes(half)] = (grad * sig).astype(NARROW)
            gate_grad[rows, lanes(half)] = (grad * wide * sig * (1.0 - sig)).astype(NARROW)
    weight_grad[...] = total[0:OWN]
    taps_grad[...] = total[OWN : OWN + TAPS]
    gain_grad[...] = total[OWN + TAPS :]


def to_block(value):
    pairs = []
    for far in range(FAR):
        for near in range(CLOSE):
            for core in range(2):
                target = (far + OFFSETS[core][near]) % FAR
                pairs.append(((far * CLOSE + near) * 2 + core, (target * CLOSE + near) * 2 + core))
    return lax.ppermute(value, SP, pairs)


def shards(
    proj_value, proj_gate, out_cotangent, out_weight, conv_taps, norm_gain, row_mean, row_scale
):
    end_gate = jax.nn.sigmoid(proj_gate[ROWS - EDGE :].astype(WIDE))
    end = (proj_value[ROWS - EDGE :].astype(WIDE) * end_gate).astype(NARROW)
    halo = shifted(end, SP, 1)
    split = (HALVES, ROWS, LANES)
    upstream = lax.dot_general(
        out_cotangent, out_weight, (((1,), (1,)), ((), ())), preferred_element_type=WIDE
    )
    rest = (HALVES, ROWS - EDGE, LANES)
    row_gain = norm_gain.reshape(1, WIDTH)
    sides = pltpu.VMEM((HALVES, EDGE + ROWS, LANES), WIDE)
    taps_scratch = pltpu.VMEM((TAPS + 1, WIDTH), WIDE)
    gated, scaled, spread, hidden, sums, gain_part = call_with(
        forward,
        [
            ((ROWS, WIDTH), NARROW), (rest, WIDE), (rest, WIDE),
            ((ROWS - EDGE, WIDTH), NARROW), ((8, LANES), WIDE), ((HALVES, 8, LANES), WIDE),
        ],
        [sides, taps_scratch, *([pltpu.VMEM((ROWS, LANES), WIDE)] * 4)],
        proj_value, proj_gate, upstream, conv_taps, row_gain, row_mean, row_scale,
        flops=100 * ROWS * WIDTH,
    )
    edge = (HALVES, EDGE, LANES)
    place = lax.axis_index(SP).reshape(1)
    first_scaled, first_spread, first_hidden, message, gain_part = scalar_call(
        head,
        [
            (edge, WIDE), (edge, WIDE), ((EDGE, WIDTH), NARROW),
            ((TP, 8, LANES), WIDE), ((HALVES, 8, LANES), WIDE),
        ],
        place, halo, gated, upstream, conv_taps, row_gain, row_mean, row_scale, sums,
        gain_part,
        scratch=[
            pltpu.VMEM((HALVES, 2 * EDGE, LANES), WIDE),
            taps_scratch,
            pltpu.VMEM((2, LANES, LANES), WIDE),
        ],
        flops=10 * ROWS * WIDTH,
    )
    sums = exchange(message, "tp", SUMS_ORDER)
    rows = CLOSE * BLOCK + 2 * SMALL
    mine, other, small, extended = scalar_call(
        backward,
        [
            ((CLOSE, BLOCK, WIDTH), WIDE), ((rows, WIDTH), NARROW), ((SMALL, WIDTH), WIDE),
            ((HALVES, ROWS + 2 * EDGE, LANES), WIDE),
        ],
        place, sums, scaled, spread, first_scaled, first_spread, halo, gated, row_scale, gain_part,
        out_cotangent, hidden, first_hidden,
        scratch=[sides, pltpu.VMEM((ROWS, WIDTH), NARROW)], flops=2 * ROWS * WIDTH * MODEL,
    )
    other = lax.ppermute(other, "c", [(0, 1), (1, 0)])
    d_gated, margin = call_with(
        gated_gradient, [(split, WIDE), ((HALVES, EDGE, LANES), WIDE)], [taps_scratch],
        extended, conv_taps, flops=100 * ROWS * WIDTH,
    )
    (pieces,) = call(
        pack, [((CLOSE, BLOCK + SMALL, WIDTH), NARROW)], mine, small, other, flops=1 << 20
    )
    arrived = exchange(pieces, NEAR)
    (payload,) = call(fold_near, [((BLOCK + SMALL, WIDTH), NARROW)], arrived, flops=1 << 20)
    payload = to_block(payload)
    late = shifted(margin, SP, -1)
    (message,) = call(hand_out, [((2 * CLOSE, OWN + SMALL, WIDTH), NARROW)], payload, flops=1 << 16)
    arrived = exchange(message, (*NEAR, "c"), GATHER_ORDER)
    (total,) = call(totals, [((OWN + SMALL, WIDTH), WIDE)], arrived, flops=1 << 20)
    narrow = ((ROWS, WIDTH), NARROW)
    value_grad, gate_grad, weight_grad, taps_grad, gain_grad = call(
        finish,
        [narrow, narrow, ((OWN, WIDTH), WIDE), ((TAPS, WIDTH), WIDE), ((1, WIDTH), WIDE)],
        total, d_gated, late, proj_value, proj_gate, flops=10 * ROWS * WIDTH,
    )
    return (value_grad, gate_grad, weight_grad, taps_grad, gain_grad.reshape(WIDTH))


def call_with(body, outs, scratch, *args, flops=0, limit=6):
    shapes = [jax.ShapeDtypeStruct(shape, dtype) for shape, dtype in outs]
    size = sum(a.size * a.dtype.itemsize for a in (*args, *shapes))
    return pl.pallas_call(
        body,
        out_shape=shapes,
        scratch_shapes=scratch,
        compiler_params=pltpu.CompilerParams(vmem_limit_bytes=limit << 20),
        cost_estimate=pl.CostEstimate(flops=flops, bytes_accessed=size, transcendentals=0),
    )(*args)


def scalar_call(body, outs, scalar, *args, scratch=(), flops=1 << 20, limit=6):
    shapes = [jax.ShapeDtypeStruct(shape, dtype) for shape, dtype in outs]
    size = sum(a.size * a.dtype.itemsize for a in (*args, *shapes))
    whole = pl.BlockSpec(memory_space=pltpu.VMEM)
    return pl.pallas_call(
        body,
        out_shape=shapes,
        in_specs=[pl.BlockSpec(memory_space=pltpu.SMEM), *([whole] * len(args))],
        out_specs=[whole] * len(shapes),
        scratch_shapes=scratch,
        compiler_params=pltpu.CompilerParams(vmem_limit_bytes=limit << 20),
        cost_estimate=pl.CostEstimate(flops=flops, bytes_accessed=size, transcendentals=0),
    )(scalar, *args)


def solution(mesh):
    sizes = [size for _, size in AXES]
    split = Mesh(mesh.devices.reshape(*sizes, mesh.shape["tp"]), (*SP, "tp"))
    placed = (
        P(SP, "tp"),
        P(SP, "tp"),
        P(SP, None),
        P("tp", None),
        P(None, "tp"),
        P("tp"),
        P(SP),
        P(SP),
    )
    return jax.shard_map(
        shards,
        mesh=split,
        in_specs=placed,
        out_specs=(P(SP, "tp"), P(SP, "tp"), P(SP, "tp"), P(None, "tp"), P("tp")),
        check_vma=False,
    )
```

```python
import jax
import jax.numpy as jnp
from jax import lax
from jax.experimental import pallas as pl
from jax.experimental.pallas import tpu as pltpu
from jax.sharding import Mesh
from jax.sharding import PartitionSpec as P


SP = ("zh", "zl", "x", "c")
NEAR = ("zl", "x")
FAR = 16
CLOSE = 8
AXES = (("zh", FAR), ("zl", 2), ("x", 4), ("c", 2))
TP = 4
SUMS_ORDER = [3, 0, 1, 2]
OFFSETS = ((0, -1, -2, -3, 3, 2, 1, -4), (6, 7, 8, 5, -7, -6, -5, 4))
BLOCK = CLOSE * 2 * 8
GATHER_ORDER = [(place + 1) % (2 * CLOSE) for place in range(2 * CLOSE)]
TAPS = 31
SMALL = TAPS + 1
ROWS = 384
EDGE = 32
LANES = 128
HALVES = 2
WIDTH = HALVES * LANES
MODEL = 2048
OWN = 8
PART_ENDS = (128, 256, 352)
CHUNK = 64
WIDE = jnp.float32
NARROW = jnp.bfloat16


def shifted(value, axis, steps):
    count = lax.axis_size(axis)
    first, last = (max(0, -steps), min(count, count - steps))
    return lax.ppermute(value, axis, [(source, source + steps) for source in range(first, last)])


def exchange(pieces, axes, order=None):
    groups = order and [order]
    return lax.all_to_all(pieces, axes, 0, 0, tiled=True, axis_index_groups=groups)


def lanes(half):
    return slice(half * LANES, (half + 1) * LANES)


def column(row):
    return jnp.transpose(jnp.broadcast_to(row, (LANES, LANES)))


def call(body, outs, *args, flops=0, limit=6):
    shapes = [jax.ShapeDtypeStruct(shape, dtype) for shape, dtype in outs]
    size = sum(a.size * a.dtype.itemsize for a in (*args, *shapes))
    return pl.pallas_call(
        body,
        out_shape=shapes,
        compiler_params=pltpu.CompilerParams(vmem_limit_bytes=limit << 20),
        cost_estimate=pl.CostEstimate(flops=flops, bytes_accessed=size, transcendentals=0),
    )(*args)


def norm_backward(normed, factor, gain_row, upstream):
    active = normed * gain_row
    sig = jax.nn.sigmoid(active)
    hidden = (active * sig).astype(NARROW)
    d_active = upstream * sig * (1.0 + active * (1.0 - sig))
    d_normed = d_active * gain_row
    gain_part = jnp.sum((d_active * normed).reshape(normed.shape[0] // 8, 8, LANES), 0)
    return hidden, factor * d_normed, factor * normed, d_normed, d_normed * normed, gain_part


def convolve(source, half, taps_wide, start, size):
    conv = jnp.zeros((size, LANES), WIDE)
    for tap in range(TAPS):
        begin = start + tap + EDGE - TAPS + 1
        conv = conv + taps_wide[tap : tap + 1, lanes(half)] * source[half, begin : begin + size]
    return conv


def column_sums(source):
    return jnp.sum(jnp.transpose(source), 0, keepdims=True)


def both_blocks(cotangent, place, near):
    far, core = place[0] // (2 * CLOSE), place[0] % 2
    low, high = OFFSETS[0][near], OFFSETS[1][near]
    own = lax.rem(far + jnp.where(core == 0, low, high) + FAR, FAR)
    theirs = lax.rem(far + jnp.where(core == 0, high, low) + FAR, FAR)
    columns = [pl.ds(pl.multiple_of(block * BLOCK, BLOCK), BLOCK) for block in (own, theirs)]
    return jnp.concatenate([cotangent[:, columns[0]], cotangent[:, columns[1]]], 1)


def forward(
    place, value, gate, cotangent, weight, far_taps, far_gain, far_mean, far_scale,
    gated, scaled, spread, sums, gain_part, first_upstream, first_cotangent, product,
    held_value, held_gate, held, held_weight, taps, gain, mean, scale, arrivals,
    taps_wide, mean_columns, scale_columns, sum_first, sum_second,
    hidden, normed, upstream,
):
    copies = [
        pltpu.make_async_copy(source, target, arrivals.at[i])
        for i, (source, target) in enumerate(
            (
                (value, held_value), (gate, held_gate), (far_taps, taps), (far_mean, mean),
                (far_scale, scale), (far_gain, gain), (weight, held_weight), (cotangent, held),
            )
        )
    ]
    for copy in copies:
        copy.start()
    sum_first[0:EDGE] = jnp.zeros((EDGE, LANES), WIDE)
    sum_second[0:EDGE] = jnp.zeros((EDGE, LANES), WIDE)
    hidden[0:EDGE] = jnp.zeros((EDGE, WIDTH), WIDE)
    for copy in copies[:6]:
        copy.wait()
    taps_wide[0:TAPS] = taps[...].astype(WIDE)
    for block in range(ROWS // LANES):
        rows = slice(block * LANES, (block + 1) * LANES)
        mean_columns[rows] = column(mean[rows].reshape(1, LANES))
        scale_columns[rows] = column(scale[rows].reshape(1, LANES))
    for half in range(HALVES):
        for start in range(0, ROWS, CHUNK):
            rows = slice(start, start + CHUNK)
            sig = jax.nn.sigmoid(held_gate[rows, lanes(half)].astype(WIDE))
            narrow = (held_value[rows, lanes(half)].astype(WIDE) * sig).astype(NARROW)
            gated[half, rows] = narrow.astype(WIDE)
        for start in range(EDGE, ROWS, EDGE):
            rows = slice(start, start + EDGE)
            conv = convolve(gated, half, taps_wide, start - EDGE, EDGE)
            normed[half, rows] = (conv - mean_columns[rows]) * scale_columns[rows]
    copies[6].wait()
    copies[7].wait()
    upstream[...] = lax.dot_general(
        held[...], held_weight[...], (((1,), (1,)), ((), ())), preferred_element_type=WIDE
    )
    first_upstream[...] = upstream[0:EDGE]
    first_cotangent[...] = held[0:EDGE]
    for half in range(HALVES):
        gain_row = gain[0:1, lanes(half)]
        gain_sum = jnp.zeros((8, LANES), WIDE)
        for start in range(EDGE, ROWS, EDGE):
            rows = slice(start, start + EDGE)
            narrow, own_scaled, own_spread, first, second, part = norm_backward(
                normed[half, rows], scale_columns[rows], gain_row, upstream[rows, lanes(half)]
            )
            hidden[rows, lanes(half)] = narrow.astype(WIDE)
            scaled[half, start - EDGE : start] = own_scaled
            spread[half, start - EDGE : start] = own_spread
            gain_sum = gain_sum + part
            if half == 0:
                sum_first[rows] = first
                sum_second[rows] = second
            else:
                sum_first[rows] = sum_first[rows] + first
                sum_second[rows] = sum_second[rows] + second
        gain_part[half] = gain_sum
    found = [
        column_sums(source[block * LANES : (block + 1) * LANES])
        for source in (sum_first, sum_second)
        for block in range(ROWS // LANES)
    ]
    sums[...] = jnp.concatenate([*found, jnp.zeros((2, LANES), WIDE)], 0)
    turned = jnp.transpose(hidden[...]).astype(NARROW)
    for near in range(CLOSE):
        product[near] = jnp.dot(
            turned, both_blocks(held, place, near), preferred_element_type=WIDE
        )


def head(
    halo, gated, upstream, taps, gain, mean, scale, sums, gain_part,
    scaled, spread, hidden, message, gain_total,
    padded, taps_wide, turned,
):
    taps_wide[0:TAPS] = taps[...].astype(WIDE)
    rows = slice(0, EDGE)
    mean_columns = column(mean[0:LANES].reshape(1, LANES))[rows]
    scale_columns = column(scale[0:LANES].reshape(1, LANES))[rows]
    turned[...] = jnp.zeros((2, LANES, LANES), WIDE)
    for half in range(HALVES):
        padded[half, rows] = halo[:, lanes(half)].astype(WIDE)
        padded[half, EDGE:] = gated[half, rows]
    for half in range(HALVES):
        conv = convolve(padded, half, taps_wide, 0, EDGE)
        normed = (conv - mean_columns) * scale_columns
        narrow, own_scaled, own_spread, first, second, part = norm_backward(
            normed, scale_columns, gain[0:1, lanes(half)], upstream[rows, lanes(half)]
        )
        hidden[:, lanes(half)] = narrow
        scaled[half] = own_scaled
        spread[half] = own_spread
        gain_total[half] = gain_part[half] + part
        turned[0, rows] = turned[0, rows] + first
        turned[1, rows] = turned[1, rows] + second
    blocks = ROWS // LANES
    total = sums[...]
    extra = [column_sums(turned[0]), column_sums(turned[1])]
    none = jnp.zeros((blocks - 1, LANES), WIDE)
    last = jnp.zeros((2, LANES), WIDE)
    total = total + jnp.concatenate([extra[0], none, extra[1], none, last], 0)
    for peer in range(TP):
        message[peer] = total


def head_product(cotangent, hidden, place, near, side):
    columns = both_blocks(cotangent, place, near)[:, side * BLOCK : (side + 1) * BLOCK]
    return lax.dot_general(
        hidden[...], columns, (((0,), (0,)), ((), ())), preferred_element_type=WIDE
    )


def backward(
    place, sums, scaled, spread, first_scaled, first_spread, halo, gated, scale, gain_part,
    first_cotangent, first_hidden, product,
    other, small, extended,
    joint,
):
    for half in range(HALVES):
        joint[half, 0:EDGE] = halo[:, lanes(half)].astype(WIDE)
        joint[half, EDGE:] = gated[half, 0:8]
    total = (sums[0] + sums[1]) + (sums[2] + sums[3])
    total = total * (1.0 / (TP * WIDTH))
    blocks = ROWS // LANES
    for half in range(HALVES):
        extended[half, 0:EDGE] = jnp.zeros((EDGE, LANES), WIDE)
        extended[half, EDGE + ROWS :] = jnp.zeros((EDGE, LANES), WIDE)
    for block in range(blocks):
        rows = slice(block * LANES, (block + 1) * LANES)
        first = column(total[block : block + 1] * scale[rows].reshape(1, LANES))
        second = column(total[blocks + block : blocks + block + 1])
        for half in range(HALVES):
            cut = 0
            if block == 0:
                cut = EDGE
                d_conv = first_scaled[half] - first[0:cut] - first_spread[half] * second[0:cut]
                extended[half, EDGE : EDGE + cut] = d_conv
            rows = slice(block * LANES + cut - EDGE, (block + 1) * LANES - EDGE)
            d_conv = scaled[half, rows] - first[cut:] - spread[half, rows] * second[cut:]
            extended[half, EDGE + block * LANES + cut : EDGE + (block + 1) * LANES] = d_conv
    lead = EDGE - TAPS + 1
    groups = ROWS // 8
    for offset in range(8):
        steps = [q for q in range(5) if 0 <= 8 * q + offset - lead < TAPS]
        found = {(half, q): jnp.zeros((8, LANES), WIDE) for half in range(HALVES) for q in steps}
        loaded = {}
        for m in range(groups + steps[-1]):
            for half in range(HALVES):
                if m < groups:
                    begin = EDGE + 8 * m
                    loaded[half, m] = extended[half, begin : begin + 8]
                begin = 8 * m + offset
                if begin < EDGE:
                    moved = joint[half, begin : begin + 8]
                else:
                    moved = gated[half, begin - EDGE : begin - EDGE + 8]
                for q in steps:
                    if 0 <= m - q < groups:
                        found[half, q] = found[half, q] + loaded[half, m - q] * moved
        for half in range(HALVES):
            for q in steps:
                tap = 8 * q + offset - lead
                small[tap : tap + 1, lanes(half)] = jnp.sum(found[half, q], 0, keepdims=True)
        near = offset
        whole = product[near, :, BLOCK:] + head_product(first_cotangent, first_hidden, place, near, 1)
        other[near * WIDTH : (near + 1) * WIDTH] = whole.astype(NARROW)
    for half in range(HALVES):
        small[TAPS:SMALL, lanes(half)] = jnp.sum(gain_part[half], 0, keepdims=True)
    for half in range(HALVES):
        value = small[:, lanes(half)]
        top = value.astype(NARROW)
        begin = CLOSE * WIDTH + half * 2 * SMALL
        other[begin : begin + SMALL] = top
        other[begin + SMALL : begin + 2 * SMALL] = (value - top.astype(WIDE)).astype(NARROW)


def pack(mine, small, other, pieces):
    for half in range(HALVES):
        begin = CLOSE * WIDTH + half * 2 * SMALL
        top = other[begin : begin + SMALL].astype(WIDE)
        rest = other[begin + SMALL : begin + 2 * SMALL].astype(WIDE)
        both = (small[:, lanes(half)] + (top + rest)).astype(NARROW)
        for near in range(CLOSE):
            pieces[near, WIDTH + half * SMALL : WIDTH + (half + 1) * SMALL] = both
    for near in range(CLOSE):
        for start in range(0, WIDTH, 64):
            rows = slice(start, start + 64)
            there = other[near * WIDTH + start : near * WIDTH + start + 64].astype(WIDE)
            pieces[near, rows] = (mine[near, rows] + there).astype(NARROW)


def gated_gradient(
    place, extended, taps, value, gate, first_cotangent, first_hidden, product,
    value_grad, gate_grad, margin, last, mine,
    taps_wide, held_value_grad, held_gate_grad, departures,
):
    taps_wide[0:TAPS] = taps[...].astype(WIDE)
    parts = []
    for start in range(0, EDGE + ROWS, EDGE):
        rows = slice(start - EDGE, start)
        for half in range(HALVES):
            found = jnp.zeros((EDGE, LANES), WIDE)
            for tap in range(TAPS):
                begin = start + TAPS - 1 - tap
                found = found + taps_wide[tap : tap + 1, lanes(half)] * extended[half, begin : begin + EDGE]
            if start == 0:
                margin[half] = found
                continue
            sig = jax.nn.sigmoid(gate[rows, lanes(half)].astype(WIDE))
            slope = value[rows, lanes(half)].astype(WIDE) * sig * (1.0 - sig)
            if start == ROWS:
                last[0, half], last[1, half], last[2, half] = found, sig, slope
            else:
                held_value_grad[rows, lanes(half)] = (found * sig).astype(NARROW)
                held_gate_grad[rows, lanes(half)] = (found * slope).astype(NARROW)
        if start in PART_ENDS:
            part = PART_ENDS.index(start)
            begin = PART_ENDS[part - 1] if part else 0
            sent = pl.ds(begin, start - begin)
            for i, (source, target) in enumerate(
                ((held_value_grad, value_grad), (held_gate_grad, gate_grad))
            ):
                parts.append(
                    pltpu.make_async_copy(
                        source.at[sent], target.at[sent], departures.at[2 * part + i]
                    )
                )
                parts[-1].start()
    for near in range(CLOSE):
        mine[near] = product[near, :, 0:BLOCK] + head_product(
            first_cotangent, first_hidden, place, near, 0
        )
    for part in parts:
        part.wait()


def fold_near(arrived, payload):
    for start in range(0, WIDTH + 2 * SMALL, 64):
        rows = slice(start, start + 64)
        total = arrived[0, rows].astype(WIDE)
        for near in range(1, CLOSE):
            total = total + arrived[near, rows].astype(WIDE)
        payload[rows] = total.astype(NARROW)


def hand_out(payload, message):
    weights = jnp.transpose(payload[0:WIDTH].astype(WIDE)).astype(NARROW)
    small = jnp.concatenate([payload[WIDTH : WIDTH + SMALL], payload[WIDTH + SMALL :]], 1)
    for position, member in enumerate(GATHER_ORDER):
        message[position, 0:OWN] = weights[member * OWN : (member + 1) * OWN]
        message[position, OWN:] = small


def totals(arrived, total):
    for start in range(0, OWN + SMALL, 8):
        rows = slice(start, start + 8)
        found = arrived[0, rows].astype(WIDE)
        for position in range(1, 2 * CLOSE):
            found = found + arrived[position, rows].astype(WIDE)
        total[rows] = found


def finish(
    value_part, gate_part, total, last, late,
    value_grad, gate_grad, weight_grad, taps_grad, gain_grad,
    held_value_grad, held_gate_grad, departures,
):
    del value_part, gate_part
    for half in range(HALVES):
        grad = last[0, half] + late[half]
        held_value_grad[:, lanes(half)] = (grad * last[1, half]).astype(NARROW)
        held_gate_grad[:, lanes(half)] = (grad * last[2, half]).astype(NARROW)
    rows = pl.ds(ROWS - EDGE, EDGE)
    copies = [
        pltpu.make_async_copy(held_value_grad, value_grad.at[rows], departures.at[0]),
        pltpu.make_async_copy(held_gate_grad, gate_grad.at[rows], departures.at[1]),
    ]
    for copy in copies:
        copy.start()
    weight_grad[...] = total[0:OWN]
    taps_grad[...] = total[OWN : OWN + TAPS]
    gain_grad[...] = total[OWN + TAPS :]
    for copy in copies:
        copy.wait()


def to_block(value):
    pairs = []
    for far in range(FAR):
        for near in range(CLOSE):
            for core in range(2):
                target = (far + OFFSETS[core][near]) % FAR
                pairs.append(((far * CLOSE + near) * 2 + core, (target * CLOSE + near) * 2 + core))
    return lax.ppermute(value, SP, pairs)


def shards(
    proj_value, proj_gate, out_cotangent, out_weight, conv_taps, norm_gain, row_mean, row_scale
):
    end_gate = jax.nn.sigmoid(proj_gate[ROWS - EDGE :].astype(WIDE))
    end = (proj_value[ROWS - EDGE :].astype(WIDE) * end_gate).astype(NARROW)
    halo = shifted(end, SP, 1)
    split = (HALVES, ROWS, LANES)
    rest = (HALVES, ROWS - EDGE, LANES)
    row_gain = norm_gain.reshape(1, WIDTH)
    sides = pltpu.VMEM((HALVES, EDGE + ROWS, LANES), WIDE)
    taps_scratch = pltpu.VMEM((TAPS + 1, WIDTH), WIDE)
    place = lax.axis_index(SP).reshape(1)
    narrow = ((ROWS, WIDTH), NARROW)
    gated, scaled, spread, sums, gain_part, first_upstream, first_cotangent, product = (
        scalar_call(
            forward,
            [
                (split, WIDE), (rest, WIDE), (rest, WIDE), ((8, LANES), WIDE),
                ((HALVES, 8, LANES), WIDE), ((EDGE, WIDTH), WIDE), ((EDGE, MODEL), NARROW),
                ((CLOSE, WIDTH, 2 * BLOCK), WIDE),
            ],
            place, proj_value, proj_gate, out_cotangent, out_weight,
            conv_taps, row_gain, row_mean, row_scale, in_hbm=8,
            scratch=[
                pltpu.VMEM(*narrow), pltpu.VMEM(*narrow), pltpu.VMEM((ROWS, MODEL), NARROW),
                pltpu.VMEM((WIDTH, MODEL), NARROW), pltpu.VMEM((TAPS, WIDTH), NARROW),
                pltpu.VMEM((1, WIDTH), WIDE), pltpu.VMEM((ROWS,), WIDE),
                pltpu.VMEM((ROWS,), WIDE), pltpu.SemaphoreType.DMA((8,)),
                taps_scratch, *([pltpu.VMEM((ROWS, LANES), WIDE)] * 4),
                pltpu.VMEM((ROWS, WIDTH), WIDE), pltpu.VMEM(split, WIDE),
                pltpu.VMEM((ROWS, WIDTH), WIDE),
            ],
            flops=4 * ROWS * WIDTH * MODEL, limit=12,
        )
    )
    edge = (HALVES, EDGE, LANES)
    first_scaled, first_spread, first_hidden, message, gain_part = call_with(
        head,
        [
            (edge, WIDE), (edge, WIDE), ((EDGE, WIDTH), NARROW),
            ((TP, 8, LANES), WIDE), ((HALVES, 8, LANES), WIDE),
        ],
        [
            pltpu.VMEM((HALVES, 2 * EDGE, LANES), WIDE),
            taps_scratch,
            pltpu.VMEM((2, LANES, LANES), WIDE),
        ],
        halo, gated, first_upstream, conv_taps, row_gain, row_mean, row_scale, sums,
        gain_part, flops=10 * ROWS * WIDTH,
    )
    sums = exchange(message, "tp", SUMS_ORDER)
    rows = CLOSE * WIDTH + 4 * SMALL
    other, small, extended = scalar_call(
        backward,
        [
            ((rows, BLOCK), NARROW), ((SMALL, WIDTH), WIDE),
            ((HALVES, ROWS + 2 * EDGE, LANES), WIDE),
        ],
        place, sums, scaled, spread, first_scaled, first_spread, halo, gated, row_scale,
        gain_part, first_cotangent, first_hidden, product,
        scratch=[pltpu.VMEM((HALVES, EDGE + 8, LANES), WIDE)], flops=100 * ROWS * WIDTH,
    )
    other = lax.ppermute(other, "c", [(0, 1), (1, 0)])
    value_grad, gate_grad, margin, last, mine = scalar_call(
        gated_gradient,
        [
            narrow, narrow, (edge, WIDE), ((3, *edge), WIDE),
            ((CLOSE, WIDTH, BLOCK), WIDE),
        ],
        place, extended, conv_taps, proj_value, proj_gate,
        first_cotangent, first_hidden, product, outs_in_hbm=2,
        scratch=[
            taps_scratch, pltpu.VMEM(*narrow), pltpu.VMEM(*narrow),
            pltpu.SemaphoreType.DMA((2 * len(PART_ENDS),)),
        ],
        flops=100 * ROWS * WIDTH,
    )
    (pieces,) = call(
        pack, [((CLOSE, WIDTH + 2 * SMALL, BLOCK), NARROW)], mine, small, other, flops=1 << 20
    )
    arrived = exchange(pieces, NEAR)
    (payload,) = call(
        fold_near, [((WIDTH + 2 * SMALL, BLOCK), NARROW)], arrived, flops=1 << 20
    )
    payload = to_block(payload)
    late = shifted(margin, SP, -1)
    (message,) = call(hand_out, [((2 * CLOSE, OWN + SMALL, WIDTH), NARROW)], payload, flops=1 << 16)
    arrived = exchange(message, (*NEAR, "c"), GATHER_ORDER)
    (total,) = call(totals, [((OWN + SMALL, WIDTH), WIDE)], arrived, flops=1 << 20)
    value_grad, gate_grad, weight_grad, taps_grad, gain_grad = last_call(
        [narrow, narrow, ((OWN, WIDTH), WIDE), ((TAPS, WIDTH), WIDE), ((1, WIDTH), WIDE)],
        value_grad, gate_grad, total, last, late,
    )
    return (value_grad, gate_grad, weight_grad, taps_grad, gain_grad.reshape(WIDTH))


def call_with(body, outs, scratch, *args, flops=0, limit=6):
    shapes = [jax.ShapeDtypeStruct(shape, dtype) for shape, dtype in outs]
    size = sum(a.size * a.dtype.itemsize for a in (*args, *shapes))
    return pl.pallas_call(
        body,
        out_shape=shapes,
        scratch_shapes=scratch,
        compiler_params=pltpu.CompilerParams(vmem_limit_bytes=limit << 20),
        cost_estimate=pl.CostEstimate(flops=flops, bytes_accessed=size, transcendentals=0),
    )(*args)


def scalar_call(
    body, outs, scalar, *args, scratch=(), flops=1 << 20, limit=6, in_hbm=0, outs_in_hbm=0
):
    shapes = [jax.ShapeDtypeStruct(shape, dtype) for shape, dtype in outs]
    placed = [pltpu.HBM(*out) for out in outs[:outs_in_hbm]] + shapes[outs_in_hbm:]
    size = sum(a.size * a.dtype.itemsize for a in (*args, *shapes))
    whole = pl.BlockSpec(memory_space=pltpu.VMEM)
    far = [pltpu.with_memory_space_constraint(a, pltpu.HBM) for a in args[:in_hbm]]
    return pl.pallas_call(
        body,
        out_shape=placed,
        in_specs=[
            pl.BlockSpec(memory_space=pltpu.SMEM),
            *([pl.BlockSpec(memory_space=pltpu.HBM)] * in_hbm),
            *([whole] * (len(args) - in_hbm)),
        ],
        out_specs=[
            *([pl.BlockSpec(memory_space=pltpu.HBM)] * outs_in_hbm),
            *([whole] * (len(shapes) - outs_in_hbm)),
        ],
        scratch_shapes=scratch,
        compiler_params=pltpu.CompilerParams(vmem_limit_bytes=limit << 20),
        cost_estimate=pl.CostEstimate(flops=flops, bytes_accessed=size, transcendentals=0),
    )(scalar, *far, *args[in_hbm:])


def last_call(outs, *args):
    shapes = [jax.ShapeDtypeStruct(shape, dtype) for shape, dtype in outs]
    far, whole = pl.BlockSpec(memory_space=pltpu.HBM), pl.BlockSpec(memory_space=pltpu.VMEM)
    edge = pltpu.VMEM((EDGE, WIDTH), NARROW)
    held = [pltpu.with_memory_space_constraint(a, pltpu.HBM) for a in args[:2]]
    return pl.pallas_call(
        finish,
        out_shape=[*(pltpu.HBM(*out) for out in outs[:2]), *shapes[2:]],
        in_specs=[far, far, whole, whole, whole],
        out_specs=[far, far, whole, whole, whole],
        scratch_shapes=[edge, edge, pltpu.SemaphoreType.DMA((2,))],
        input_output_aliases={0: 0, 1: 1},
        compiler_params=pltpu.CompilerParams(vmem_limit_bytes=6 << 20),
        cost_estimate=pl.CostEstimate(flops=1 << 16, bytes_accessed=1 << 18, transcendentals=0),
        name="finish",
    )(*held, *args[2:])


def solution(mesh):
    sizes = [size for _, size in AXES]
    split = Mesh(mesh.devices.reshape(*sizes, mesh.shape["tp"]), (*SP, "tp"))
    placed = (
        P(SP, "tp"),
        P(SP, "tp"),
        P(SP, None),
        P("tp", None),
        P(None, "tp"),
        P("tp"),
        P(SP),
        P(SP),
    )
    return jax.shard_map(
        shards,
        mesh=split,
        in_specs=placed,
        out_specs=(P(SP, "tp"), P(SP, "tp"), P(SP, "tp"), P(None, "tp"), P("tp")),
        check_vma=False,
    )
```

```python
import jax
import jax.numpy as jnp
from jax import lax
from jax.experimental import pallas as pl
from jax.experimental.pallas import tpu as pltpu
from jax.sharding import Mesh
from jax.sharding import PartitionSpec as P


SP = ("zh", "zl", "x", "c")
NEAR = ("zl", "x")
FAR = 16
CLOSE = 8
AXES = (("zh", FAR), ("zl", 2), ("x", 4), ("c", 2))
TP = 4
SUMS_ORDER = [3, 0, 1, 2]
OFFSETS = ((0, -1, -2, -3, 3, 2, 1, -4), (6, 7, 8, 5, -7, -6, -5, 4))
BLOCK = CLOSE * 2 * 8
GATHER_ORDER = [(place + 1) % (2 * CLOSE) for place in range(2 * CLOSE)]
TAPS = 31
SMALL = TAPS + 1
ROWS = 384
EDGE = 32
LANES = 128
HALVES = 2
WIDTH = HALVES * LANES
MODEL = 2048
OWN = 8
CHUNK = 64
WIDE = jnp.float32
NARROW = jnp.bfloat16


def shifted(value, axis, steps):
    count = lax.axis_size(axis)
    first, last = (max(0, -steps), min(count, count - steps))
    return lax.ppermute(value, axis, [(source, source + steps) for source in range(first, last)])


def exchange(pieces, axes, order=None):
    groups = order and [order]
    return lax.all_to_all(pieces, axes, 0, 0, tiled=True, axis_index_groups=groups)


def lanes(half):
    return slice(half * LANES, (half + 1) * LANES)


def column(row):
    return jnp.transpose(jnp.broadcast_to(row, (LANES, LANES)))


def call(body, outs, *args, flops=0, limit=6):
    shapes = [jax.ShapeDtypeStruct(shape, dtype) for shape, dtype in outs]
    size = sum(a.size * a.dtype.itemsize for a in (*args, *shapes))
    return pl.pallas_call(
        body,
        out_shape=shapes,
        compiler_params=pltpu.CompilerParams(vmem_limit_bytes=limit << 20),
        cost_estimate=pl.CostEstimate(flops=flops, bytes_accessed=size, transcendentals=0),
    )(*args)


def norm_backward(normed, factor, gain_row, upstream):
    active = normed * gain_row
    sig = jax.nn.sigmoid(active)
    hidden = (active * sig).astype(NARROW)
    d_active = upstream * sig * (1.0 + active * (1.0 - sig))
    d_normed = d_active * gain_row
    gain_part = jnp.sum((d_active * normed).reshape(normed.shape[0] // 8, 8, LANES), 0)
    return hidden, factor * d_normed, factor * normed, d_normed, d_normed * normed, gain_part


def convolve(source, half, taps_wide, start, size):
    conv = jnp.zeros((size, LANES), WIDE)
    for tap in range(TAPS):
        begin = start + tap + EDGE - TAPS + 1
        conv = conv + taps_wide[tap : tap + 1, lanes(half)] * source[half, begin : begin + size]
    return conv


def column_sums(source):
    return jnp.sum(jnp.transpose(source), 0, keepdims=True)


def both_blocks(cotangent, place, near):
    far, core = place[0] // (2 * CLOSE), place[0] % 2
    low, high = OFFSETS[0][near], OFFSETS[1][near]
    own = lax.rem(far + jnp.where(core == 0, low, high) + FAR, FAR)
    theirs = lax.rem(far + jnp.where(core == 0, high, low) + FAR, FAR)
    columns = [pl.ds(pl.multiple_of(block * BLOCK, BLOCK), BLOCK) for block in (own, theirs)]
    return jnp.concatenate([cotangent[:, columns[0]], cotangent[:, columns[1]]], 1)


def forward(
    place, value, gate, cotangent, weight, far_taps, far_gain, far_mean, far_scale,
    gated, scaled, spread, sums, gain_part, first_upstream, first_cotangent, product,
    held_value, held_gate, held, held_weight, taps, gain, mean, scale, arrivals,
    padded, taps_wide, mean_columns, scale_columns, sum_first, sum_second,
    hidden, normed, upstream,
):
    copies = [
        pltpu.make_async_copy(source, target, arrivals.at[i])
        for i, (source, target) in enumerate(
            (
                (value, held_value), (gate, held_gate), (far_taps, taps), (far_mean, mean),
                (far_scale, scale), (far_gain, gain), (weight, held_weight), (cotangent, held),
            )
        )
    ]
    for copy in copies:
        copy.start()
    sum_first[0:EDGE] = jnp.zeros((EDGE, LANES), WIDE)
    sum_second[0:EDGE] = jnp.zeros((EDGE, LANES), WIDE)
    hidden[0:EDGE] = jnp.zeros((EDGE, WIDTH), WIDE)
    for copy in copies[:6]:
        copy.wait()
    taps_wide[0:TAPS] = taps[...].astype(WIDE)
    for block in range(ROWS // LANES):
        rows = slice(block * LANES, (block + 1) * LANES)
        mean_columns[rows] = column(mean[rows].reshape(1, LANES))
        scale_columns[rows] = column(scale[rows].reshape(1, LANES))
    for half in range(HALVES):
        for start in range(0, ROWS, CHUNK):
            rows = slice(start, start + CHUNK)
            sig = jax.nn.sigmoid(held_gate[rows, lanes(half)].astype(WIDE))
            narrow = (held_value[rows, lanes(half)].astype(WIDE) * sig).astype(NARROW)
            gated[rows, lanes(half)] = narrow
            padded[half, EDGE + start : EDGE + start + CHUNK] = narrow.astype(WIDE)
        for start in range(EDGE, ROWS, EDGE):
            rows = slice(start, start + EDGE)
            conv = convolve(padded, half, taps_wide, start, EDGE)
            normed[half, rows] = (conv - mean_columns[rows]) * scale_columns[rows]
    copies[6].wait()
    copies[7].wait()
    upstream[...] = lax.dot_general(
        held[...], held_weight[...], (((1,), (1,)), ((), ())), preferred_element_type=WIDE
    )
    first_upstream[...] = upstream[0:EDGE]
    first_cotangent[...] = held[0:EDGE]
    for half in range(HALVES):
        gain_row = gain[0:1, lanes(half)]
        gain_sum = jnp.zeros((8, LANES), WIDE)
        for start in range(EDGE, ROWS, EDGE):
            rows = slice(start, start + EDGE)
            narrow, own_scaled, own_spread, first, second, part = norm_backward(
                normed[half, rows], scale_columns[rows], gain_row, upstream[rows, lanes(half)]
            )
            hidden[rows, lanes(half)] = narrow.astype(WIDE)
            scaled[half, start - EDGE : start] = own_scaled
            spread[half, start - EDGE : start] = own_spread
            gain_sum = gain_sum + part
            if half == 0:
                sum_first[rows] = first
                sum_second[rows] = second
            else:
                sum_first[rows] = sum_first[rows] + first
                sum_second[rows] = sum_second[rows] + second
        gain_part[half] = gain_sum
    found = [
        column_sums(source[block * LANES : (block + 1) * LANES])
        for source in (sum_first, sum_second)
        for block in range(ROWS // LANES)
    ]
    sums[...] = jnp.concatenate([*found, jnp.zeros((2, LANES), WIDE)], 0)
    turned = jnp.transpose(hidden[...]).astype(NARROW)
    for near in range(CLOSE):
        product[near] = jnp.dot(
            turned, both_blocks(held, place, near), preferred_element_type=WIDE
        )


def head(
    halo, gated, upstream, taps, gain, mean, scale, sums, gain_part,
    scaled, spread, hidden, message, gain_total,
    padded, taps_wide, turned,
):
    taps_wide[0:TAPS] = taps[...].astype(WIDE)
    rows = slice(0, EDGE)
    mean_columns = column(mean[0:LANES].reshape(1, LANES))[rows]
    scale_columns = column(scale[0:LANES].reshape(1, LANES))[rows]
    turned[...] = jnp.zeros((2, LANES, LANES), WIDE)
    for half in range(HALVES):
        padded[half, rows] = halo[:, lanes(half)].astype(WIDE)
        padded[half, EDGE:] = gated[rows, lanes(half)].astype(WIDE)
    for half in range(HALVES):
        conv = convolve(padded, half, taps_wide, 0, EDGE)
        normed = (conv - mean_columns) * scale_columns
        narrow, own_scaled, own_spread, first, second, part = norm_backward(
            normed, scale_columns, gain[0:1, lanes(half)], upstream[rows, lanes(half)]
        )
        hidden[:, lanes(half)] = narrow
        scaled[half] = own_scaled
        spread[half] = own_spread
        gain_total[half] = gain_part[half] + part
        turned[0, rows] = turned[0, rows] + first
        turned[1, rows] = turned[1, rows] + second
    blocks = ROWS // LANES
    total = sums[...]
    extra = [column_sums(turned[0]), column_sums(turned[1])]
    none = jnp.zeros((blocks - 1, LANES), WIDE)
    last = jnp.zeros((2, LANES), WIDE)
    total = total + jnp.concatenate([extra[0], none, extra[1], none, last], 0)
    for peer in range(TP):
        message[peer] = total


def backward(
    place, sums, scaled, spread, first_scaled, first_spread, halo, gated, scale, gain_part,
    first_cotangent, first_hidden, product,
    mine, other, small, extended,
    padded,
):
    for half in range(HALVES):
        padded[half, 0:EDGE] = halo[:, lanes(half)].astype(WIDE)
        padded[half, EDGE:] = gated[:, lanes(half)].astype(WIDE)
    total = (sums[0] + sums[1]) + (sums[2] + sums[3])
    total = total * (1.0 / (TP * WIDTH))
    blocks = ROWS // LANES
    for half in range(HALVES):
        extended[half, 0:EDGE] = jnp.zeros((EDGE, LANES), WIDE)
        extended[half, EDGE + ROWS :] = jnp.zeros((EDGE, LANES), WIDE)
    for block in range(blocks):
        rows = slice(block * LANES, (block + 1) * LANES)
        first = column(total[block : block + 1] * scale[rows].reshape(1, LANES))
        second = column(total[blocks + block : blocks + block + 1])
        for half in range(HALVES):
            cut = 0
            if block == 0:
                cut = EDGE
                d_conv = first_scaled[half] - first[0:cut] - first_spread[half] * second[0:cut]
                extended[half, EDGE : EDGE + cut] = d_conv
            rows = slice(block * LANES + cut - EDGE, (block + 1) * LANES - EDGE)
            d_conv = scaled[half, rows] - first[cut:] - spread[half, rows] * second[cut:]
            extended[half, EDGE + block * LANES + cut : EDGE + (block + 1) * LANES] = d_conv
    lead = EDGE - TAPS + 1
    groups = ROWS // 8
    for offset in range(8):
        steps = [q for q in range(5) if 0 <= 8 * q + offset - lead < TAPS]
        found = {(half, q): jnp.zeros((8, LANES), WIDE) for half in range(HALVES) for q in steps}
        loaded = {}
        for m in range(groups + steps[-1]):
            for half in range(HALVES):
                if m < groups:
                    begin = EDGE + 8 * m
                    loaded[half, m] = extended[half, begin : begin + 8]
                moved = padded[half, 8 * m + offset : 8 * m + offset + 8]
                for q in steps:
                    if 0 <= m - q < groups:
                        found[half, q] = found[half, q] + loaded[half, m - q] * moved
        for half in range(HALVES):
            for q in steps:
                tap = 8 * q + offset - lead
                small[tap : tap + 1, lanes(half)] = jnp.sum(found[half, q], 0, keepdims=True)
        near = offset
        whole = product[near] + lax.dot_general(
            first_hidden[...], both_blocks(first_cotangent, place, near),
            (((0,), (0,)), ((), ())), preferred_element_type=WIDE,
        )
        mine[near] = whole[:, 0:BLOCK]
        other[near * WIDTH : (near + 1) * WIDTH] = whole[:, BLOCK:].astype(NARROW)
    for half in range(HALVES):
        small[TAPS:SMALL, lanes(half)] = jnp.sum(gain_part[half], 0, keepdims=True)
    for half in range(HALVES):
        value = small[:, lanes(half)]
        top = value.astype(NARROW)
        begin = CLOSE * WIDTH + half * 2 * SMALL
        other[begin : begin + SMALL] = top
        other[begin + SMALL : begin + 2 * SMALL] = (value - top.astype(WIDE)).astype(NARROW)


def pack(mine, small, other, pieces):
    for half in range(HALVES):
        begin = CLOSE * WIDTH + half * 2 * SMALL
        top = other[begin : begin + SMALL].astype(WIDE)
        rest = other[begin + SMALL : begin + 2 * SMALL].astype(WIDE)
        both = (small[:, lanes(half)] + (top + rest)).astype(NARROW)
        for near in range(CLOSE):
            pieces[near, WIDTH + half * SMALL : WIDTH + (half + 1) * SMALL] = both
    for near in range(CLOSE):
        for start in range(0, WIDTH, 64):
            rows = slice(start, start + 64)
            there = other[near * WIDTH + start : near * WIDTH + start + 64].astype(WIDE)
            pieces[near, rows] = (mine[near, rows] + there).astype(NARROW)


def gated_gradient(extended, taps, d_gated, margin, taps_wide):
    taps_wide[0:TAPS] = taps[...].astype(WIDE)
    for half in range(HALVES):
        for start in range(0, EDGE + ROWS, EDGE):
            found = jnp.zeros((EDGE, LANES), WIDE)
            for tap in range(TAPS):
                begin = start + TAPS - 1 - tap
                found = found + taps_wide[tap : tap + 1, lanes(half)] * extended[half, begin : begin + EDGE]
            if start == 0:
                margin[half] = found
            else:
                d_gated[half, start - EDGE : start] = found


def fold_near(arrived, payload):
    for start in range(0, WIDTH + 2 * SMALL, 64):
        rows = slice(start, start + 64)
        total = arrived[0, rows].astype(WIDE)
        for near in range(1, CLOSE):
            total = total + arrived[near, rows].astype(WIDE)
        payload[rows] = total.astype(NARROW)


def hand_out(payload, message):
    weights = jnp.transpose(payload[0:WIDTH].astype(WIDE)).astype(NARROW)
    small = jnp.concatenate([payload[WIDTH : WIDTH + SMALL], payload[WIDTH + SMALL :]], 1)
    for position, member in enumerate(GATHER_ORDER):
        message[position, 0:OWN] = weights[member * OWN : (member + 1) * OWN]
        message[position, OWN:] = small


def totals(arrived, total):
    for start in range(0, OWN + SMALL, 8):
        rows = slice(start, start + 8)
        found = arrived[0, rows].astype(WIDE)
        for position in range(1, 2 * CLOSE):
            found = found + arrived[position, rows].astype(WIDE)
        total[rows] = found


def finish(
    total, d_gated, late, value, gate,
    value_grad, gate_grad, weight_grad, taps_grad, gain_grad,
):
    for half in range(HALVES):
        for start in range(0, ROWS, EDGE):
            rows = slice(start, start + EDGE)
            grad = d_gated[half, rows]
            if start == ROWS - EDGE:
                grad = grad + late[half]
            sig = jax.nn.sigmoid(gate[rows, lanes(half)].astype(WIDE))
            wide = value[rows, lanes(half)].astype(WIDE)
            value_grad[rows, lanes(half)] = (grad * sig).astype(NARROW)
            gate_grad[rows, lanes(half)] = (grad * wide * sig * (1.0 - sig)).astype(NARROW)
    weight_grad[...] = total[0:OWN]
    taps_grad[...] = total[OWN : OWN + TAPS]
    gain_grad[...] = total[OWN + TAPS :]


def to_block(value):
    pairs = []
    for far in range(FAR):
        for near in range(CLOSE):
            for core in range(2):
                target = (far + OFFSETS[core][near]) % FAR
                pairs.append(((far * CLOSE + near) * 2 + core, (target * CLOSE + near) * 2 + core))
    return lax.ppermute(value, SP, pairs)


def shards(
    proj_value, proj_gate, out_cotangent, out_weight, conv_taps, norm_gain, row_mean, row_scale
):
    end_gate = jax.nn.sigmoid(proj_gate[ROWS - EDGE :].astype(WIDE))
    end = (proj_value[ROWS - EDGE :].astype(WIDE) * end_gate).astype(NARROW)
    halo = shifted(end, SP, 1)
    split = (HALVES, ROWS, LANES)
    rest = (HALVES, ROWS - EDGE, LANES)
    row_gain = norm_gain.reshape(1, WIDTH)
    sides = pltpu.VMEM((HALVES, EDGE + ROWS, LANES), WIDE)
    taps_scratch = pltpu.VMEM((TAPS + 1, WIDTH), WIDE)
    place = lax.axis_index(SP).reshape(1)
    narrow = ((ROWS, WIDTH), NARROW)
    gated, scaled, spread, sums, gain_part, first_upstream, first_cotangent, product = (
        scalar_call(
            forward,
            [
                narrow, (rest, WIDE), (rest, WIDE), ((8, LANES), WIDE),
                ((HALVES, 8, LANES), WIDE), ((EDGE, WIDTH), WIDE), ((EDGE, MODEL), NARROW),
                ((CLOSE, WIDTH, 2 * BLOCK), WIDE),
            ],
            place, proj_value, proj_gate, out_cotangent, out_weight,
            conv_taps, row_gain, row_mean, row_scale, in_hbm=8,
            scratch=[
                pltpu.VMEM(*narrow), pltpu.VMEM(*narrow), pltpu.VMEM((ROWS, MODEL), NARROW),
                pltpu.VMEM((WIDTH, MODEL), NARROW), pltpu.VMEM((TAPS, WIDTH), NARROW),
                pltpu.VMEM((1, WIDTH), WIDE), pltpu.VMEM((ROWS,), WIDE),
                pltpu.VMEM((ROWS,), WIDE), pltpu.SemaphoreType.DMA((8,)),
                sides, taps_scratch, *([pltpu.VMEM((ROWS, LANES), WIDE)] * 4),
                pltpu.VMEM((ROWS, WIDTH), WIDE), pltpu.VMEM(split, WIDE),
                pltpu.VMEM((ROWS, WIDTH), WIDE),
            ],
            flops=4 * ROWS * WIDTH * MODEL, limit=12,
        )
    )
    edge = (HALVES, EDGE, LANES)
    first_scaled, first_spread, first_hidden, message, gain_part = call_with(
        head,
        [
            (edge, WIDE), (edge, WIDE), ((EDGE, WIDTH), NARROW),
            ((TP, 8, LANES), WIDE), ((HALVES, 8, LANES), WIDE),
        ],
        [
            pltpu.VMEM((HALVES, 2 * EDGE, LANES), WIDE),
            taps_scratch,
            pltpu.VMEM((2, LANES, LANES), WIDE),
        ],
        halo, gated, first_upstream, conv_taps, row_gain, row_mean, row_scale, sums,
        gain_part, flops=10 * ROWS * WIDTH,
    )
    sums = exchange(message, "tp", SUMS_ORDER)
    rows = CLOSE * WIDTH + 4 * SMALL
    mine, other, small, extended = scalar_call(
        backward,
        [
            ((CLOSE, WIDTH, BLOCK), WIDE), ((rows, BLOCK), NARROW), ((SMALL, WIDTH), WIDE),
            ((HALVES, ROWS + 2 * EDGE, LANES), WIDE),
        ],
        place, sums, scaled, spread, first_scaled, first_spread, halo, gated, row_scale, gain_part,
        first_cotangent, first_hidden, product, scratch=[sides], flops=100 * ROWS * WIDTH,
    )
    other = lax.ppermute(other, "c", [(0, 1), (1, 0)])
    d_gated, margin = call_with(
        gated_gradient, [(split, WIDE), ((HALVES, EDGE, LANES), WIDE)], [taps_scratch],
        extended, conv_taps, flops=100 * ROWS * WIDTH,
    )
    (pieces,) = call(
        pack, [((CLOSE, WIDTH + 2 * SMALL, BLOCK), NARROW)], mine, small, other, flops=1 << 20
    )
    arrived = exchange(pieces, NEAR)
    (payload,) = call(
        fold_near, [((WIDTH + 2 * SMALL, BLOCK), NARROW)], arrived, flops=1 << 20
    )
    payload = to_block(payload)
    late = shifted(margin, SP, -1)
    (message,) = call(hand_out, [((2 * CLOSE, OWN + SMALL, WIDTH), NARROW)], payload, flops=1 << 16)
    arrived = exchange(message, (*NEAR, "c"), GATHER_ORDER)
    (total,) = call(totals, [((OWN + SMALL, WIDTH), WIDE)], arrived, flops=1 << 20)
    value_grad, gate_grad, weight_grad, taps_grad, gain_grad = call(
        finish,
        [narrow, narrow, ((OWN, WIDTH), WIDE), ((TAPS, WIDTH), WIDE), ((1, WIDTH), WIDE)],
        total, d_gated, late, proj_value, proj_gate, flops=10 * ROWS * WIDTH,
    )
    return (value_grad, gate_grad, weight_grad, taps_grad, gain_grad.reshape(WIDTH))


def call_with(body, outs, scratch, *args, flops=0, limit=6):
    shapes = [jax.ShapeDtypeStruct(shape, dtype) for shape, dtype in outs]
    size = sum(a.size * a.dtype.itemsize for a in (*args, *shapes))
    return pl.pallas_call(
        body,
        out_shape=shapes,
        scratch_shapes=scratch,
        compiler_params=pltpu.CompilerParams(vmem_limit_bytes=limit << 20),
        cost_estimate=pl.CostEstimate(flops=flops, bytes_accessed=size, transcendentals=0),
    )(*args)


def scalar_call(
    body, outs, scalar, *args, scratch=(), flops=1 << 20, limit=6, in_hbm=0
):
    shapes = [jax.ShapeDtypeStruct(shape, dtype) for shape, dtype in outs]
    size = sum(a.size * a.dtype.itemsize for a in (*args, *shapes))
    whole = pl.BlockSpec(memory_space=pltpu.VMEM)
    far = [pltpu.with_memory_space_constraint(a, pltpu.HBM) for a in args[:in_hbm]]
    return pl.pallas_call(
        body,
        out_shape=shapes,
        in_specs=[
            pl.BlockSpec(memory_space=pltpu.SMEM),
            *([pl.BlockSpec(memory_space=pltpu.HBM)] * in_hbm),
            *([whole] * (len(args) - in_hbm)),
        ],
        out_specs=[whole] * len(shapes),
        scratch_shapes=scratch,
        compiler_params=pltpu.CompilerParams(vmem_limit_bytes=limit << 20),
        cost_estimate=pl.CostEstimate(flops=flops, bytes_accessed=size, transcendentals=0),
    )(scalar, *far, *args[in_hbm:])


def solution(mesh):
    sizes = [size for _, size in AXES]
    split = Mesh(mesh.devices.reshape(*sizes, mesh.shape["tp"]), (*SP, "tp"))
    placed = (
        P(SP, "tp"),
        P(SP, "tp"),
        P(SP, None),
        P("tp", None),
        P(None, "tp"),
        P("tp"),
        P(SP),
        P(SP),
    )
    return jax.shard_map(
        shards,
        mesh=split,
        in_specs=placed,
        out_specs=(P(SP, "tp"), P(SP, "tp"), P(SP, "tp"), P(None, "tp"), P("tp")),
        check_vma=False,
    )
```

```python
import jax
import jax.numpy as jnp
from jax import lax
from jax.experimental import pallas as pl
from jax.experimental.pallas import tpu as pltpu
from jax.sharding import Mesh
from jax.sharding import PartitionSpec as P


SP = ("zh", "zl", "x", "c")
NEAR = ("zl", "x")
FAR = 16
CLOSE = 8
AXES = (("zh", FAR), ("zl", 2), ("x", 4), ("c", 2))
TP = 4
SUMS_ORDER = [3, 0, 1, 2]
OFFSETS = ((0, -1, -2, -3, 3, 2, 1, -4), (6, 7, 8, 5, -7, -6, -5, 4))
BLOCK = CLOSE * 2 * 8
GATHER_ORDER = [(place + 7) % (2 * CLOSE) for place in range(2 * CLOSE)]
TAPS = 31
SMALL = TAPS + 1
ROWS = 384
EDGE = 32
LANES = 128
HALVES = 2
WIDTH = HALVES * LANES
MODEL = 2048
OWN = 8
CHUNK = 64
WIDE = jnp.float32
NARROW = jnp.bfloat16


def shifted(value, axis, steps):
    count = lax.axis_size(axis)
    first, last = (max(0, -steps), min(count, count - steps))
    return lax.ppermute(value, axis, [(source, source + steps) for source in range(first, last)])


def exchange(pieces, axes, order=None):
    groups = order and [order]
    return lax.all_to_all(pieces, axes, 0, 0, tiled=True, axis_index_groups=groups)


def lanes(half):
    return slice(half * LANES, (half + 1) * LANES)


def column(row):
    return jnp.transpose(jnp.broadcast_to(row, (LANES, LANES)))


def call(body, outs, *args, flops=0, limit=6):
    shapes = [jax.ShapeDtypeStruct(shape, dtype) for shape, dtype in outs]
    size = sum(a.size * a.dtype.itemsize for a in (*args, *shapes))
    return pl.pallas_call(
        body,
        out_shape=shapes,
        compiler_params=pltpu.CompilerParams(vmem_limit_bytes=limit << 20),
        cost_estimate=pl.CostEstimate(flops=flops, bytes_accessed=size, transcendentals=0),
    )(*args)


def norm_backward(normed, factor, gain_row, upstream):
    active = normed * gain_row
    sig = jax.nn.sigmoid(active)
    hidden = (active * sig).astype(NARROW)
    d_active = upstream * sig * (1.0 + active * (1.0 - sig))
    d_normed = d_active * gain_row
    gain_part = jnp.sum((d_active * normed).reshape(normed.shape[0] // 8, 8, LANES), 0)
    return hidden, factor * d_normed, factor * normed, d_normed, d_normed * normed, gain_part


def convolve(source, half, taps_wide, start, size):
    conv = jnp.zeros((size, LANES), WIDE)
    for tap in range(TAPS):
        begin = start + tap + EDGE - TAPS + 1
        conv = conv + taps_wide[tap : tap + 1, lanes(half)] * source[half, begin : begin + size]
    return conv


def column_sums(source):
    return jnp.sum(jnp.transpose(source), 0, keepdims=True)


def both_blocks(cotangent, place, near):
    far, core = place[0] // (2 * CLOSE), place[0] % 2
    low, high = OFFSETS[0][near], OFFSETS[1][near]
    own = lax.rem(far + jnp.where(core == 0, low, high) + FAR, FAR)
    theirs = lax.rem(far + jnp.where(core == 0, high, low) + FAR, FAR)
    columns = [pl.ds(pl.multiple_of(block * BLOCK, BLOCK), BLOCK) for block in (own, theirs)]
    return jnp.concatenate([cotangent[:, columns[0]], cotangent[:, columns[1]]], 1)


def forward(
    place, value, gate, cotangent, weight, far_taps, far_gain, far_mean, far_scale,
    gated, scaled, spread, sums, gain_part, first_upstream, first_cotangent, product,
    held_value, held_gate, held, held_weight, taps, gain, mean, scale, arrivals,
    padded, taps_wide, mean_columns, scale_columns, sum_first, sum_second,
    hidden, normed, upstream,
):
    copies = [
        pltpu.make_async_copy(source, target, arrivals.at[i])
        for i, (source, target) in enumerate(
            (
                (value, held_value), (gate, held_gate), (far_taps, taps), (far_mean, mean),
                (far_scale, scale), (far_gain, gain), (weight, held_weight), (cotangent, held),
            )
        )
    ]
    for copy in copies:
        copy.start()
    sum_first[0:EDGE] = jnp.zeros((EDGE, LANES), WIDE)
    sum_second[0:EDGE] = jnp.zeros((EDGE, LANES), WIDE)
    hidden[0:EDGE] = jnp.zeros((EDGE, WIDTH), WIDE)
    for copy in copies[:6]:
        copy.wait()
    taps_wide[0:TAPS] = taps[...].astype(WIDE)
    for block in range(ROWS // LANES):
        rows = slice(block * LANES, (block + 1) * LANES)
        mean_columns[rows] = column(mean[rows].reshape(1, LANES))
        scale_columns[rows] = column(scale[rows].reshape(1, LANES))
    for half in range(HALVES):
        for start in range(0, ROWS, CHUNK):
            rows = slice(start, start + CHUNK)
            sig = jax.nn.sigmoid(held_gate[rows, lanes(half)].astype(WIDE))
            narrow = (held_value[rows, lanes(half)].astype(WIDE) * sig).astype(NARROW)
            gated[rows, lanes(half)] = narrow
            padded[half, EDGE + start : EDGE + start + CHUNK] = narrow.astype(WIDE)
        for start in range(EDGE, ROWS, EDGE):
            rows = slice(start, start + EDGE)
            conv = convolve(padded, half, taps_wide, start, EDGE)
            normed[half, rows] = (conv - mean_columns[rows]) * scale_columns[rows]
    copies[6].wait()
    copies[7].wait()
    upstream[...] = lax.dot_general(
        held[...], held_weight[...], (((1,), (1,)), ((), ())), preferred_element_type=WIDE
    )
    first_upstream[...] = upstream[0:EDGE]
    first_cotangent[...] = held[0:EDGE]
    for half in range(HALVES):
        gain_row = gain[0:1, lanes(half)]
        gain_sum = jnp.zeros((8, LANES), WIDE)
        for start in range(EDGE, ROWS, EDGE):
            rows = slice(start, start + EDGE)
            narrow, own_scaled, own_spread, first, second, part = norm_backward(
                normed[half, rows], scale_columns[rows], gain_row, upstream[rows, lanes(half)]
            )
            hidden[rows, lanes(half)] = narrow.astype(WIDE)
            scaled[half, start - EDGE : start] = own_scaled
            spread[half, start - EDGE : start] = own_spread
            gain_sum = gain_sum + part
            if half == 0:
                sum_first[rows] = first
                sum_second[rows] = second
            else:
                sum_first[rows] = sum_first[rows] + first
                sum_second[rows] = sum_second[rows] + second
        gain_part[half] = gain_sum
    found = [
        column_sums(source[block * LANES : (block + 1) * LANES])
        for source in (sum_first, sum_second)
        for block in range(ROWS // LANES)
    ]
    sums[...] = jnp.concatenate([*found, jnp.zeros((2, LANES), WIDE)], 0)
    turned = jnp.transpose(hidden[...]).astype(NARROW)
    for near in range(CLOSE):
        product[near] = jnp.dot(
            turned, both_blocks(held, place, near), preferred_element_type=WIDE
        )


def head(
    halo, gated, upstream, taps, gain, mean, scale, sums, gain_part,
    scaled, spread, hidden, message, gain_total,
    padded, taps_wide, turned,
):
    taps_wide[0:TAPS] = taps[...].astype(WIDE)
    rows = slice(0, EDGE)
    mean_columns = column(mean[0:LANES].reshape(1, LANES))[rows]
    scale_columns = column(scale[0:LANES].reshape(1, LANES))[rows]
    turned[...] = jnp.zeros((2, LANES, LANES), WIDE)
    for half in range(HALVES):
        padded[half, rows] = halo[:, lanes(half)].astype(WIDE)
        padded[half, EDGE:] = gated[rows, lanes(half)].astype(WIDE)
    for half in range(HALVES):
        conv = convolve(padded, half, taps_wide, 0, EDGE)
        normed = (conv - mean_columns) * scale_columns
        narrow, own_scaled, own_spread, first, second, part = norm_backward(
            normed, scale_columns, gain[0:1, lanes(half)], upstream[rows, lanes(half)]
        )
        hidden[:, lanes(half)] = narrow
        scaled[half] = own_scaled
        spread[half] = own_spread
        gain_total[half] = gain_part[half] + part
        turned[0, rows] = turned[0, rows] + first
        turned[1, rows] = turned[1, rows] + second
    blocks = ROWS // LANES
    total = sums[...]
    extra = [column_sums(turned[0]), column_sums(turned[1])]
    none = jnp.zeros((blocks - 1, LANES), WIDE)
    last = jnp.zeros((2, LANES), WIDE)
    total = total + jnp.concatenate([extra[0], none, extra[1], none, last], 0)
    for peer in range(TP):
        message[peer] = total


def head_product(cotangent, hidden, place, near, side):
    columns = both_blocks(cotangent, place, near)[:, side * BLOCK : (side + 1) * BLOCK]
    return lax.dot_general(
        hidden[...], columns, (((0,), (0,)), ((), ())), preferred_element_type=WIDE
    )


def backward(
    place, sums, scaled, spread, first_scaled, first_spread, halo, gated, scale, gain_part,
    first_cotangent, first_hidden, product,
    other, small, extended,
    padded,
):
    for half in range(HALVES):
        padded[half, 0:EDGE] = halo[:, lanes(half)].astype(WIDE)
        padded[half, EDGE:] = gated[:, lanes(half)].astype(WIDE)
    total = (sums[0] + sums[1]) + (sums[2] + sums[3])
    total = total * (1.0 / (TP * WIDTH))
    blocks = ROWS // LANES
    for half in range(HALVES):
        extended[half, 0:EDGE] = jnp.zeros((EDGE, LANES), WIDE)
        extended[half, EDGE + ROWS :] = jnp.zeros((EDGE, LANES), WIDE)
    for block in range(blocks):
        rows = slice(block * LANES, (block + 1) * LANES)
        first = column(total[block : block + 1] * scale[rows].reshape(1, LANES))
        second = column(total[blocks + block : blocks + block + 1])
        for half in range(HALVES):
            cut = 0
            if block == 0:
                cut = EDGE
                d_conv = first_scaled[half] - first[0:cut] - first_spread[half] * second[0:cut]
                extended[half, EDGE : EDGE + cut] = d_conv
            rows = slice(block * LANES + cut - EDGE, (block + 1) * LANES - EDGE)
            d_conv = scaled[half, rows] - first[cut:] - spread[half, rows] * second[cut:]
            extended[half, EDGE + block * LANES + cut : EDGE + (block + 1) * LANES] = d_conv
    lead = EDGE - TAPS + 1
    groups = ROWS // 8
    for offset in range(8):
        steps = [q for q in range(5) if 0 <= 8 * q + offset - lead < TAPS]
        found = {(half, q): jnp.zeros((8, LANES), WIDE) for half in range(HALVES) for q in steps}
        loaded = {}
        for m in range(groups + steps[-1]):
            for half in range(HALVES):
                if m < groups:
                    begin = EDGE + 8 * m
                    loaded[half, m] = extended[half, begin : begin + 8]
                moved = padded[half, 8 * m + offset : 8 * m + offset + 8]
                for q in steps:
                    if 0 <= m - q < groups:
                        found[half, q] = found[half, q] + loaded[half, m - q] * moved
        for half in range(HALVES):
            for q in steps:
                tap = 8 * q + offset - lead
                small[tap : tap + 1, lanes(half)] = jnp.sum(found[half, q], 0, keepdims=True)
        near = offset
        whole = product[near, :, BLOCK:] + head_product(
            first_cotangent, first_hidden, place, near, 1
        )
        other[near * WIDTH : (near + 1) * WIDTH] = whole.astype(NARROW)
    for half in range(HALVES):
        small[TAPS:SMALL, lanes(half)] = jnp.sum(gain_part[half], 0, keepdims=True)
    for half in range(HALVES):
        value = small[:, lanes(half)]
        top = value.astype(NARROW)
        begin = CLOSE * WIDTH + half * 2 * SMALL
        other[begin : begin + SMALL] = top
        other[begin + SMALL : begin + 2 * SMALL] = (value - top.astype(WIDE)).astype(NARROW)


def pack(mine, small, other, pieces):
    for half in range(HALVES):
        begin = CLOSE * WIDTH + half * 2 * SMALL
        top = other[begin : begin + SMALL].astype(WIDE)
        rest = other[begin + SMALL : begin + 2 * SMALL].astype(WIDE)
        both = (small[:, lanes(half)] + (top + rest)).astype(NARROW)
        for near in range(CLOSE):
            pieces[near, WIDTH + half * SMALL : WIDTH + (half + 1) * SMALL] = both
    for near in range(CLOSE):
        for start in range(0, WIDTH, 64):
            rows = slice(start, start + 64)
            there = other[near * WIDTH + start : near * WIDTH + start + 64].astype(WIDE)
            pieces[near, rows] = (mine[near, rows] + there).astype(NARROW)


def gated_gradient(
    place, extended, taps, first_cotangent, first_hidden, product,
    d_gated, margin, mine,
    taps_wide,
):
    for near in range(CLOSE):
        mine[near] = product[near, :, 0:BLOCK] + head_product(
            first_cotangent, first_hidden, place, near, 0
        )
    taps_wide[0:TAPS] = taps[...].astype(WIDE)
    for half in range(HALVES):
        for start in range(0, EDGE + ROWS, EDGE):
            found = jnp.zeros((EDGE, LANES), WIDE)
            for tap in range(TAPS):
                begin = start + TAPS - 1 - tap
                found = found + taps_wide[tap : tap + 1, lanes(half)] * extended[half, begin : begin + EDGE]
            if start == 0:
                margin[half] = found
            else:
                d_gated[half, start - EDGE : start] = found


def fold_near(arrived, payload):
    for start in range(0, WIDTH + 2 * SMALL, 64):
        rows = slice(start, start + 64)
        total = arrived[0, rows].astype(WIDE)
        for near in range(1, CLOSE):
            total = total + arrived[near, rows].astype(WIDE)
        payload[rows] = total.astype(NARROW)


def hand_out(payload, message):
    weights = jnp.transpose(payload[0:WIDTH].astype(WIDE)).astype(NARROW)
    small = jnp.concatenate([payload[WIDTH : WIDTH + SMALL], payload[WIDTH + SMALL :]], 1)
    for position, member in enumerate(GATHER_ORDER):
        message[position, 0:OWN] = weights[member * OWN : (member + 1) * OWN]
        message[position, OWN:] = small


def totals(arrived, total):
    for start in range(0, OWN + SMALL, 8):
        rows = slice(start, start + 8)
        found = arrived[0, rows].astype(WIDE)
        for position in range(1, 2 * CLOSE):
            found = found + arrived[position, rows].astype(WIDE)
        total[rows] = found


def finish(
    total, d_gated, late, value, gate,
    value_grad, gate_grad, weight_grad, taps_grad, gain_grad,
):
    for half in range(HALVES):
        for start in range(0, ROWS, EDGE):
            rows = slice(start, start + EDGE)
            grad = d_gated[half, rows]
            if start == ROWS - EDGE:
                grad = grad + late[half]
            sig = jax.nn.sigmoid(gate[rows, lanes(half)].astype(WIDE))
            wide = value[rows, lanes(half)].astype(WIDE)
            value_grad[rows, lanes(half)] = (grad * sig).astype(NARROW)
            gate_grad[rows, lanes(half)] = (grad * wide * sig * (1.0 - sig)).astype(NARROW)
    weight_grad[...] = total[0:OWN]
    taps_grad[...] = total[OWN : OWN + TAPS]
    gain_grad[...] = total[OWN + TAPS :]


def to_block(value):
    pairs = []
    for far in range(FAR):
        for near in range(CLOSE):
            for core in range(2):
                target = (far + OFFSETS[core][near]) % FAR
                pairs.append(((far * CLOSE + near) * 2 + core, (target * CLOSE + near) * 2 + core))
    return lax.ppermute(value, SP, pairs)


def shards(
    proj_value, proj_gate, out_cotangent, out_weight, conv_taps, norm_gain, row_mean, row_scale
):
    end_gate = jax.nn.sigmoid(proj_gate[ROWS - EDGE :].astype(WIDE))
    end = (proj_value[ROWS - EDGE :].astype(WIDE) * end_gate).astype(NARROW)
    halo = shifted(end, SP, 1)
    split = (HALVES, ROWS, LANES)
    rest = (HALVES, ROWS - EDGE, LANES)
    row_gain = norm_gain.reshape(1, WIDTH)
    sides = pltpu.VMEM((HALVES, EDGE + ROWS, LANES), WIDE)
    taps_scratch = pltpu.VMEM((TAPS + 1, WIDTH), WIDE)
    place = lax.axis_index(SP).reshape(1)
    narrow = ((ROWS, WIDTH), NARROW)
    gated, scaled, spread, sums, gain_part, first_upstream, first_cotangent, product = (
        scalar_call(
            forward,
            [
                narrow, (rest, WIDE), (rest, WIDE), ((8, LANES), WIDE),
                ((HALVES, 8, LANES), WIDE), ((EDGE, WIDTH), WIDE), ((EDGE, MODEL), NARROW),
                ((CLOSE, WIDTH, 2 * BLOCK), WIDE),
            ],
            place, proj_value, proj_gate, out_cotangent, out_weight,
            conv_taps, row_gain, row_mean, row_scale, in_hbm=8,
            scratch=[
                pltpu.VMEM(*narrow), pltpu.VMEM(*narrow), pltpu.VMEM((ROWS, MODEL), NARROW),
                pltpu.VMEM((WIDTH, MODEL), NARROW), pltpu.VMEM((TAPS, WIDTH), NARROW),
                pltpu.VMEM((1, WIDTH), WIDE), pltpu.VMEM((ROWS,), WIDE),
                pltpu.VMEM((ROWS,), WIDE), pltpu.SemaphoreType.DMA((8,)),
                sides, taps_scratch, *([pltpu.VMEM((ROWS, LANES), WIDE)] * 4),
                pltpu.VMEM((ROWS, WIDTH), WIDE), pltpu.VMEM(split, WIDE),
                pltpu.VMEM((ROWS, WIDTH), WIDE),
            ],
            flops=4 * ROWS * WIDTH * MODEL, limit=12,
        )
    )
    edge = (HALVES, EDGE, LANES)
    first_scaled, first_spread, first_hidden, message, gain_part = call_with(
        head,
        [
            (edge, WIDE), (edge, WIDE), ((EDGE, WIDTH), NARROW),
            ((TP, 8, LANES), WIDE), ((HALVES, 8, LANES), WIDE),
        ],
        [
            pltpu.VMEM((HALVES, 2 * EDGE, LANES), WIDE),
            taps_scratch,
            pltpu.VMEM((2, LANES, LANES), WIDE),
        ],
        halo, gated, first_upstream, conv_taps, row_gain, row_mean, row_scale, sums,
        gain_part, flops=10 * ROWS * WIDTH,
    )
    sums = exchange(message, "tp", SUMS_ORDER)
    rows = CLOSE * WIDTH + 4 * SMALL
    other, small, extended = scalar_call(
        backward,
        [
            ((rows, BLOCK), NARROW), ((SMALL, WIDTH), WIDE),
            ((HALVES, ROWS + 2 * EDGE, LANES), WIDE),
        ],
        place, sums, scaled, spread, first_scaled, first_spread, halo, gated, row_scale, gain_part,
        first_cotangent, first_hidden, product, scratch=[sides], flops=100 * ROWS * WIDTH,
    )
    other = lax.ppermute(other, "c", [(0, 1), (1, 0)])
    d_gated, margin, mine = scalar_call(
        gated_gradient,
        [(split, WIDE), ((HALVES, EDGE, LANES), WIDE), ((CLOSE, WIDTH, BLOCK), WIDE)],
        place, extended, conv_taps, first_cotangent, first_hidden, product,
        scratch=[taps_scratch], flops=100 * ROWS * WIDTH,
    )
    (pieces,) = call(
        pack, [((CLOSE, WIDTH + 2 * SMALL, BLOCK), NARROW)], mine, small, other, flops=1 << 20
    )
    arrived = exchange(pieces, NEAR)
    (payload,) = call(
        fold_near, [((WIDTH + 2 * SMALL, BLOCK), NARROW)], arrived, flops=1 << 20
    )
    payload = to_block(payload)
    late = shifted(margin, SP, -1)
    (message,) = call(hand_out, [((2 * CLOSE, OWN + SMALL, WIDTH), NARROW)], payload, flops=1 << 16)
    arrived = exchange(message, (*NEAR, "c"), GATHER_ORDER)
    (total,) = call(totals, [((OWN + SMALL, WIDTH), WIDE)], arrived, flops=1 << 20)
    value_grad, gate_grad, weight_grad, taps_grad, gain_grad = call(
        finish,
        [narrow, narrow, ((OWN, WIDTH), WIDE), ((TAPS, WIDTH), WIDE), ((1, WIDTH), WIDE)],
        total, d_gated, late, proj_value, proj_gate, flops=10 * ROWS * WIDTH,
    )
    return (value_grad, gate_grad, weight_grad, taps_grad, gain_grad.reshape(WIDTH))


def call_with(body, outs, scratch, *args, flops=0, limit=6):
    shapes = [jax.ShapeDtypeStruct(shape, dtype) for shape, dtype in outs]
    size = sum(a.size * a.dtype.itemsize for a in (*args, *shapes))
    return pl.pallas_call(
        body,
        out_shape=shapes,
        scratch_shapes=scratch,
        compiler_params=pltpu.CompilerParams(vmem_limit_bytes=limit << 20),
        cost_estimate=pl.CostEstimate(flops=flops, bytes_accessed=size, transcendentals=0),
    )(*args)


def scalar_call(
    body, outs, scalar, *args, scratch=(), flops=1 << 20, limit=6, in_hbm=0
):
    shapes = [jax.ShapeDtypeStruct(shape, dtype) for shape, dtype in outs]
    size = sum(a.size * a.dtype.itemsize for a in (*args, *shapes))
    whole = pl.BlockSpec(memory_space=pltpu.VMEM)
    far = [pltpu.with_memory_space_constraint(a, pltpu.HBM) for a in args[:in_hbm]]
    return pl.pallas_call(
        body,
        out_shape=shapes,
        in_specs=[
            pl.BlockSpec(memory_space=pltpu.SMEM),
            *([pl.BlockSpec(memory_space=pltpu.HBM)] * in_hbm),
            *([whole] * (len(args) - in_hbm)),
        ],
        out_specs=[whole] * len(shapes),
        scratch_shapes=scratch,
        compiler_params=pltpu.CompilerParams(vmem_limit_bytes=limit << 20),
        cost_estimate=pl.CostEstimate(flops=flops, bytes_accessed=size, transcendentals=0),
    )(scalar, *far, *args[in_hbm:])


def solution(mesh):
    sizes = [size for _, size in AXES]
    split = Mesh(mesh.devices.reshape(*sizes, mesh.shape["tp"]), (*SP, "tp"))
    placed = (
        P(SP, "tp"),
        P(SP, "tp"),
        P(SP, None),
        P("tp", None),
        P(None, "tp"),
        P("tp"),
        P(SP),
        P(SP),
    )
    return jax.shard_map(
        shards,
        mesh=split,
        in_specs=placed,
        out_specs=(P(SP, "tp"), P(SP, "tp"), P(SP, "tp"), P(None, "tp"), P("tp")),
        check_vma=False,
    )
```

```python
import jax
import jax.numpy as jnp
from jax import lax
from jax.experimental import pallas as pl
from jax.experimental.pallas import tpu as pltpu
from jax.sharding import Mesh
from jax.sharding import PartitionSpec as P


SP = ("zh", "zl", "x", "c")
NEAR = ("zl", "x")
FAR = 16
CLOSE = 8
AXES = (("zh", FAR), ("zl", 2), ("x", 4), ("c", 2))
TP = 4
SUMS_ORDER = [2, 3, 0, 1]
OFFSETS = ((0, -1, -2, -3, 3, 2, 1, -4), (6, 7, 8, 5, -7, -6, -5, 4))
BLOCK = CLOSE * 2 * 8
NEAR_ORDER = [(place + 4) % CLOSE for place in range(CLOSE)]
GATHER_ORDER = [(place + 7) % (2 * CLOSE) for place in range(2 * CLOSE)]
TAPS = 31
SMALL = TAPS + 1
ROWS = 384
EDGE = 32
LANES = 128
HALVES = 2
WIDTH = HALVES * LANES
MODEL = 2048
OWN = 8
CHUNK = 64
WIDE = jnp.float32
NARROW = jnp.bfloat16


def shifted(value, axis, steps):
    count = lax.axis_size(axis)
    first, last = (max(0, -steps), min(count, count - steps))
    return lax.ppermute(value, axis, [(source, source + steps) for source in range(first, last)])


def exchange(pieces, axes, order=None):
    groups = order and [order]
    return lax.all_to_all(pieces, axes, 0, 0, tiled=True, axis_index_groups=groups)


def lanes(half):
    return slice(half * LANES, (half + 1) * LANES)


def column(row):
    return jnp.transpose(jnp.broadcast_to(row, (LANES, LANES)))


def call(body, outs, *args, flops=0, limit=6):
    shapes = [jax.ShapeDtypeStruct(shape, dtype) for shape, dtype in outs]
    size = sum(a.size * a.dtype.itemsize for a in (*args, *shapes))
    return pl.pallas_call(
        body,
        out_shape=shapes,
        compiler_params=pltpu.CompilerParams(vmem_limit_bytes=limit << 20),
        cost_estimate=pl.CostEstimate(flops=flops, bytes_accessed=size, transcendentals=0),
    )(*args)


def norm_backward(normed, factor, gain_row, upstream):
    active = normed * gain_row
    sig = jax.nn.sigmoid(active)
    hidden = (active * sig).astype(NARROW)
    d_active = upstream * sig * (1.0 + active * (1.0 - sig))
    d_normed = d_active * gain_row
    gain_part = jnp.sum((d_active * normed).reshape(normed.shape[0] // 8, 8, LANES), 0)
    return hidden, factor * d_normed, factor * normed, d_normed, d_normed * normed, gain_part


def convolve(source, half, taps_wide, start, size):
    conv = jnp.zeros((size, LANES), WIDE)
    for tap in range(TAPS):
        begin = start + tap + EDGE - TAPS + 1
        conv = conv + taps_wide[tap : tap + 1, lanes(half)] * source[half, begin : begin + size]
    return conv


def column_sums(source):
    return jnp.sum(jnp.transpose(source), 0, keepdims=True)


def both_blocks(cotangent, place, near):
    far, core = place[0] // (2 * CLOSE), place[0] % 2
    low, high = OFFSETS[0][near], OFFSETS[1][near]
    own = lax.rem(far + jnp.where(core == 0, low, high) + FAR, FAR)
    theirs = lax.rem(far + jnp.where(core == 0, high, low) + FAR, FAR)
    columns = [pl.ds(pl.multiple_of(block * BLOCK, BLOCK), BLOCK) for block in (own, theirs)]
    return jnp.concatenate([cotangent[:, columns[0]], cotangent[:, columns[1]]], 1)


def load(
    value, gate, taps, gain, mean, scale,
    end, held_value, held_gate, held_taps, held_gain, held_mean, held_scale,
    arrivals,
):
    copies = [
        pltpu.make_async_copy(source, target, arrivals.at[i])
        for i, (source, target) in enumerate(
            (
                (value, held_value), (gate, held_gate), (taps, held_taps), (gain, held_gain),
                (mean, held_mean), (scale, held_scale),
            )
        )
    ]
    for copy in copies:
        copy.start()
    for copy in copies:
        copy.wait()
    rows = slice(ROWS - EDGE, ROWS)
    sig = jax.nn.sigmoid(held_gate[rows].astype(WIDE))
    end[...] = (held_value[rows].astype(WIDE) * sig).astype(NARROW)


def forward(
    place, cotangent, weight, held_value, held_gate, taps, gain, mean, scale,
    gated, scaled, spread, sums, gain_part, first_upstream, first_cotangent, product,
    held, held_weight, arrivals,
    padded, taps_wide, mean_columns, scale_columns, sum_first, sum_second,
    hidden, normed, upstream,
):
    copies = [
        pltpu.make_async_copy(source, target, arrivals.at[i])
        for i, (source, target) in enumerate(
            ((weight, held_weight), (cotangent, held))
        )
    ]
    for copy in copies:
        copy.start()
    sum_first[0:EDGE] = jnp.zeros((EDGE, LANES), WIDE)
    sum_second[0:EDGE] = jnp.zeros((EDGE, LANES), WIDE)
    hidden[0:EDGE] = jnp.zeros((EDGE, WIDTH), WIDE)
    taps_wide[0:TAPS] = taps[...].astype(WIDE)
    for block in range(ROWS // LANES):
        rows = slice(block * LANES, (block + 1) * LANES)
        mean_columns[rows] = column(mean[rows].reshape(1, LANES))
        scale_columns[rows] = column(scale[rows].reshape(1, LANES))
    for half in range(HALVES):
        for start in range(0, ROWS, CHUNK):
            rows = slice(start, start + CHUNK)
            sig = jax.nn.sigmoid(held_gate[rows, lanes(half)].astype(WIDE))
            narrow = (held_value[rows, lanes(half)].astype(WIDE) * sig).astype(NARROW)
            gated[rows, lanes(half)] = narrow
            padded[half, EDGE + start : EDGE + start + CHUNK] = narrow.astype(WIDE)
        for start in range(EDGE, ROWS, EDGE):
            rows = slice(start, start + EDGE)
            conv = convolve(padded, half, taps_wide, start, EDGE)
            normed[half, rows] = (conv - mean_columns[rows]) * scale_columns[rows]
    for copy in copies:
        copy.wait()
    upstream[...] = lax.dot_general(
        held[...], held_weight[...], (((1,), (1,)), ((), ())), preferred_element_type=WIDE
    )
    first_upstream[...] = upstream[0:EDGE]
    first_cotangent[...] = held[0:EDGE]
    for half in range(HALVES):
        gain_row = gain[0:1, lanes(half)]
        gain_sum = jnp.zeros((8, LANES), WIDE)
        for start in range(EDGE, ROWS, EDGE):
            rows = slice(start, start + EDGE)
            narrow, own_scaled, own_spread, first, second, part = norm_backward(
                normed[half, rows], scale_columns[rows], gain_row, upstream[rows, lanes(half)]
            )
            hidden[rows, lanes(half)] = narrow.astype(WIDE)
            scaled[half, start - EDGE : start] = own_scaled
            spread[half, start - EDGE : start] = own_spread
            gain_sum = gain_sum + part
            if half == 0:
                sum_first[rows] = first
                sum_second[rows] = second
            else:
                sum_first[rows] = sum_first[rows] + first
                sum_second[rows] = sum_second[rows] + second
        gain_part[half] = gain_sum
    found = [
        column_sums(source[block * LANES : (block + 1) * LANES])
        for source in (sum_first, sum_second)
        for block in range(ROWS // LANES)
    ]
    sums[...] = jnp.concatenate([*found, jnp.zeros((2, LANES), WIDE)], 0)
    turned = jnp.transpose(hidden[...]).astype(NARROW)
    for near in range(CLOSE):
        product[near] = jnp.dot(
            turned, both_blocks(held, place, near), preferred_element_type=WIDE
        )


def head(
    halo, gated, upstream, taps, gain, mean, scale, sums, gain_part,
    scaled, spread, hidden, message, gain_total,
    padded, taps_wide, turned,
):
    taps_wide[0:TAPS] = taps[...].astype(WIDE)
    rows = slice(0, EDGE)
    mean_columns = column(mean[0:LANES].reshape(1, LANES))[rows]
    scale_columns = column(scale[0:LANES].reshape(1, LANES))[rows]
    turned[...] = jnp.zeros((2, LANES, LANES), WIDE)
    for half in range(HALVES):
        padded[half, rows] = halo[:, lanes(half)].astype(WIDE)
        padded[half, EDGE:] = gated[rows, lanes(half)].astype(WIDE)
    for half in range(HALVES):
        conv = convolve(padded, half, taps_wide, 0, EDGE)
        normed = (conv - mean_columns) * scale_columns
        narrow, own_scaled, own_spread, first, second, part = norm_backward(
            normed, scale_columns, gain[0:1, lanes(half)], upstream[rows, lanes(half)]
        )
        hidden[:, lanes(half)] = narrow
        scaled[half] = own_scaled
        spread[half] = own_spread
        gain_total[half] = gain_part[half] + part
        turned[0, rows] = turned[0, rows] + first
        turned[1, rows] = turned[1, rows] + second
    blocks = ROWS // LANES
    total = sums[...]
    extra = [column_sums(turned[0]), column_sums(turned[1])]
    none = jnp.zeros((blocks - 1, LANES), WIDE)
    last = jnp.zeros((2, LANES), WIDE)
    total = total + jnp.concatenate([extra[0], none, extra[1], none, last], 0)
    for peer in range(TP):
        message[peer] = total


def head_product(cotangent, hidden, place, near, side):
    columns = both_blocks(cotangent, place, near)[:, side * BLOCK : (side + 1) * BLOCK]
    return lax.dot_general(
        hidden[...], columns, (((0,), (0,)), ((), ())), preferred_element_type=WIDE
    )


def backward(
    place, sums, scaled, spread, first_scaled, first_spread, halo, gated, scale, gain_part,
    first_cotangent, first_hidden, product,
    other, small, extended,
    padded,
):
    for half in range(HALVES):
        padded[half, 0:EDGE] = halo[:, lanes(half)].astype(WIDE)
        padded[half, EDGE:] = gated[:, lanes(half)].astype(WIDE)
    total = (sums[0] + sums[1]) + (sums[2] + sums[3])
    total = total * (1.0 / (TP * WIDTH))
    blocks = ROWS // LANES
    for half in range(HALVES):
        extended[half, 0:EDGE] = jnp.zeros((EDGE, LANES), WIDE)
        extended[half, EDGE + ROWS :] = jnp.zeros((EDGE, LANES), WIDE)
    for block in range(blocks):
        rows = slice(block * LANES, (block + 1) * LANES)
        first = column(total[block : block + 1] * scale[rows].reshape(1, LANES))
        second = column(total[blocks + block : blocks + block + 1])
        for half in range(HALVES):
            cut = 0
            if block == 0:
                cut = EDGE
                d_conv = first_scaled[half] - first[0:cut] - first_spread[half] * second[0:cut]
                extended[half, EDGE : EDGE + cut] = d_conv
            rows = slice(block * LANES + cut - EDGE, (block + 1) * LANES - EDGE)
            d_conv = scaled[half, rows] - first[cut:] - spread[half, rows] * second[cut:]
            extended[half, EDGE + block * LANES + cut : EDGE + (block + 1) * LANES] = d_conv
    lead = EDGE - TAPS + 1
    groups = ROWS // 8
    for offset in range(8):
        steps = [q for q in range(5) if 0 <= 8 * q + offset - lead < TAPS]
        found = {(half, q): jnp.zeros((8, LANES), WIDE) for half in range(HALVES) for q in steps}
        loaded = {}
        for m in range(groups + steps[-1]):
            for half in range(HALVES):
                if m < groups:
                    begin = EDGE + 8 * m
                    loaded[half, m] = extended[half, begin : begin + 8]
                moved = padded[half, 8 * m + offset : 8 * m + offset + 8]
                for q in steps:
                    if 0 <= m - q < groups:
                        found[half, q] = found[half, q] + loaded[half, m - q] * moved
        for half in range(HALVES):
            for q in steps:
                tap = 8 * q + offset - lead
                small[tap : tap + 1, lanes(half)] = jnp.sum(found[half, q], 0, keepdims=True)
        near = offset
        whole = product[near, :, BLOCK:] + head_product(
            first_cotangent, first_hidden, place, near, 1
        )
        other[near * WIDTH : (near + 1) * WIDTH] = whole.astype(NARROW)
    for half in range(HALVES):
        small[TAPS:SMALL, lanes(half)] = jnp.sum(gain_part[half], 0, keepdims=True)
    for half in range(HALVES):
        value = small[:, lanes(half)]
        top = value.astype(NARROW)
        begin = CLOSE * WIDTH + half * 2 * SMALL
        other[begin : begin + SMALL] = top
        other[begin + SMALL : begin + 2 * SMALL] = (value - top.astype(WIDE)).astype(NARROW)


def pack(mine, small, other, pieces):
    for half in range(HALVES):
        begin = CLOSE * WIDTH + half * 2 * SMALL
        top = other[begin : begin + SMALL].astype(WIDE)
        rest = other[begin + SMALL : begin + 2 * SMALL].astype(WIDE)
        both = (small[:, lanes(half)] + (top + rest)).astype(NARROW)
        for near in range(CLOSE):
            pieces[near, WIDTH + half * SMALL : WIDTH + (half + 1) * SMALL] = both
    for near in range(CLOSE):
        for start in range(0, WIDTH, 64):
            rows = slice(start, start + 64)
            there = other[near * WIDTH + start : near * WIDTH + start + 64].astype(WIDE)
            pieces[NEAR_ORDER.index(near), rows] = (mine[near, rows] + there).astype(NARROW)


def gated_gradient(
    place, extended, taps, value, gate, first_cotangent, first_hidden, product,
    value_grad, gate_grad, margin, last, mine,
    taps_wide,
):
    for near in range(CLOSE):
        mine[near] = product[near, :, 0:BLOCK] + head_product(
            first_cotangent, first_hidden, place, near, 0
        )
    taps_wide[0:TAPS] = taps[...].astype(WIDE)
    for half in range(HALVES):
        for start in range(0, EDGE + ROWS, EDGE):
            found = jnp.zeros((EDGE, LANES), WIDE)
            for tap in range(TAPS):
                begin = start + TAPS - 1 - tap
                found = found + taps_wide[tap : tap + 1, lanes(half)] * extended[half, begin : begin + EDGE]
            if start == 0:
                margin[half] = found
                continue
            rows = slice(start - EDGE, start)
            sig = jax.nn.sigmoid(gate[rows, lanes(half)].astype(WIDE))
            slope = value[rows, lanes(half)].astype(WIDE) * sig * (1.0 - sig)
            if start == ROWS:
                last[0, half], last[1, half], last[2, half] = found, sig, slope
            else:
                value_grad[rows, lanes(half)] = (found * sig).astype(NARROW)
                gate_grad[rows, lanes(half)] = (found * slope).astype(NARROW)


def fold_near(arrived, payload):
    for start in range(0, WIDTH + 2 * SMALL, 64):
        rows = slice(start, start + 64)
        total = arrived[0, rows].astype(WIDE)
        for near in range(1, CLOSE):
            total = total + arrived[near, rows].astype(WIDE)
        payload[rows] = total.astype(NARROW)


def hand_out(payload, message):
    weights = jnp.transpose(payload[0:WIDTH].astype(WIDE)).astype(NARROW)
    small = jnp.concatenate([payload[WIDTH : WIDTH + SMALL], payload[WIDTH + SMALL :]], 1)
    for position, member in enumerate(GATHER_ORDER):
        message[position, 0:OWN] = weights[member * OWN : (member + 1) * OWN]
        message[position, OWN:] = small


def totals(arrived, total):
    for start in range(0, OWN + SMALL, 8):
        rows = slice(start, start + 8)
        found = arrived[0, rows].astype(WIDE)
        for position in range(1, 2 * CLOSE):
            found = found + arrived[position, rows].astype(WIDE)
        total[rows] = found


def finish(
    total, value_part, gate_part, last, late,
    value_grad, gate_grad, weight_grad, taps_grad, gain_grad,
    value_end, gate_end, taps_held, gain_held, departures,
):
    main, end = pl.ds(0, ROWS - EDGE), pl.ds(ROWS - EDGE, EDGE)
    taps_held[...] = total[OWN : OWN + TAPS]
    gain_held[...] = total[OWN + TAPS :]
    for half in range(HALVES):
        grad = last[0, half] + late[half]
        value_end[:, lanes(half)] = (grad * last[1, half]).astype(NARROW)
        gate_end[:, lanes(half)] = (grad * last[2, half]).astype(NARROW)
    copies = [
        pltpu.make_async_copy(value_part, value_grad.at[main], departures.at[0]),
        pltpu.make_async_copy(gate_part, gate_grad.at[main], departures.at[1]),
        pltpu.make_async_copy(total.at[pl.ds(0, OWN)], weight_grad, departures.at[2]),
        pltpu.make_async_copy(taps_held, taps_grad, departures.at[3]),
        pltpu.make_async_copy(gain_held, gain_grad, departures.at[4]),
        pltpu.make_async_copy(value_end, value_grad.at[end], departures.at[5]),
        pltpu.make_async_copy(gate_end, gate_grad.at[end], departures.at[6]),
    ]
    for copy in copies:
        copy.start()
    for copy in copies:
        copy.wait()


def to_block(value):
    pairs = []
    for far in range(FAR):
        for near in range(CLOSE):
            for core in range(2):
                target = (far + OFFSETS[core][near]) % FAR
                pairs.append(((far * CLOSE + near) * 2 + core, (target * CLOSE + near) * 2 + core))
    return lax.ppermute(value, SP, pairs)


def shards(
    proj_value, proj_gate, out_cotangent, out_weight, conv_taps, norm_gain, row_mean, row_scale
):
    row_gain = norm_gain.reshape(1, WIDTH)
    end, proj_value, proj_gate, conv_taps, row_gain, row_mean, row_scale = load_call(
        proj_value, proj_gate, conv_taps, row_gain, row_mean, row_scale
    )
    halo = shifted(end, SP, 1)
    split = (HALVES, ROWS, LANES)
    rest = (HALVES, ROWS - EDGE, LANES)
    sides = pltpu.VMEM((HALVES, EDGE + ROWS, LANES), WIDE)
    taps_scratch = pltpu.VMEM((TAPS + 1, WIDTH), WIDE)
    place = lax.axis_index(SP).reshape(1)
    narrow = ((ROWS, WIDTH), NARROW)
    gated, scaled, spread, sums, gain_part, first_upstream, first_cotangent, product = (
        scalar_call(
            forward,
            [
                narrow, (rest, WIDE), (rest, WIDE), ((8, LANES), WIDE),
                ((HALVES, 8, LANES), WIDE), ((EDGE, WIDTH), WIDE), ((EDGE, MODEL), NARROW),
                ((CLOSE, WIDTH, 2 * BLOCK), WIDE),
            ],
            place, out_cotangent, out_weight, proj_value, proj_gate,
            conv_taps, row_gain, row_mean, row_scale, in_hbm=2,
            scratch=[
                pltpu.VMEM((ROWS, MODEL), NARROW), pltpu.VMEM((WIDTH, MODEL), NARROW),
                pltpu.SemaphoreType.DMA((2,)),
                sides, taps_scratch, *([pltpu.VMEM((ROWS, LANES), WIDE)] * 4),
                pltpu.VMEM((ROWS, WIDTH), WIDE), pltpu.VMEM(split, WIDE),
                pltpu.VMEM((ROWS, WIDTH), WIDE),
            ],
            flops=4 * ROWS * WIDTH * MODEL, limit=12,
        )
    )
    edge = (HALVES, EDGE, LANES)
    first_scaled, first_spread, first_hidden, message, gain_part = call_with(
        head,
        [
            (edge, WIDE), (edge, WIDE), ((EDGE, WIDTH), NARROW),
            ((TP, 8, LANES), WIDE), ((HALVES, 8, LANES), WIDE),
        ],
        [
            pltpu.VMEM((HALVES, 2 * EDGE, LANES), WIDE),
            taps_scratch,
            pltpu.VMEM((2, LANES, LANES), WIDE),
        ],
        halo, gated, first_upstream, conv_taps, row_gain, row_mean, row_scale, sums,
        gain_part, flops=10 * ROWS * WIDTH,
    )
    sums = exchange(message, "tp", SUMS_ORDER)
    rows = CLOSE * WIDTH + 4 * SMALL
    other, small, extended = scalar_call(
        backward,
        [
            ((rows, BLOCK), NARROW), ((SMALL, WIDTH), WIDE),
            ((HALVES, ROWS + 2 * EDGE, LANES), WIDE),
        ],
        place, sums, scaled, spread, first_scaled, first_spread, halo, gated, row_scale, gain_part,
        first_cotangent, first_hidden, product, scratch=[sides], flops=100 * ROWS * WIDTH,
    )
    other = lax.ppermute(other, "c", [(0, 1), (1, 0)])
    main = ((ROWS - EDGE, WIDTH), NARROW)
    value_part, gate_part, margin, last, mine = scalar_call(
        gated_gradient,
        [main, main, (edge, WIDE), ((3, *edge), WIDE), ((CLOSE, WIDTH, BLOCK), WIDE)],
        place, extended, conv_taps, proj_value, proj_gate, first_cotangent, first_hidden,
        product, scratch=[taps_scratch], flops=100 * ROWS * WIDTH,
    )
    (pieces,) = call(
        pack, [((CLOSE, WIDTH + 2 * SMALL, BLOCK), NARROW)], mine, small, other, flops=1 << 20
    )
    arrived = exchange(pieces, NEAR, NEAR_ORDER)
    (payload,) = call(
        fold_near, [((WIDTH + 2 * SMALL, BLOCK), NARROW)], arrived, flops=1 << 20
    )
    payload = to_block(payload)
    late = shifted(margin, SP, -1)
    (message,) = call(hand_out, [((2 * CLOSE, OWN + SMALL, WIDTH), NARROW)], payload, flops=1 << 16)
    arrived = exchange(message, (*NEAR, "c"), GATHER_ORDER)
    (total,) = call(totals, [((OWN + SMALL, WIDTH), WIDE)], arrived, flops=1 << 20)
    value_grad, gate_grad, weight_grad, taps_grad, gain_grad = last_call(
        [narrow, narrow, ((OWN, WIDTH), WIDE), ((TAPS, WIDTH), WIDE), ((1, WIDTH), WIDE)],
        total, value_part, gate_part, last, late,
    )
    return (value_grad, gate_grad, weight_grad, taps_grad, gain_grad.reshape(WIDTH))


def call_with(body, outs, scratch, *args, flops=0, limit=6):
    shapes = [jax.ShapeDtypeStruct(shape, dtype) for shape, dtype in outs]
    size = sum(a.size * a.dtype.itemsize for a in (*args, *shapes))
    return pl.pallas_call(
        body,
        out_shape=shapes,
        scratch_shapes=scratch,
        compiler_params=pltpu.CompilerParams(vmem_limit_bytes=limit << 20),
        cost_estimate=pl.CostEstimate(flops=flops, bytes_accessed=size, transcendentals=0),
    )(*args)


def scalar_call(
    body, outs, scalar, *args, scratch=(), flops=1 << 20, limit=6, in_hbm=0
):
    shapes = [jax.ShapeDtypeStruct(shape, dtype) for shape, dtype in outs]
    size = sum(a.size * a.dtype.itemsize for a in (*args, *shapes))
    whole = pl.BlockSpec(memory_space=pltpu.VMEM)
    far = [pltpu.with_memory_space_constraint(a, pltpu.HBM) for a in args[:in_hbm]]
    return pl.pallas_call(
        body,
        out_shape=shapes,
        in_specs=[
            pl.BlockSpec(memory_space=pltpu.SMEM),
            *([pl.BlockSpec(memory_space=pltpu.HBM)] * in_hbm),
            *([whole] * (len(args) - in_hbm)),
        ],
        out_specs=[whole] * len(shapes),
        scratch_shapes=scratch,
        compiler_params=pltpu.CompilerParams(vmem_limit_bytes=limit << 20),
        cost_estimate=pl.CostEstimate(flops=flops, bytes_accessed=size, transcendentals=0),
    )(scalar, *far, *args[in_hbm:])


def load_call(*args):
    held = [pltpu.with_memory_space_constraint(a, pltpu.HBM) for a in args]
    shapes = [jax.ShapeDtypeStruct((EDGE, WIDTH), NARROW)]
    shapes += [jax.ShapeDtypeStruct(a.shape, a.dtype) for a in args]
    return pl.pallas_call(
        load,
        out_shape=shapes,
        in_specs=[pl.BlockSpec(memory_space=pltpu.HBM)] * len(args),
        out_specs=[pl.BlockSpec(memory_space=pltpu.VMEM)] * len(shapes),
        scratch_shapes=[pltpu.SemaphoreType.DMA((len(args),))],
        compiler_params=pltpu.CompilerParams(vmem_limit_bytes=6 << 20),
        cost_estimate=pl.CostEstimate(flops=1 << 16, bytes_accessed=1 << 19, transcendentals=0),
        name="load",
    )(*held)


def last_call(outs, *args):
    edge = pltpu.VMEM((EDGE, WIDTH), NARROW)
    return pl.pallas_call(
        finish,
        out_shape=[pltpu.HBM(*out) for out in outs],
        in_specs=[pl.BlockSpec(memory_space=pltpu.VMEM)] * len(args),
        out_specs=[pl.BlockSpec(memory_space=pltpu.HBM)] * len(outs),
        scratch_shapes=[
            edge, edge, pltpu.VMEM(*outs[3]), pltpu.VMEM(*outs[4]), pltpu.SemaphoreType.DMA((7,)),
        ],
        compiler_params=pltpu.CompilerParams(vmem_limit_bytes=6 << 20),
        cost_estimate=pl.CostEstimate(flops=1 << 16, bytes_accessed=1 << 19, transcendentals=0),
        name="finish",
    )(*args)


def solution(mesh):
    sizes = [size for _, size in AXES]
    split = Mesh(mesh.devices.reshape(*sizes, mesh.shape["tp"]), (*SP, "tp"))
    placed = (
        P(SP, "tp"),
        P(SP, "tp"),
        P(SP, None),
        P("tp", None),
        P(None, "tp"),
        P("tp"),
        P(SP),
        P(SP),
    )
    return jax.shard_map(
        shards,
        mesh=split,
        in_specs=placed,
        out_specs=(P(SP, "tp"), P(SP, "tp"), P(SP, "tp"), P(None, "tp"), P("tp")),
        check_vma=False,
    )
```

```python
import jax
import jax.numpy as jnp
from jax import lax
from jax.experimental import pallas as pl
from jax.experimental.pallas import tpu as pltpu
from jax.sharding import Mesh
from jax.sharding import PartitionSpec as P


SP = ("zh", "zl", "x", "c")
NEAR = ("zl", "x")
FAR = 16
CLOSE = 8
AXES = (("zh", FAR), ("zl", 2), ("x", 4), ("c", 2))
TP = 4
SUMS_ORDER = [2, 3, 0, 1]
OFFSETS = ((0, -1, -2, -3, 3, 2, 1, -4), (6, 7, 8, 5, -7, -6, -5, 4))
BLOCK = CLOSE * 2 * 8
NEAR_ORDER = [(place + 4) % CLOSE for place in range(CLOSE)]
GATHER_ORDER = [(place + 7) % (2 * CLOSE) for place in range(2 * CLOSE)]
TAPS = 31
SMALL = TAPS + 1
ROWS = 384
EDGE = 32
LANES = 128
HALVES = 2
WIDTH = HALVES * LANES
MODEL = 2048
OWN = 8
CHUNK = 64
WIDE = jnp.float32
NARROW = jnp.bfloat16


def shifted(value, axis, steps):
    count = lax.axis_size(axis)
    first, last = (max(0, -steps), min(count, count - steps))
    return lax.ppermute(value, axis, [(source, source + steps) for source in range(first, last)])


def exchange(pieces, axes, order=None):
    groups = order and [order]
    return lax.all_to_all(pieces, axes, 0, 0, tiled=True, axis_index_groups=groups)


def lanes(half):
    return slice(half * LANES, (half + 1) * LANES)


def column(row):
    return jnp.transpose(jnp.broadcast_to(row, (LANES, LANES)))


def call(body, outs, *args, flops=0, limit=6):
    shapes = [jax.ShapeDtypeStruct(shape, dtype) for shape, dtype in outs]
    size = sum(a.size * a.dtype.itemsize for a in (*args, *shapes))
    return pl.pallas_call(
        body,
        out_shape=shapes,
        compiler_params=pltpu.CompilerParams(vmem_limit_bytes=limit << 20),
        cost_estimate=pl.CostEstimate(flops=flops, bytes_accessed=size, transcendentals=0),
    )(*args)


def norm_backward(normed, factor, gain_row, upstream):
    active = normed * gain_row
    sig = jax.nn.sigmoid(active)
    hidden = (active * sig).astype(NARROW)
    d_active = upstream * sig * (1.0 + active * (1.0 - sig))
    d_normed = d_active * gain_row
    gain_part = jnp.sum((d_active * normed).reshape(normed.shape[0] // 8, 8, LANES), 0)
    return hidden, factor * d_normed, factor * normed, d_normed, d_normed * normed, gain_part


def convolve(source, half, taps_wide, start, size):
    conv = jnp.zeros((size, LANES), WIDE)
    for tap in range(TAPS):
        begin = start + tap + EDGE - TAPS + 1
        conv = conv + taps_wide[tap : tap + 1, lanes(half)] * source[half, begin : begin + size]
    return conv


def column_sums(source):
    return jnp.sum(jnp.transpose(source), 0, keepdims=True)


def both_blocks(cotangent, place, near):
    far, core = place[0] // (2 * CLOSE), place[0] % 2
    low, high = OFFSETS[0][near], OFFSETS[1][near]
    own = lax.rem(far + jnp.where(core == 0, low, high) + FAR, FAR)
    theirs = lax.rem(far + jnp.where(core == 0, high, low) + FAR, FAR)
    columns = [pl.ds(pl.multiple_of(block * BLOCK, BLOCK), BLOCK) for block in (own, theirs)]
    return jnp.concatenate([cotangent[:, columns[0]], cotangent[:, columns[1]]], 1)


def in_chunks(pairs, arrivals):
    copies = []
    for source, target, parts in pairs:
        for part in range(parts):
            if parts > 1:
                size = source.shape[0] // parts
                rows = pl.ds(part * size, size)
                ends = source.at[rows], target.at[rows]
            else:
                ends = source, target
            copies.append(pltpu.make_async_copy(*ends, arrivals.at[len(copies)]))
    return copies


def load(
    value, gate, taps, gain, mean, scale,
    end, held_value, held_gate, held_taps, held_gain, held_mean, held_scale,
    arrivals,
):
    pairs = (
        (value, held_value, 3), (gate, held_gate, 3), (taps, held_taps, 1), (gain, held_gain, 1),
        (mean, held_mean, 1), (scale, held_scale, 1),
    )
    copies = in_chunks(pairs, arrivals)
    for copy in copies:
        copy.start()
    for copy in copies:
        copy.wait()
    rows = slice(ROWS - EDGE, ROWS)
    sig = jax.nn.sigmoid(held_gate[rows].astype(WIDE))
    end[...] = (held_value[rows].astype(WIDE) * sig).astype(NARROW)


def forward(
    place, cotangent, weight, held_value, held_gate, taps, gain, mean, scale,
    gated, scaled, spread, sums, gain_part, first_upstream, first_cotangent, product,
    held, held_weight, arrivals,
    padded, taps_wide, mean_columns, scale_columns, sum_first, sum_second,
    hidden, normed, upstream,
):
    copies = in_chunks(((weight, held_weight, 4), (cotangent, held, 6)), arrivals)
    for copy in copies:
        copy.start()
    sum_first[0:EDGE] = jnp.zeros((EDGE, LANES), WIDE)
    sum_second[0:EDGE] = jnp.zeros((EDGE, LANES), WIDE)
    hidden[0:EDGE] = jnp.zeros((EDGE, WIDTH), WIDE)
    taps_wide[0:TAPS] = taps[...].astype(WIDE)
    for block in range(ROWS // LANES):
        rows = slice(block * LANES, (block + 1) * LANES)
        mean_columns[rows] = column(mean[rows].reshape(1, LANES))
        scale_columns[rows] = column(scale[rows].reshape(1, LANES))
    for half in range(HALVES):
        for start in range(0, ROWS, CHUNK):
            rows = slice(start, start + CHUNK)
            sig = jax.nn.sigmoid(held_gate[rows, lanes(half)].astype(WIDE))
            narrow = (held_value[rows, lanes(half)].astype(WIDE) * sig).astype(NARROW)
            gated[rows, lanes(half)] = narrow
            padded[half, EDGE + start : EDGE + start + CHUNK] = narrow.astype(WIDE)
        for start in range(EDGE, ROWS, EDGE):
            rows = slice(start, start + EDGE)
            conv = convolve(padded, half, taps_wide, start, EDGE)
            normed[half, rows] = (conv - mean_columns[rows]) * scale_columns[rows]
    for copy in copies:
        copy.wait()
    upstream[...] = lax.dot_general(
        held[...], held_weight[...], (((1,), (1,)), ((), ())), preferred_element_type=WIDE
    )
    first_upstream[...] = upstream[0:EDGE]
    first_cotangent[...] = held[0:EDGE]
    for half in range(HALVES):
        gain_row = gain[0:1, lanes(half)]
        gain_sum = jnp.zeros((8, LANES), WIDE)
        for start in range(EDGE, ROWS, EDGE):
            rows = slice(start, start + EDGE)
            narrow, own_scaled, own_spread, first, second, part = norm_backward(
                normed[half, rows], scale_columns[rows], gain_row, upstream[rows, lanes(half)]
            )
            hidden[rows, lanes(half)] = narrow.astype(WIDE)
            scaled[half, start - EDGE : start] = own_scaled
            spread[half, start - EDGE : start] = own_spread
            gain_sum = gain_sum + part
            if half == 0:
                sum_first[rows] = first
                sum_second[rows] = second
            else:
                sum_first[rows] = sum_first[rows] + first
                sum_second[rows] = sum_second[rows] + second
        gain_part[half] = gain_sum
    found = [
        column_sums(source[block * LANES : (block + 1) * LANES])
        for source in (sum_first, sum_second)
        for block in range(ROWS // LANES)
    ]
    sums[...] = jnp.concatenate([*found, jnp.zeros((2, LANES), WIDE)], 0)
    turned = jnp.transpose(hidden[...]).astype(NARROW)
    for near in range(CLOSE):
        product[near] = jnp.dot(
            turned, both_blocks(held, place, near), preferred_element_type=WIDE
        )


def head(
    halo, gated, upstream, taps, gain, mean, scale, sums, gain_part,
    scaled, spread, hidden, message, gain_total,
    padded, taps_wide, turned,
):
    taps_wide[0:TAPS] = taps[...].astype(WIDE)
    rows = slice(0, EDGE)
    mean_columns = column(mean[0:LANES].reshape(1, LANES))[rows]
    scale_columns = column(scale[0:LANES].reshape(1, LANES))[rows]
    turned[...] = jnp.zeros((2, LANES, LANES), WIDE)
    for half in range(HALVES):
        padded[half, rows] = halo[:, lanes(half)].astype(WIDE)
        padded[half, EDGE:] = gated[rows, lanes(half)].astype(WIDE)
    for half in range(HALVES):
        conv = convolve(padded, half, taps_wide, 0, EDGE)
        normed = (conv - mean_columns) * scale_columns
        narrow, own_scaled, own_spread, first, second, part = norm_backward(
            normed, scale_columns, gain[0:1, lanes(half)], upstream[rows, lanes(half)]
        )
        hidden[:, lanes(half)] = narrow
        scaled[half] = own_scaled
        spread[half] = own_spread
        gain_total[half] = gain_part[half] + part
        turned[0, rows] = turned[0, rows] + first
        turned[1, rows] = turned[1, rows] + second
    blocks = ROWS // LANES
    total = sums[...]
    extra = [column_sums(turned[0]), column_sums(turned[1])]
    none = jnp.zeros((blocks - 1, LANES), WIDE)
    last = jnp.zeros((2, LANES), WIDE)
    total = total + jnp.concatenate([extra[0], none, extra[1], none, last], 0)
    for peer in range(TP):
        message[peer] = total


def head_product(cotangent, hidden, place, near, side):
    columns = both_blocks(cotangent, place, near)[:, side * BLOCK : (side + 1) * BLOCK]
    return lax.dot_general(
        hidden[...], columns, (((0,), (0,)), ((), ())), preferred_element_type=WIDE
    )


def backward(
    place, sums, scaled, spread, first_scaled, first_spread, halo, gated, scale, gain_part,
    first_cotangent, first_hidden, product,
    other, small, extended,
    padded,
):
    for half in range(HALVES):
        padded[half, 0:EDGE] = halo[:, lanes(half)].astype(WIDE)
        padded[half, EDGE:] = gated[:, lanes(half)].astype(WIDE)
    total = (sums[0] + sums[1]) + (sums[2] + sums[3])
    total = total * (1.0 / (TP * WIDTH))
    blocks = ROWS // LANES
    for half in range(HALVES):
        extended[half, 0:EDGE] = jnp.zeros((EDGE, LANES), WIDE)
        extended[half, EDGE + ROWS :] = jnp.zeros((EDGE, LANES), WIDE)
    for block in range(blocks):
        rows = slice(block * LANES, (block + 1) * LANES)
        first = column(total[block : block + 1] * scale[rows].reshape(1, LANES))
        second = column(total[blocks + block : blocks + block + 1])
        for half in range(HALVES):
            cut = 0
            if block == 0:
                cut = EDGE
                d_conv = first_scaled[half] - first[0:cut] - first_spread[half] * second[0:cut]
                extended[half, EDGE : EDGE + cut] = d_conv
            rows = slice(block * LANES + cut - EDGE, (block + 1) * LANES - EDGE)
            d_conv = scaled[half, rows] - first[cut:] - spread[half, rows] * second[cut:]
            extended[half, EDGE + block * LANES + cut : EDGE + (block + 1) * LANES] = d_conv
    lead = EDGE - TAPS + 1
    groups = ROWS // 8
    for offset in range(8):
        steps = [q for q in range(5) if 0 <= 8 * q + offset - lead < TAPS]
        found = {(half, q): jnp.zeros((8, LANES), WIDE) for half in range(HALVES) for q in steps}
        loaded = {}
        for m in range(groups + steps[-1]):
            for half in range(HALVES):
                if m < groups:
                    begin = EDGE + 8 * m
                    loaded[half, m] = extended[half, begin : begin + 8]
                moved = padded[half, 8 * m + offset : 8 * m + offset + 8]
                for q in steps:
                    if 0 <= m - q < groups:
                        found[half, q] = found[half, q] + loaded[half, m - q] * moved
        for half in range(HALVES):
            for q in steps:
                tap = 8 * q + offset - lead
                small[tap : tap + 1, lanes(half)] = jnp.sum(found[half, q], 0, keepdims=True)
        near = offset
        whole = product[near, :, BLOCK:] + head_product(
            first_cotangent, first_hidden, place, near, 1
        )
        other[near * WIDTH : (near + 1) * WIDTH] = whole.astype(NARROW)
    for half in range(HALVES):
        small[TAPS:SMALL, lanes(half)] = jnp.sum(gain_part[half], 0, keepdims=True)
    for half in range(HALVES):
        value = small[:, lanes(half)]
        top = value.astype(NARROW)
        begin = CLOSE * WIDTH + half * 2 * SMALL
        other[begin : begin + SMALL] = top
        other[begin + SMALL : begin + 2 * SMALL] = (value - top.astype(WIDE)).astype(NARROW)


def pack(mine, small, other, pieces):
    for half in range(HALVES):
        begin = CLOSE * WIDTH + half * 2 * SMALL
        top = other[begin : begin + SMALL].astype(WIDE)
        rest = other[begin + SMALL : begin + 2 * SMALL].astype(WIDE)
        both = (small[:, lanes(half)] + (top + rest)).astype(NARROW)
        for near in range(CLOSE):
            pieces[near, WIDTH + half * SMALL : WIDTH + (half + 1) * SMALL] = both
    for near in range(CLOSE):
        for start in range(0, WIDTH, 64):
            rows = slice(start, start + 64)
            there = other[near * WIDTH + start : near * WIDTH + start + 64].astype(WIDE)
            pieces[NEAR_ORDER.index(near), rows] = (mine[near, rows] + there).astype(NARROW)


def gated_gradient(
    place, extended, taps, value, gate, first_cotangent, first_hidden, product,
    value_grad, gate_grad, margin, last, mine,
    taps_wide,
):
    for near in range(CLOSE):
        mine[near] = product[near, :, 0:BLOCK] + head_product(
            first_cotangent, first_hidden, place, near, 0
        )
    taps_wide[0:TAPS] = taps[...].astype(WIDE)
    for half in range(HALVES):
        for start in range(0, EDGE + ROWS, EDGE):
            found = jnp.zeros((EDGE, LANES), WIDE)
            for tap in range(TAPS):
                begin = start + TAPS - 1 - tap
                found = found + taps_wide[tap : tap + 1, lanes(half)] * extended[half, begin : begin + EDGE]
            if start == 0:
                margin[half] = found
                continue
            rows = slice(start - EDGE, start)
            sig = jax.nn.sigmoid(gate[rows, lanes(half)].astype(WIDE))
            slope = value[rows, lanes(half)].astype(WIDE) * sig * (1.0 - sig)
            if start == ROWS:
                last[0, half], last[1, half], last[2, half] = found, sig, slope
            else:
                value_grad[rows, lanes(half)] = (found * sig).astype(NARROW)
                gate_grad[rows, lanes(half)] = (found * slope).astype(NARROW)


def fold_near(arrived, payload):
    for start in range(0, WIDTH + 2 * SMALL, 64):
        rows = slice(start, start + 64)
        total = arrived[0, rows].astype(WIDE)
        for near in range(1, CLOSE):
            total = total + arrived[near, rows].astype(WIDE)
        payload[rows] = total.astype(NARROW)


def hand_out(payload, message):
    weights = jnp.transpose(payload[0:WIDTH].astype(WIDE)).astype(NARROW)
    small = jnp.concatenate([payload[WIDTH : WIDTH + SMALL], payload[WIDTH + SMALL :]], 1)
    for position, member in enumerate(GATHER_ORDER):
        message[position, 0:OWN] = weights[member * OWN : (member + 1) * OWN]
        message[position, OWN:] = small


def totals(arrived, total):
    for start in range(0, OWN + SMALL, 8):
        rows = slice(start, start + 8)
        found = arrived[0, rows].astype(WIDE)
        for position in range(1, 2 * CLOSE):
            found = found + arrived[position, rows].astype(WIDE)
        total[rows] = found


def finish(
    total, value_part, gate_part, last, late,
    value_grad, gate_grad, weight_grad, taps_grad, gain_grad,
    value_end, gate_end, taps_held, gain_held, departures,
):
    main, end = pl.ds(0, ROWS - EDGE), pl.ds(ROWS - EDGE, EDGE)
    taps_held[...] = total[OWN : OWN + TAPS]
    gain_held[...] = total[OWN + TAPS :]
    for half in range(HALVES):
        grad = last[0, half] + late[half]
        value_end[:, lanes(half)] = (grad * last[1, half]).astype(NARROW)
        gate_end[:, lanes(half)] = (grad * last[2, half]).astype(NARROW)
    copies = [
        pltpu.make_async_copy(value_part, value_grad.at[main], departures.at[0]),
        pltpu.make_async_copy(gate_part, gate_grad.at[main], departures.at[1]),
        pltpu.make_async_copy(total.at[pl.ds(0, OWN)], weight_grad, departures.at[2]),
        pltpu.make_async_copy(taps_held, taps_grad, departures.at[3]),
        pltpu.make_async_copy(gain_held, gain_grad, departures.at[4]),
        pltpu.make_async_copy(value_end, value_grad.at[end], departures.at[5]),
        pltpu.make_async_copy(gate_end, gate_grad.at[end], departures.at[6]),
    ]
    for copy in copies:
        copy.start()
    for copy in copies:
        copy.wait()


def to_block(value):
    pairs = []
    for far in range(FAR):
        for near in range(CLOSE):
            for core in range(2):
                target = (far + OFFSETS[core][near]) % FAR
                pairs.append(((far * CLOSE + near) * 2 + core, (target * CLOSE + near) * 2 + core))
    return lax.ppermute(value, SP, pairs)


def shards(
    proj_value, proj_gate, out_cotangent, out_weight, conv_taps, norm_gain, row_mean, row_scale
):
    row_gain = norm_gain.reshape(1, WIDTH)
    end, proj_value, proj_gate, conv_taps, row_gain, row_mean, row_scale = load_call(
        proj_value, proj_gate, conv_taps, row_gain, row_mean, row_scale
    )
    halo = shifted(end, SP, 1)
    split = (HALVES, ROWS, LANES)
    rest = (HALVES, ROWS - EDGE, LANES)
    sides = pltpu.VMEM((HALVES, EDGE + ROWS, LANES), WIDE)
    taps_scratch = pltpu.VMEM((TAPS + 1, WIDTH), WIDE)
    place = lax.axis_index(SP).reshape(1)
    narrow = ((ROWS, WIDTH), NARROW)
    gated, scaled, spread, sums, gain_part, first_upstream, first_cotangent, product = (
        scalar_call(
            forward,
            [
                narrow, (rest, WIDE), (rest, WIDE), ((8, LANES), WIDE),
                ((HALVES, 8, LANES), WIDE), ((EDGE, WIDTH), WIDE), ((EDGE, MODEL), NARROW),
                ((CLOSE, WIDTH, 2 * BLOCK), WIDE),
            ],
            place, out_cotangent, out_weight, proj_value, proj_gate,
            conv_taps, row_gain, row_mean, row_scale, in_hbm=2,
            scratch=[
                pltpu.VMEM((ROWS, MODEL), NARROW), pltpu.VMEM((WIDTH, MODEL), NARROW),
                pltpu.SemaphoreType.DMA((10,)),
                sides, taps_scratch, *([pltpu.VMEM((ROWS, LANES), WIDE)] * 4),
                pltpu.VMEM((ROWS, WIDTH), WIDE), pltpu.VMEM(split, WIDE),
                pltpu.VMEM((ROWS, WIDTH), WIDE),
            ],
            flops=4 * ROWS * WIDTH * MODEL, limit=12,
        )
    )
    edge = (HALVES, EDGE, LANES)
    first_scaled, first_spread, first_hidden, message, gain_part = call_with(
        head,
        [
            (edge, WIDE), (edge, WIDE), ((EDGE, WIDTH), NARROW),
            ((TP, 8, LANES), WIDE), ((HALVES, 8, LANES), WIDE),
        ],
        [
            pltpu.VMEM((HALVES, 2 * EDGE, LANES), WIDE),
            taps_scratch,
            pltpu.VMEM((2, LANES, LANES), WIDE),
        ],
        halo, gated, first_upstream, conv_taps, row_gain, row_mean, row_scale, sums,
        gain_part, flops=10 * ROWS * WIDTH,
    )
    sums = exchange(message, "tp", SUMS_ORDER)
    rows = CLOSE * WIDTH + 4 * SMALL
    other, small, extended = scalar_call(
        backward,
        [
            ((rows, BLOCK), NARROW), ((SMALL, WIDTH), WIDE),
            ((HALVES, ROWS + 2 * EDGE, LANES), WIDE),
        ],
        place, sums, scaled, spread, first_scaled, first_spread, halo, gated, row_scale, gain_part,
        first_cotangent, first_hidden, product, scratch=[sides], flops=100 * ROWS * WIDTH,
    )
    other = lax.ppermute(other, "c", [(0, 1), (1, 0)])
    main = ((ROWS - EDGE, WIDTH), NARROW)
    value_part, gate_part, margin, last, mine = scalar_call(
        gated_gradient,
        [main, main, (edge, WIDE), ((3, *edge), WIDE), ((CLOSE, WIDTH, BLOCK), WIDE)],
        place, extended, conv_taps, proj_value, proj_gate, first_cotangent, first_hidden,
        product, scratch=[taps_scratch], flops=100 * ROWS * WIDTH,
    )
    (pieces,) = call(
        pack, [((CLOSE, WIDTH + 2 * SMALL, BLOCK), NARROW)], mine, small, other, flops=1 << 20
    )
    arrived = exchange(pieces, NEAR, NEAR_ORDER)
    (payload,) = call(
        fold_near, [((WIDTH + 2 * SMALL, BLOCK), NARROW)], arrived, flops=1 << 20
    )
    payload = to_block(payload)
    late = shifted(margin, SP, -1)
    (message,) = call(hand_out, [((2 * CLOSE, OWN + SMALL, WIDTH), NARROW)], payload, flops=1 << 16)
    arrived = exchange(message, (*NEAR, "c"), GATHER_ORDER)
    (total,) = call(totals, [((OWN + SMALL, WIDTH), WIDE)], arrived, flops=1 << 20)
    value_grad, gate_grad, weight_grad, taps_grad, gain_grad = last_call(
        [narrow, narrow, ((OWN, WIDTH), WIDE), ((TAPS, WIDTH), WIDE), ((1, WIDTH), WIDE)],
        total, value_part, gate_part, last, late,
    )
    return (value_grad, gate_grad, weight_grad, taps_grad, gain_grad.reshape(WIDTH))


def call_with(body, outs, scratch, *args, flops=0, limit=6):
    shapes = [jax.ShapeDtypeStruct(shape, dtype) for shape, dtype in outs]
    size = sum(a.size * a.dtype.itemsize for a in (*args, *shapes))
    return pl.pallas_call(
        body,
        out_shape=shapes,
        scratch_shapes=scratch,
        compiler_params=pltpu.CompilerParams(vmem_limit_bytes=limit << 20),
        cost_estimate=pl.CostEstimate(flops=flops, bytes_accessed=size, transcendentals=0),
    )(*args)


def scalar_call(
    body, outs, scalar, *args, scratch=(), flops=1 << 20, limit=6, in_hbm=0
):
    shapes = [jax.ShapeDtypeStruct(shape, dtype) for shape, dtype in outs]
    size = sum(a.size * a.dtype.itemsize for a in (*args, *shapes))
    whole = pl.BlockSpec(memory_space=pltpu.VMEM)
    far = [pltpu.with_memory_space_constraint(a, pltpu.HBM) for a in args[:in_hbm]]
    return pl.pallas_call(
        body,
        out_shape=shapes,
        in_specs=[
            pl.BlockSpec(memory_space=pltpu.SMEM),
            *([pl.BlockSpec(memory_space=pltpu.HBM)] * in_hbm),
            *([whole] * (len(args) - in_hbm)),
        ],
        out_specs=[whole] * len(shapes),
        scratch_shapes=scratch,
        compiler_params=pltpu.CompilerParams(vmem_limit_bytes=limit << 20),
        cost_estimate=pl.CostEstimate(flops=flops, bytes_accessed=size, transcendentals=0),
    )(scalar, *far, *args[in_hbm:])


def load_call(*args):
    held = [pltpu.with_memory_space_constraint(a, pltpu.HBM) for a in args]
    shapes = [jax.ShapeDtypeStruct((EDGE, WIDTH), NARROW)]
    shapes += [jax.ShapeDtypeStruct(a.shape, a.dtype) for a in args]
    return pl.pallas_call(
        load,
        out_shape=shapes,
        in_specs=[pl.BlockSpec(memory_space=pltpu.HBM)] * len(args),
        out_specs=[pl.BlockSpec(memory_space=pltpu.VMEM)] * len(shapes),
        scratch_shapes=[pltpu.SemaphoreType.DMA((10,))],
        compiler_params=pltpu.CompilerParams(vmem_limit_bytes=6 << 20),
        cost_estimate=pl.CostEstimate(flops=1 << 16, bytes_accessed=1 << 19, transcendentals=0),
        name="load",
    )(*held)


def last_call(outs, *args):
    edge = pltpu.VMEM((EDGE, WIDTH), NARROW)
    return pl.pallas_call(
        finish,
        out_shape=[pltpu.HBM(*out) for out in outs],
        in_specs=[pl.BlockSpec(memory_space=pltpu.VMEM)] * len(args),
        out_specs=[pl.BlockSpec(memory_space=pltpu.HBM)] * len(outs),
        scratch_shapes=[
            edge, edge, pltpu.VMEM(*outs[3]), pltpu.VMEM(*outs[4]), pltpu.SemaphoreType.DMA((7,)),
        ],
        compiler_params=pltpu.CompilerParams(vmem_limit_bytes=6 << 20),
        cost_estimate=pl.CostEstimate(flops=1 << 16, bytes_accessed=1 << 19, transcendentals=0),
        name="finish",
    )(*args)


def solution(mesh):
    sizes = [size for _, size in AXES]
    split = Mesh(mesh.devices.reshape(*sizes, mesh.shape["tp"]), (*SP, "tp"))
    placed = (
        P(SP, "tp"),
        P(SP, "tp"),
        P(SP, None),
        P("tp", None),
        P(None, "tp"),
        P("tp"),
        P(SP),
        P(SP),
    )
    return jax.shard_map(
        shards,
        mesh=split,
        in_specs=placed,
        out_specs=(P(SP, "tp"), P(SP, "tp"), P(SP, "tp"), P(None, "tp"), P("tp")),
        check_vma=False,
    )
```

```python
import jax
import jax.numpy as jnp
from jax import lax
from jax.experimental import pallas as pl
from jax.experimental.pallas import tpu as pltpu
from jax.sharding import Mesh
from jax.sharding import PartitionSpec as P


SP = ("zh", "zl", "x", "c")
NEAR = ("zl", "x")
FAR = 16
CLOSE = 8
AXES = (("zh", FAR), ("zl", 2), ("x", 4), ("c", 2))
TP = 4
SUMS_ORDER = [2, 3, 0, 1]
OFFSETS = ((0, -1, -2, -3, 3, 2, 1, -4), (6, 7, 8, 5, -7, -6, -5, 4))
BLOCK = CLOSE * 2 * 8
NEAR_ORDER = [(place + 4) % CLOSE for place in range(CLOSE)]
GATHER_ORDER = [(place + 7) % (2 * CLOSE) for place in range(2 * CLOSE)]
TAPS = 31
SMALL = TAPS + 1
ROWS = 384
EDGE = 32
LANES = 128
HALVES = 2
WIDTH = HALVES * LANES
MODEL = 2048
OWN = 8
CHUNK = 64
WIDE = jnp.float32
NARROW = jnp.bfloat16


def shifted(value, axis, steps):
    count = lax.axis_size(axis)
    first, last = (max(0, -steps), min(count, count - steps))
    return lax.ppermute(value, axis, [(source, source + steps) for source in range(first, last)])


def exchange(pieces, axes, order=None):
    groups = order and [order]
    return lax.all_to_all(pieces, axes, 0, 0, tiled=True, axis_index_groups=groups)


def lanes(half):
    return slice(half * LANES, (half + 1) * LANES)


def column(row):
    return jnp.transpose(jnp.broadcast_to(row, (LANES, LANES)))


def call(body, outs, *args, flops=0, limit=6):
    shapes = [jax.ShapeDtypeStruct(shape, dtype) for shape, dtype in outs]
    size = sum(a.size * a.dtype.itemsize for a in (*args, *shapes))
    return pl.pallas_call(
        body,
        out_shape=shapes,
        compiler_params=pltpu.CompilerParams(vmem_limit_bytes=limit << 20),
        cost_estimate=pl.CostEstimate(flops=flops, bytes_accessed=size, transcendentals=0),
    )(*args)


def norm_backward(normed, factor, gain_row, upstream):
    active = normed * gain_row
    sig = jax.nn.sigmoid(active)
    hidden = (active * sig).astype(NARROW)
    d_active = upstream * sig * (1.0 + active * (1.0 - sig))
    d_normed = d_active * gain_row
    gain_part = jnp.sum((d_active * normed).reshape(normed.shape[0] // 8, 8, LANES), 0)
    return hidden, factor * d_normed, factor * normed, d_normed, d_normed * normed, gain_part


def convolve(source, half, taps_wide, start, size):
    conv = jnp.zeros((size, LANES), WIDE)
    for tap in range(TAPS):
        begin = start + tap + EDGE - TAPS + 1
        conv = conv + taps_wide[tap : tap + 1, lanes(half)] * source[half, begin : begin + size]
    return conv


def column_sums(source):
    return jnp.sum(jnp.transpose(source), 0, keepdims=True)


def block_columns(place, near, side):
    far, core = place[0] // (2 * CLOSE), place[0] % 2
    low, high = OFFSETS[0][near], OFFSETS[1][near]
    step = jnp.where(core == side, low, high)
    block = lax.rem(far + step + FAR, FAR)
    return pl.ds(pl.multiple_of(block * BLOCK, BLOCK), BLOCK)


def main_product(turned, cotangent, place, side, product):
    for near in range(0, CLOSE, 2):
        pair = [cotangent[:, block_columns(place, near + i, side)] for i in range(2)]
        both = jnp.dot(turned, jnp.concatenate(pair, 1), preferred_element_type=WIDE)
        for i in range(2):
            product[near + i] = both[:, i * BLOCK : (i + 1) * BLOCK]


def forward(
    place, value, gate, cotangent, weight, far_taps, far_gain, far_mean, far_scale,
    gated, scaled, spread, sums, gain_part, first_upstream, held, across, product,
    held_value, held_gate, held_weight, taps, gain, mean, scale, arrivals,
    padded, taps_wide, mean_columns, scale_columns, sum_first, sum_second,
    hidden, normed, upstream,
):
    copies = [
        pltpu.make_async_copy(source, target, arrivals.at[i])
        for i, (source, target) in enumerate(
            (
                (value, held_value), (gate, held_gate), (far_taps, taps), (far_mean, mean),
                (far_scale, scale), (far_gain, gain), (weight, held_weight), (cotangent, held),
            )
        )
    ]
    for copy in copies:
        copy.start()
    sum_first[0:EDGE] = jnp.zeros((EDGE, LANES), WIDE)
    sum_second[0:EDGE] = jnp.zeros((EDGE, LANES), WIDE)
    hidden[0:EDGE] = jnp.zeros((EDGE, WIDTH), WIDE)
    for copy in copies[:6]:
        copy.wait()
    taps_wide[0:TAPS] = taps[...].astype(WIDE)
    for block in range(ROWS // LANES):
        rows = slice(block * LANES, (block + 1) * LANES)
        mean_columns[rows] = column(mean[rows].reshape(1, LANES))
        scale_columns[rows] = column(scale[rows].reshape(1, LANES))
    for half in range(HALVES):
        for start in range(0, ROWS, CHUNK):
            rows = slice(start, start + CHUNK)
            sig = jax.nn.sigmoid(held_gate[rows, lanes(half)].astype(WIDE))
            narrow = (held_value[rows, lanes(half)].astype(WIDE) * sig).astype(NARROW)
            gated[rows, lanes(half)] = narrow
            padded[half, EDGE + start : EDGE + start + CHUNK] = narrow.astype(WIDE)
        for start in range(EDGE, ROWS, EDGE):
            rows = slice(start, start + EDGE)
            conv = convolve(padded, half, taps_wide, start, EDGE)
            normed[half, rows] = (conv - mean_columns[rows]) * scale_columns[rows]
    copies[6].wait()
    copies[7].wait()
    upstream[...] = lax.dot_general(
        held[...], held_weight[...], (((1,), (1,)), ((), ())), preferred_element_type=WIDE
    )
    first_upstream[...] = upstream[0:EDGE]
    for half in range(HALVES):
        gain_row = gain[0:1, lanes(half)]
        gain_sum = jnp.zeros((8, LANES), WIDE)
        for start in range(EDGE, ROWS, EDGE):
            rows = slice(start, start + EDGE)
            narrow, own_scaled, own_spread, first, second, part = norm_backward(
                normed[half, rows], scale_columns[rows], gain_row, upstream[rows, lanes(half)]
            )
            hidden[rows, lanes(half)] = narrow.astype(WIDE)
            scaled[half, start - EDGE : start] = own_scaled
            spread[half, start - EDGE : start] = own_spread
            gain_sum = gain_sum + part
            if half == 0:
                sum_first[rows] = first
                sum_second[rows] = second
            else:
                sum_first[rows] = sum_first[rows] + first
                sum_second[rows] = sum_second[rows] + second
        gain_part[half] = gain_sum
    found = [
        column_sums(source[block * LANES : (block + 1) * LANES])
        for source in (sum_first, sum_second)
        for block in range(ROWS // LANES)
    ]
    sums[...] = jnp.concatenate([*found, jnp.zeros((2, LANES), WIDE)], 0)
    across[...] = jnp.transpose(hidden[...]).astype(NARROW)
    main_product(across[...], held, place, 1, product)


def head(
    halo, gated, upstream, taps, gain, mean, scale, sums, gain_part,
    scaled, spread, hidden, message, gain_total,
    padded, taps_wide, turned,
):
    taps_wide[0:TAPS] = taps[...].astype(WIDE)
    rows = slice(0, EDGE)
    mean_columns = column(mean[0:LANES].reshape(1, LANES))[rows]
    scale_columns = column(scale[0:LANES].reshape(1, LANES))[rows]
    turned[...] = jnp.zeros((2, LANES, LANES), WIDE)
    for half in range(HALVES):
        padded[half, rows] = halo[:, lanes(half)].astype(WIDE)
        padded[half, EDGE:] = gated[rows, lanes(half)].astype(WIDE)
    for half in range(HALVES):
        conv = convolve(padded, half, taps_wide, 0, EDGE)
        normed = (conv - mean_columns) * scale_columns
        narrow, own_scaled, own_spread, first, second, part = norm_backward(
            normed, scale_columns, gain[0:1, lanes(half)], upstream[rows, lanes(half)]
        )
        hidden[:, lanes(half)] = narrow
        scaled[half] = own_scaled
        spread[half] = own_spread
        gain_total[half] = gain_part[half] + part
        turned[0, rows] = turned[0, rows] + first
        turned[1, rows] = turned[1, rows] + second
    blocks = ROWS // LANES
    total = sums[...]
    extra = [column_sums(turned[0]), column_sums(turned[1])]
    none = jnp.zeros((blocks - 1, LANES), WIDE)
    last = jnp.zeros((2, LANES), WIDE)
    total = total + jnp.concatenate([extra[0], none, extra[1], none, last], 0)
    for peer in range(TP):
        message[peer] = total


def head_product(cotangent, hidden, place, near, side):
    columns = cotangent[0:EDGE, block_columns(place, near, side)]
    return lax.dot_general(
        hidden[...], columns, (((0,), (0,)), ((), ())), preferred_element_type=WIDE
    )


def backward(
    place, sums, scaled, spread, first_scaled, first_spread, halo, gated, scale, gain_part,
    cotangent, first_hidden, product,
    other, small, extended,
    padded,
):
    for half in range(HALVES):
        padded[half, 0:EDGE] = halo[:, lanes(half)].astype(WIDE)
        padded[half, EDGE:] = gated[:, lanes(half)].astype(WIDE)
    total = (sums[0] + sums[1]) + (sums[2] + sums[3])
    total = total * (1.0 / (TP * WIDTH))
    blocks = ROWS // LANES
    for half in range(HALVES):
        extended[half, 0:EDGE] = jnp.zeros((EDGE, LANES), WIDE)
        extended[half, EDGE + ROWS :] = jnp.zeros((EDGE, LANES), WIDE)
    for block in range(blocks):
        rows = slice(block * LANES, (block + 1) * LANES)
        first = column(total[block : block + 1] * scale[rows].reshape(1, LANES))
        second = column(total[blocks + block : blocks + block + 1])
        for half in range(HALVES):
            cut = 0
            if block == 0:
                cut = EDGE
                d_conv = first_scaled[half] - first[0:cut] - first_spread[half] * second[0:cut]
                extended[half, EDGE : EDGE + cut] = d_conv
            rows = slice(block * LANES + cut - EDGE, (block + 1) * LANES - EDGE)
            d_conv = scaled[half, rows] - first[cut:] - spread[half, rows] * second[cut:]
            extended[half, EDGE + block * LANES + cut : EDGE + (block + 1) * LANES] = d_conv
    lead = EDGE - TAPS + 1
    groups = ROWS // 8
    for offset in range(8):
        steps = [q for q in range(5) if 0 <= 8 * q + offset - lead < TAPS]
        found = {(half, q): jnp.zeros((8, LANES), WIDE) for half in range(HALVES) for q in steps}
        loaded = {}
        for m in range(groups + steps[-1]):
            for half in range(HALVES):
                if m < groups:
                    begin = EDGE + 8 * m
                    loaded[half, m] = extended[half, begin : begin + 8]
                moved = padded[half, 8 * m + offset : 8 * m + offset + 8]
                for q in steps:
                    if 0 <= m - q < groups:
                        found[half, q] = found[half, q] + loaded[half, m - q] * moved
        for half in range(HALVES):
            for q in steps:
                tap = 8 * q + offset - lead
                small[tap : tap + 1, lanes(half)] = jnp.sum(found[half, q], 0, keepdims=True)
        near = offset
        whole = product[near] + head_product(cotangent, first_hidden, place, near, 1)
        other[near * WIDTH : (near + 1) * WIDTH] = whole.astype(NARROW)
    for half in range(HALVES):
        small[TAPS:SMALL, lanes(half)] = jnp.sum(gain_part[half], 0, keepdims=True)
    for half in range(HALVES):
        value = small[:, lanes(half)]
        top = value.astype(NARROW)
        begin = CLOSE * WIDTH + half * 2 * SMALL
        other[begin : begin + SMALL] = top
        other[begin + SMALL : begin + 2 * SMALL] = (value - top.astype(WIDE)).astype(NARROW)


def pack(mine, small, other, pieces):
    for half in range(HALVES):
        begin = CLOSE * WIDTH + half * 2 * SMALL
        top = other[begin : begin + SMALL].astype(WIDE)
        rest = other[begin + SMALL : begin + 2 * SMALL].astype(WIDE)
        both = (small[:, lanes(half)] + (top + rest)).astype(NARROW)
        for near in range(CLOSE):
            pieces[near, WIDTH + half * SMALL : WIDTH + (half + 1) * SMALL] = both
    for near in range(CLOSE):
        for start in range(0, WIDTH, 64):
            rows = slice(start, start + 64)
            there = other[near * WIDTH + start : near * WIDTH + start + 64].astype(WIDE)
            pieces[NEAR_ORDER.index(near), rows] = (mine[near, rows] + there).astype(NARROW)


def gated_gradient(
    place, extended, taps, value, gate, cotangent, first_hidden, across,
    value_grad, gate_grad, margin, last, mine,
    taps_wide,
):
    main_product(across[...], cotangent, place, 0, mine)
    for near in range(CLOSE):
        mine[near] = mine[near] + head_product(cotangent, first_hidden, place, near, 0)
    taps_wide[0:TAPS] = taps[...].astype(WIDE)
    for half in range(HALVES):
        for start in range(0, EDGE + ROWS, EDGE):
            found = jnp.zeros((EDGE, LANES), WIDE)
            for tap in range(TAPS):
                begin = start + TAPS - 1 - tap
                found = found + taps_wide[tap : tap + 1, lanes(half)] * extended[half, begin : begin + EDGE]
            if start == 0:
                margin[half] = found
                continue
            rows = slice(start - EDGE, start)
            sig = jax.nn.sigmoid(gate[rows, lanes(half)].astype(WIDE))
            slope = value[rows, lanes(half)].astype(WIDE) * sig * (1.0 - sig)
            if start == ROWS:
                last[0, half], last[1, half], last[2, half] = found, sig, slope
            else:
                value_grad[rows, lanes(half)] = (found * sig).astype(NARROW)
                gate_grad[rows, lanes(half)] = (found * slope).astype(NARROW)


def fold_near(arrived, payload):
    for start in range(0, WIDTH + 2 * SMALL, 64):
        rows = slice(start, start + 64)
        total = arrived[0, rows].astype(WIDE)
        for near in range(1, CLOSE):
            total = total + arrived[near, rows].astype(WIDE)
        payload[rows] = total.astype(NARROW)


def hand_out(payload, message):
    weights = jnp.transpose(payload[0:WIDTH].astype(WIDE)).astype(NARROW)
    small = jnp.concatenate([payload[WIDTH : WIDTH + SMALL], payload[WIDTH + SMALL :]], 1)
    for position, member in enumerate(GATHER_ORDER):
        message[position, 0:OWN] = weights[member * OWN : (member + 1) * OWN]
        message[position, OWN:] = small


def totals(arrived, total):
    for start in range(0, OWN + SMALL, 8):
        rows = slice(start, start + 8)
        found = arrived[0, rows].astype(WIDE)
        for position in range(1, 2 * CLOSE):
            found = found + arrived[position, rows].astype(WIDE)
        total[rows] = found


def finish(
    total, value_part, gate_part, last, late,
    value_grad, gate_grad, weight_grad, taps_grad, gain_grad,
    value_end, gate_end, taps_held, gain_held, departures,
):
    main, end = pl.ds(0, ROWS - EDGE), pl.ds(ROWS - EDGE, EDGE)
    taps_held[...] = total[OWN : OWN + TAPS]
    gain_held[...] = total[OWN + TAPS :]
    for half in range(HALVES):
        grad = last[0, half] + late[half]
        value_end[:, lanes(half)] = (grad * last[1, half]).astype(NARROW)
        gate_end[:, lanes(half)] = (grad * last[2, half]).astype(NARROW)
    copies = [
        pltpu.make_async_copy(value_part, value_grad.at[main], departures.at[0]),
        pltpu.make_async_copy(gate_part, gate_grad.at[main], departures.at[1]),
        pltpu.make_async_copy(total.at[pl.ds(0, OWN)], weight_grad, departures.at[2]),
        pltpu.make_async_copy(taps_held, taps_grad, departures.at[3]),
        pltpu.make_async_copy(gain_held, gain_grad, departures.at[4]),
        pltpu.make_async_copy(value_end, value_grad.at[end], departures.at[5]),
        pltpu.make_async_copy(gate_end, gate_grad.at[end], departures.at[6]),
    ]
    for copy in copies:
        copy.start()
    for copy in copies:
        copy.wait()


def to_block(value):
    pairs = []
    for far in range(FAR):
        for near in range(CLOSE):
            for core in range(2):
                target = (far + OFFSETS[core][near]) % FAR
                pairs.append(((far * CLOSE + near) * 2 + core, (target * CLOSE + near) * 2 + core))
    return lax.ppermute(value, SP, pairs)


def shards(
    proj_value, proj_gate, out_cotangent, out_weight, conv_taps, norm_gain, row_mean, row_scale
):
    end_gate = jax.nn.sigmoid(proj_gate[ROWS - EDGE :].astype(WIDE))
    end = (proj_value[ROWS - EDGE :].astype(WIDE) * end_gate).astype(NARROW)
    halo = shifted(end, SP, 1)
    split = (HALVES, ROWS, LANES)
    rest = (HALVES, ROWS - EDGE, LANES)
    row_gain = norm_gain.reshape(1, WIDTH)
    sides = pltpu.VMEM((HALVES, EDGE + ROWS, LANES), WIDE)
    taps_scratch = pltpu.VMEM((TAPS + 1, WIDTH), WIDE)
    place = lax.axis_index(SP).reshape(1)
    narrow = ((ROWS, WIDTH), NARROW)
    gated, scaled, spread, sums, gain_part, first_upstream, cotangent, across, product = (
        scalar_call(
            forward,
            [
                narrow, (rest, WIDE), (rest, WIDE), ((8, LANES), WIDE),
                ((HALVES, 8, LANES), WIDE), ((EDGE, WIDTH), WIDE), ((ROWS, MODEL), NARROW),
                ((WIDTH, ROWS), NARROW), ((CLOSE, WIDTH, BLOCK), WIDE),
            ],
            place, proj_value, proj_gate, out_cotangent, out_weight,
            conv_taps, row_gain, row_mean, row_scale, in_hbm=8,
            scratch=[
                pltpu.VMEM(*narrow), pltpu.VMEM(*narrow),
                pltpu.VMEM((WIDTH, MODEL), NARROW), pltpu.VMEM((TAPS, WIDTH), NARROW),
                pltpu.VMEM((1, WIDTH), WIDE), pltpu.VMEM((ROWS,), WIDE),
                pltpu.VMEM((ROWS,), WIDE), pltpu.SemaphoreType.DMA((8,)),
                sides, taps_scratch, *([pltpu.VMEM((ROWS, LANES), WIDE)] * 4),
                pltpu.VMEM((ROWS, WIDTH), WIDE), pltpu.VMEM(split, WIDE),
                pltpu.VMEM((ROWS, WIDTH), WIDE),
            ],
            flops=4 * ROWS * WIDTH * MODEL, limit=12,
        )
    )
    edge = (HALVES, EDGE, LANES)
    first_scaled, first_spread, first_hidden, message, gain_part = call_with(
        head,
        [
            (edge, WIDE), (edge, WIDE), ((EDGE, WIDTH), NARROW),
            ((TP, 8, LANES), WIDE), ((HALVES, 8, LANES), WIDE),
        ],
        [
            pltpu.VMEM((HALVES, 2 * EDGE, LANES), WIDE),
            taps_scratch,
            pltpu.VMEM((2, LANES, LANES), WIDE),
        ],
        halo, gated, first_upstream, conv_taps, row_gain, row_mean, row_scale, sums,
        gain_part, flops=10 * ROWS * WIDTH,
    )
    sums = exchange(message, "tp", SUMS_ORDER)
    rows = CLOSE * WIDTH + 4 * SMALL
    other, small, extended = scalar_call(
        backward,
        [
            ((rows, BLOCK), NARROW), ((SMALL, WIDTH), WIDE),
            ((HALVES, ROWS + 2 * EDGE, LANES), WIDE),
        ],
        place, sums, scaled, spread, first_scaled, first_spread, halo, gated, row_scale, gain_part,
        cotangent, first_hidden, product, scratch=[sides], flops=100 * ROWS * WIDTH,
    )
    other = lax.ppermute(other, "c", [(0, 1), (1, 0)])
    main = ((ROWS - EDGE, WIDTH), NARROW)
    value_part, gate_part, margin, last, mine = scalar_call(
        gated_gradient,
        [main, main, (edge, WIDE), ((3, *edge), WIDE), ((CLOSE, WIDTH, BLOCK), WIDE)],
        place, extended, conv_taps, proj_value, proj_gate, cotangent, first_hidden,
        across, scratch=[taps_scratch], flops=100 * ROWS * WIDTH,
    )
    (pieces,) = call(
        pack, [((CLOSE, WIDTH + 2 * SMALL, BLOCK), NARROW)], mine, small, other, flops=1 << 20
    )
    arrived = exchange(pieces, NEAR, NEAR_ORDER)
    (payload,) = call(
        fold_near, [((WIDTH + 2 * SMALL, BLOCK), NARROW)], arrived, flops=1 << 20
    )
    payload = to_block(payload)
    late = shifted(margin, SP, -1)
    (message,) = call(hand_out, [((2 * CLOSE, OWN + SMALL, WIDTH), NARROW)], payload, flops=1 << 16)
    arrived = exchange(message, (*NEAR, "c"), GATHER_ORDER)
    (total,) = call(totals, [((OWN + SMALL, WIDTH), WIDE)], arrived, flops=1 << 20)
    value_grad, gate_grad, weight_grad, taps_grad, gain_grad = last_call(
        [narrow, narrow, ((OWN, WIDTH), WIDE), ((TAPS, WIDTH), WIDE), ((1, WIDTH), WIDE)],
        total, value_part, gate_part, last, late,
    )
    return (value_grad, gate_grad, weight_grad, taps_grad, gain_grad.reshape(WIDTH))


def call_with(body, outs, scratch, *args, flops=0, limit=6):
    shapes = [jax.ShapeDtypeStruct(shape, dtype) for shape, dtype in outs]
    size = sum(a.size * a.dtype.itemsize for a in (*args, *shapes))
    return pl.pallas_call(
        body,
        out_shape=shapes,
        scratch_shapes=scratch,
        compiler_params=pltpu.CompilerParams(vmem_limit_bytes=limit << 20),
        cost_estimate=pl.CostEstimate(flops=flops, bytes_accessed=size, transcendentals=0),
    )(*args)


def scalar_call(
    body, outs, scalar, *args, scratch=(), flops=1 << 20, limit=6, in_hbm=0
):
    shapes = [jax.ShapeDtypeStruct(shape, dtype) for shape, dtype in outs]
    size = sum(a.size * a.dtype.itemsize for a in (*args, *shapes))
    whole = pl.BlockSpec(memory_space=pltpu.VMEM)
    far = [pltpu.with_memory_space_constraint(a, pltpu.HBM) for a in args[:in_hbm]]
    return pl.pallas_call(
        body,
        out_shape=shapes,
        in_specs=[
            pl.BlockSpec(memory_space=pltpu.SMEM),
            *([pl.BlockSpec(memory_space=pltpu.HBM)] * in_hbm),
            *([whole] * (len(args) - in_hbm)),
        ],
        out_specs=[whole] * len(shapes),
        scratch_shapes=scratch,
        compiler_params=pltpu.CompilerParams(vmem_limit_bytes=limit << 20),
        cost_estimate=pl.CostEstimate(flops=flops, bytes_accessed=size, transcendentals=0),
    )(scalar, *far, *args[in_hbm:])


def last_call(outs, *args):
    edge = pltpu.VMEM((EDGE, WIDTH), NARROW)
    return pl.pallas_call(
        finish,
        out_shape=[pltpu.HBM(*out) for out in outs],
        in_specs=[pl.BlockSpec(memory_space=pltpu.VMEM)] * len(args),
        out_specs=[pl.BlockSpec(memory_space=pltpu.HBM)] * len(outs),
        scratch_shapes=[
            edge, edge, pltpu.VMEM(*outs[3]), pltpu.VMEM(*outs[4]), pltpu.SemaphoreType.DMA((7,)),
        ],
        compiler_params=pltpu.CompilerParams(vmem_limit_bytes=6 << 20),
        cost_estimate=pl.CostEstimate(flops=1 << 16, bytes_accessed=1 << 19, transcendentals=0),
        name="finish",
    )(*args)


def solution(mesh):
    sizes = [size for _, size in AXES]
    split = Mesh(mesh.devices.reshape(*sizes, mesh.shape["tp"]), (*SP, "tp"))
    placed = (
        P(SP, "tp"),
        P(SP, "tp"),
        P(SP, None),
        P("tp", None),
        P(None, "tp"),
        P("tp"),
        P(SP),
        P(SP),
    )
    return jax.shard_map(
        shards,
        mesh=split,
        in_specs=placed,
        out_specs=(P(SP, "tp"), P(SP, "tp"), P(SP, "tp"), P(None, "tp"), P("tp")),
        check_vma=False,
    )
```

```python
import jax
import jax.numpy as jnp
from jax import lax
from jax.experimental import pallas as pl
from jax.experimental.pallas import tpu as pltpu
from jax.sharding import Mesh
from jax.sharding import PartitionSpec as P


SP = ("zh", "zl", "x", "c")
NEAR = ("zl", "x")
FAR = 16
CLOSE = 8
AXES = (("zh", FAR), ("zl", 2), ("x", 4), ("c", 2))
TP = 4
SUMS_ORDER = [2, 3, 0, 1]
OFFSETS = ((0, -1, -2, -3, 3, 2, 1, -4), (6, 7, 8, 5, -7, -6, -5, 4))
BLOCK = CLOSE * 2 * 8
NEAR_ORDER = [(place + 4) % CLOSE for place in range(CLOSE)]
GATHER_ORDER = [(place + 7) % (2 * CLOSE) for place in range(2 * CLOSE)]
TAPS = 31
SMALL = TAPS + 1
ROWS = 384
EDGE = 32
LANES = 128
HALVES = 2
WIDTH = HALVES * LANES
MODEL = 2048
OWN = 8
CHUNK = 64
WIDE = jnp.float32
NARROW = jnp.bfloat16


def shifted(value, axis, steps):
    count = lax.axis_size(axis)
    first, last = (max(0, -steps), min(count, count - steps))
    return lax.ppermute(value, axis, [(source, source + steps) for source in range(first, last)])


def exchange(pieces, axes, order=None):
    groups = order and [order]
    return lax.all_to_all(pieces, axes, 0, 0, tiled=True, axis_index_groups=groups)


def lanes(half):
    return slice(half * LANES, (half + 1) * LANES)


def column(row):
    return jnp.transpose(jnp.broadcast_to(row, (LANES, LANES)))


def call(body, outs, *args, flops=0, limit=6):
    shapes = [jax.ShapeDtypeStruct(shape, dtype) for shape, dtype in outs]
    size = sum(a.size * a.dtype.itemsize for a in (*args, *shapes))
    return pl.pallas_call(
        body,
        out_shape=shapes,
        compiler_params=pltpu.CompilerParams(vmem_limit_bytes=limit << 20),
        cost_estimate=pl.CostEstimate(flops=flops, bytes_accessed=size, transcendentals=0),
    )(*args)


def norm_backward(normed, factor, gain_row, upstream):
    active = normed * gain_row
    sig = jax.nn.sigmoid(active)
    hidden = (active * sig).astype(NARROW)
    d_active = upstream * sig * (1.0 + active * (1.0 - sig))
    d_normed = d_active * gain_row
    gain_part = jnp.sum((d_active * normed).reshape(normed.shape[0] // 8, 8, LANES), 0)
    return hidden, factor * d_normed, factor * normed, d_normed, d_normed * normed, gain_part


def convolve(source, half, taps_wide, start, size):
    conv = jnp.zeros((size, LANES), WIDE)
    for tap in range(TAPS):
        begin = start + tap + EDGE - TAPS + 1
        conv = conv + taps_wide[tap : tap + 1, lanes(half)] * source[half, begin : begin + size]
    return conv


def column_sums(source):
    return jnp.sum(jnp.transpose(source), 0, keepdims=True)


def block_columns(place, near, side):
    far, core = place[0] // (2 * CLOSE), place[0] % 2
    low, high = OFFSETS[0][near], OFFSETS[1][near]
    step = jnp.where(core == side, low, high)
    block = lax.rem(far + step + FAR, FAR)
    return pl.ds(pl.multiple_of(block * BLOCK, BLOCK), BLOCK)


def main_product(turned, cotangent, place, side, product):
    for near in range(0, CLOSE, 2):
        pair = [cotangent[:, block_columns(place, near + i, side)] for i in range(2)]
        both = jnp.dot(turned, jnp.concatenate(pair, 1), preferred_element_type=WIDE)
        for i in range(2):
            product[near + i] = both[:, i * BLOCK : (i + 1) * BLOCK]


def load(
    value, gate, taps, gain, mean, scale,
    end, held_value, held_gate, held_taps, held_gain, held_mean, held_scale,
    arrivals,
):
    copies = [
        pltpu.make_async_copy(source, target, arrivals.at[i])
        for i, (source, target) in enumerate(
            (
                (value, held_value), (gate, held_gate), (taps, held_taps), (gain, held_gain),
                (mean, held_mean), (scale, held_scale),
            )
        )
    ]
    for copy in copies:
        copy.start()
    for copy in copies:
        copy.wait()
    rows = slice(ROWS - EDGE, ROWS)
    sig = jax.nn.sigmoid(held_gate[rows].astype(WIDE))
    end[...] = (held_value[rows].astype(WIDE) * sig).astype(NARROW)


def forward(
    place, cotangent, weight, held_value, held_gate, taps, gain, mean, scale,
    gated, scaled, spread, sums, gain_part, first_upstream, held, across, product,
    held_weight, arrivals,
    padded, taps_wide, mean_columns, scale_columns, sum_first, sum_second,
    hidden, normed, upstream,
):
    copies = [
        pltpu.make_async_copy(source, target, arrivals.at[i])
        for i, (source, target) in enumerate(
            ((weight, held_weight), (cotangent, held))
        )
    ]
    for copy in copies:
        copy.start()
    sum_first[0:EDGE] = jnp.zeros((EDGE, LANES), WIDE)
    sum_second[0:EDGE] = jnp.zeros((EDGE, LANES), WIDE)
    hidden[0:EDGE] = jnp.zeros((EDGE, WIDTH), WIDE)
    taps_wide[0:TAPS] = taps[...].astype(WIDE)
    for block in range(ROWS // LANES):
        rows = slice(block * LANES, (block + 1) * LANES)
        mean_columns[rows] = column(mean[rows].reshape(1, LANES))
        scale_columns[rows] = column(scale[rows].reshape(1, LANES))
    for half in range(HALVES):
        for start in range(0, ROWS, CHUNK):
            rows = slice(start, start + CHUNK)
            sig = jax.nn.sigmoid(held_gate[rows, lanes(half)].astype(WIDE))
            narrow = (held_value[rows, lanes(half)].astype(WIDE) * sig).astype(NARROW)
            gated[rows, lanes(half)] = narrow
            padded[half, EDGE + start : EDGE + start + CHUNK] = narrow.astype(WIDE)
        for start in range(EDGE, ROWS, EDGE):
            rows = slice(start, start + EDGE)
            conv = convolve(padded, half, taps_wide, start, EDGE)
            normed[half, rows] = (conv - mean_columns[rows]) * scale_columns[rows]
    for copy in copies:
        copy.wait()
    upstream[...] = lax.dot_general(
        held[...], held_weight[...], (((1,), (1,)), ((), ())), preferred_element_type=WIDE
    )
    first_upstream[...] = upstream[0:EDGE]
    for half in range(HALVES):
        gain_row = gain[0:1, lanes(half)]
        gain_sum = jnp.zeros((8, LANES), WIDE)
        for start in range(EDGE, ROWS, EDGE):
            rows = slice(start, start + EDGE)
            narrow, own_scaled, own_spread, first, second, part = norm_backward(
                normed[half, rows], scale_columns[rows], gain_row, upstream[rows, lanes(half)]
            )
            hidden[rows, lanes(half)] = narrow.astype(WIDE)
            scaled[half, start - EDGE : start] = own_scaled
            spread[half, start - EDGE : start] = own_spread
            gain_sum = gain_sum + part
            if half == 0:
                sum_first[rows] = first
                sum_second[rows] = second
            else:
                sum_first[rows] = sum_first[rows] + first
                sum_second[rows] = sum_second[rows] + second
        gain_part[half] = gain_sum
    found = [
        column_sums(source[block * LANES : (block + 1) * LANES])
        for source in (sum_first, sum_second)
        for block in range(ROWS // LANES)
    ]
    sums[...] = jnp.concatenate([*found, jnp.zeros((2, LANES), WIDE)], 0)
    across[...] = jnp.transpose(hidden[...]).astype(NARROW)
    main_product(across[...], held, place, 1, product)


def head(
    halo, gated, upstream, taps, gain, mean, scale, sums, gain_part,
    scaled, spread, hidden, message, gain_total,
    padded, taps_wide, turned,
):
    taps_wide[0:TAPS] = taps[...].astype(WIDE)
    rows = slice(0, EDGE)
    mean_columns = column(mean[0:LANES].reshape(1, LANES))[rows]
    scale_columns = column(scale[0:LANES].reshape(1, LANES))[rows]
    turned[...] = jnp.zeros((2, LANES, LANES), WIDE)
    for half in range(HALVES):
        padded[half, rows] = halo[:, lanes(half)].astype(WIDE)
        padded[half, EDGE:] = gated[rows, lanes(half)].astype(WIDE)
    for half in range(HALVES):
        conv = convolve(padded, half, taps_wide, 0, EDGE)
        normed = (conv - mean_columns) * scale_columns
        narrow, own_scaled, own_spread, first, second, part = norm_backward(
            normed, scale_columns, gain[0:1, lanes(half)], upstream[rows, lanes(half)]
        )
        hidden[:, lanes(half)] = narrow
        scaled[half] = own_scaled
        spread[half] = own_spread
        gain_total[half] = gain_part[half] + part
        turned[0, rows] = turned[0, rows] + first
        turned[1, rows] = turned[1, rows] + second
    blocks = ROWS // LANES
    total = sums[...]
    extra = [column_sums(turned[0]), column_sums(turned[1])]
    none = jnp.zeros((blocks - 1, LANES), WIDE)
    last = jnp.zeros((2, LANES), WIDE)
    total = total + jnp.concatenate([extra[0], none, extra[1], none, last], 0)
    for peer in range(TP):
        message[peer] = total


def head_product(cotangent, hidden, place, near, side):
    columns = cotangent[0:EDGE, block_columns(place, near, side)]
    return lax.dot_general(
        hidden[...], columns, (((0,), (0,)), ((), ())), preferred_element_type=WIDE
    )


def backward(
    place, sums, scaled, spread, first_scaled, first_spread, halo, gated, scale, gain_part,
    cotangent, first_hidden, product,
    other, small, extended,
    padded,
):
    for half in range(HALVES):
        padded[half, 0:EDGE] = halo[:, lanes(half)].astype(WIDE)
        padded[half, EDGE:] = gated[:, lanes(half)].astype(WIDE)
    total = (sums[0] + sums[1]) + (sums[2] + sums[3])
    total = total * (1.0 / (TP * WIDTH))
    blocks = ROWS // LANES
    for half in range(HALVES):
        extended[half, 0:EDGE] = jnp.zeros((EDGE, LANES), WIDE)
        extended[half, EDGE + ROWS :] = jnp.zeros((EDGE, LANES), WIDE)
    for block in range(blocks):
        rows = slice(block * LANES, (block + 1) * LANES)
        first = column(total[block : block + 1] * scale[rows].reshape(1, LANES))
        second = column(total[blocks + block : blocks + block + 1])
        for half in range(HALVES):
            cut = 0
            if block == 0:
                cut = EDGE
                d_conv = first_scaled[half] - first[0:cut] - first_spread[half] * second[0:cut]
                extended[half, EDGE : EDGE + cut] = d_conv
            rows = slice(block * LANES + cut - EDGE, (block + 1) * LANES - EDGE)
            d_conv = scaled[half, rows] - first[cut:] - spread[half, rows] * second[cut:]
            extended[half, EDGE + block * LANES + cut : EDGE + (block + 1) * LANES] = d_conv
    lead = EDGE - TAPS + 1
    groups = ROWS // 8
    for offset in range(8):
        steps = [q for q in range(5) if 0 <= 8 * q + offset - lead < TAPS]
        found = {(half, q): jnp.zeros((8, LANES), WIDE) for half in range(HALVES) for q in steps}
        loaded = {}
        for m in range(groups + steps[-1]):
            for half in range(HALVES):
                if m < groups:
                    begin = EDGE + 8 * m
                    loaded[half, m] = extended[half, begin : begin + 8]
                moved = padded[half, 8 * m + offset : 8 * m + offset + 8]
                for q in steps:
                    if 0 <= m - q < groups:
                        found[half, q] = found[half, q] + loaded[half, m - q] * moved
        for half in range(HALVES):
            for q in steps:
                tap = 8 * q + offset - lead
                small[tap : tap + 1, lanes(half)] = jnp.sum(found[half, q], 0, keepdims=True)
        near = offset
        whole = product[near] + head_product(cotangent, first_hidden, place, near, 1)
        other[near * WIDTH : (near + 1) * WIDTH] = whole.astype(NARROW)
    for half in range(HALVES):
        small[TAPS:SMALL, lanes(half)] = jnp.sum(gain_part[half], 0, keepdims=True)
    for half in range(HALVES):
        value = small[:, lanes(half)]
        top = value.astype(NARROW)
        begin = CLOSE * WIDTH + half * 2 * SMALL
        other[begin : begin + SMALL] = top
        other[begin + SMALL : begin + 2 * SMALL] = (value - top.astype(WIDE)).astype(NARROW)


def pack(mine, small, other, pieces):
    for half in range(HALVES):
        begin = CLOSE * WIDTH + half * 2 * SMALL
        top = other[begin : begin + SMALL].astype(WIDE)
        rest = other[begin + SMALL : begin + 2 * SMALL].astype(WIDE)
        both = (small[:, lanes(half)] + (top + rest)).astype(NARROW)
        for near in range(CLOSE):
            pieces[near, WIDTH + half * SMALL : WIDTH + (half + 1) * SMALL] = both
    for near in range(CLOSE):
        for start in range(0, WIDTH, 64):
            rows = slice(start, start + 64)
            there = other[near * WIDTH + start : near * WIDTH + start + 64].astype(WIDE)
            pieces[NEAR_ORDER.index(near), rows] = (mine[near, rows] + there).astype(NARROW)


def gated_gradient(
    place, extended, taps, value, gate, cotangent, first_hidden, across,
    value_grad, gate_grad, margin, last, mine,
    taps_wide,
):
    main_product(across[...], cotangent, place, 0, mine)
    for near in range(CLOSE):
        mine[near] = mine[near] + head_product(cotangent, first_hidden, place, near, 0)
    taps_wide[0:TAPS] = taps[...].astype(WIDE)
    for half in range(HALVES):
        for start in range(0, EDGE + ROWS, EDGE):
            found = jnp.zeros((EDGE, LANES), WIDE)
            for tap in range(TAPS):
                begin = start + TAPS - 1 - tap
                found = found + taps_wide[tap : tap + 1, lanes(half)] * extended[half, begin : begin + EDGE]
            if start == 0:
                margin[half] = found
                continue
            rows = slice(start - EDGE, start)
            sig = jax.nn.sigmoid(gate[rows, lanes(half)].astype(WIDE))
            slope = value[rows, lanes(half)].astype(WIDE) * sig * (1.0 - sig)
            if start == ROWS:
                last[0, half], last[1, half], last[2, half] = found, sig, slope
            else:
                value_grad[rows, lanes(half)] = (found * sig).astype(NARROW)
                gate_grad[rows, lanes(half)] = (found * slope).astype(NARROW)


def fold_near(arrived, payload):
    for start in range(0, WIDTH + 2 * SMALL, 64):
        rows = slice(start, start + 64)
        total = arrived[0, rows].astype(WIDE)
        for near in range(1, CLOSE):
            total = total + arrived[near, rows].astype(WIDE)
        payload[rows] = total.astype(NARROW)


def hand_out(payload, message):
    weights = jnp.transpose(payload[0:WIDTH].astype(WIDE)).astype(NARROW)
    small = jnp.concatenate([payload[WIDTH : WIDTH + SMALL], payload[WIDTH + SMALL :]], 1)
    for position, member in enumerate(GATHER_ORDER):
        message[position, 0:OWN] = weights[member * OWN : (member + 1) * OWN]
        message[position, OWN:] = small


def totals(arrived, total):
    for start in range(0, OWN + SMALL, 8):
        rows = slice(start, start + 8)
        found = arrived[0, rows].astype(WIDE)
        for position in range(1, 2 * CLOSE):
            found = found + arrived[position, rows].astype(WIDE)
        total[rows] = found


def finish(
    total, value_part, gate_part, last, late,
    value_grad, gate_grad, weight_grad, taps_grad, gain_grad,
    value_end, gate_end, taps_held, gain_held, departures,
):
    main, end = pl.ds(0, ROWS - EDGE), pl.ds(ROWS - EDGE, EDGE)
    taps_held[...] = total[OWN : OWN + TAPS]
    gain_held[...] = total[OWN + TAPS :]
    for half in range(HALVES):
        grad = last[0, half] + late[half]
        value_end[:, lanes(half)] = (grad * last[1, half]).astype(NARROW)
        gate_end[:, lanes(half)] = (grad * last[2, half]).astype(NARROW)
    copies = [
        pltpu.make_async_copy(value_part, value_grad.at[main], departures.at[0]),
        pltpu.make_async_copy(gate_part, gate_grad.at[main], departures.at[1]),
        pltpu.make_async_copy(total.at[pl.ds(0, OWN)], weight_grad, departures.at[2]),
        pltpu.make_async_copy(taps_held, taps_grad, departures.at[3]),
        pltpu.make_async_copy(gain_held, gain_grad, departures.at[4]),
        pltpu.make_async_copy(value_end, value_grad.at[end], departures.at[5]),
        pltpu.make_async_copy(gate_end, gate_grad.at[end], departures.at[6]),
    ]
    for copy in copies:
        copy.start()
    for copy in copies:
        copy.wait()


def to_block(value):
    pairs = []
    for far in range(FAR):
        for near in range(CLOSE):
            for core in range(2):
                target = (far + OFFSETS[core][near]) % FAR
                pairs.append(((far * CLOSE + near) * 2 + core, (target * CLOSE + near) * 2 + core))
    return lax.ppermute(value, SP, pairs)


def shards(
    proj_value, proj_gate, out_cotangent, out_weight, conv_taps, norm_gain, row_mean, row_scale
):
    row_gain = norm_gain.reshape(1, WIDTH)
    end, proj_value, proj_gate, conv_taps, row_gain, row_mean, row_scale = load_call(
        proj_value, proj_gate, conv_taps, row_gain, row_mean, row_scale
    )
    halo = shifted(end, SP, 1)
    split = (HALVES, ROWS, LANES)
    rest = (HALVES, ROWS - EDGE, LANES)
    sides = pltpu.VMEM((HALVES, EDGE + ROWS, LANES), WIDE)
    taps_scratch = pltpu.VMEM((TAPS + 1, WIDTH), WIDE)
    place = lax.axis_index(SP).reshape(1)
    narrow = ((ROWS, WIDTH), NARROW)
    gated, scaled, spread, sums, gain_part, first_upstream, cotangent, across, product = (
        scalar_call(
            forward,
            [
                narrow, (rest, WIDE), (rest, WIDE), ((8, LANES), WIDE),
                ((HALVES, 8, LANES), WIDE), ((EDGE, WIDTH), WIDE), ((ROWS, MODEL), NARROW),
                ((WIDTH, ROWS), NARROW), ((CLOSE, WIDTH, BLOCK), WIDE),
            ],
            place, out_cotangent, out_weight, proj_value, proj_gate,
            conv_taps, row_gain, row_mean, row_scale, in_hbm=2,
            scratch=[
                pltpu.VMEM((WIDTH, MODEL), NARROW), pltpu.SemaphoreType.DMA((2,)),
                sides, taps_scratch, *([pltpu.VMEM((ROWS, LANES), WIDE)] * 4),
                pltpu.VMEM((ROWS, WIDTH), WIDE), pltpu.VMEM(split, WIDE),
                pltpu.VMEM((ROWS, WIDTH), WIDE),
            ],
            flops=4 * ROWS * WIDTH * MODEL, limit=12,
        )
    )
    edge = (HALVES, EDGE, LANES)
    first_scaled, first_spread, first_hidden, message, gain_part = call_with(
        head,
        [
            (edge, WIDE), (edge, WIDE), ((EDGE, WIDTH), NARROW),
            ((TP, 8, LANES), WIDE), ((HALVES, 8, LANES), WIDE),
        ],
        [
            pltpu.VMEM((HALVES, 2 * EDGE, LANES), WIDE),
            taps_scratch,
            pltpu.VMEM((2, LANES, LANES), WIDE),
        ],
        halo, gated, first_upstream, conv_taps, row_gain, row_mean, row_scale, sums,
        gain_part, flops=10 * ROWS * WIDTH,
    )
    sums = exchange(message, "tp", SUMS_ORDER)
    rows = CLOSE * WIDTH + 4 * SMALL
    other, small, extended = scalar_call(
        backward,
        [
            ((rows, BLOCK), NARROW), ((SMALL, WIDTH), WIDE),
            ((HALVES, ROWS + 2 * EDGE, LANES), WIDE),
        ],
        place, sums, scaled, spread, first_scaled, first_spread, halo, gated, row_scale, gain_part,
        cotangent, first_hidden, product, scratch=[sides], flops=100 * ROWS * WIDTH,
    )
    other = lax.ppermute(other, "c", [(0, 1), (1, 0)])
    main = ((ROWS - EDGE, WIDTH), NARROW)
    value_part, gate_part, margin, last, mine = scalar_call(
        gated_gradient,
        [main, main, (edge, WIDE), ((3, *edge), WIDE), ((CLOSE, WIDTH, BLOCK), WIDE)],
        place, extended, conv_taps, proj_value, proj_gate, cotangent, first_hidden,
        across, scratch=[taps_scratch], flops=100 * ROWS * WIDTH,
    )
    (pieces,) = call(
        pack, [((CLOSE, WIDTH + 2 * SMALL, BLOCK), NARROW)], mine, small, other, flops=1 << 20
    )
    arrived = exchange(pieces, NEAR, NEAR_ORDER)
    (payload,) = call(
        fold_near, [((WIDTH + 2 * SMALL, BLOCK), NARROW)], arrived, flops=1 << 20
    )
    payload = to_block(payload)
    late = shifted(margin, SP, -1)
    (message,) = call(hand_out, [((2 * CLOSE, OWN + SMALL, WIDTH), NARROW)], payload, flops=1 << 16)
    arrived = exchange(message, (*NEAR, "c"), GATHER_ORDER)
    (total,) = call(totals, [((OWN + SMALL, WIDTH), WIDE)], arrived, flops=1 << 20)
    value_grad, gate_grad, weight_grad, taps_grad, gain_grad = last_call(
        [narrow, narrow, ((OWN, WIDTH), WIDE), ((TAPS, WIDTH), WIDE), ((1, WIDTH), WIDE)],
        total, value_part, gate_part, last, late,
    )
    return (value_grad, gate_grad, weight_grad, taps_grad, gain_grad.reshape(WIDTH))


def call_with(body, outs, scratch, *args, flops=0, limit=6):
    shapes = [jax.ShapeDtypeStruct(shape, dtype) for shape, dtype in outs]
    size = sum(a.size * a.dtype.itemsize for a in (*args, *shapes))
    return pl.pallas_call(
        body,
        out_shape=shapes,
        scratch_shapes=scratch,
        compiler_params=pltpu.CompilerParams(vmem_limit_bytes=limit << 20),
        cost_estimate=pl.CostEstimate(flops=flops, bytes_accessed=size, transcendentals=0),
    )(*args)


def scalar_call(
    body, outs, scalar, *args, scratch=(), flops=1 << 20, limit=6, in_hbm=0
):
    shapes = [jax.ShapeDtypeStruct(shape, dtype) for shape, dtype in outs]
    size = sum(a.size * a.dtype.itemsize for a in (*args, *shapes))
    whole = pl.BlockSpec(memory_space=pltpu.VMEM)
    far = [pltpu.with_memory_space_constraint(a, pltpu.HBM) for a in args[:in_hbm]]
    return pl.pallas_call(
        body,
        out_shape=shapes,
        in_specs=[
            pl.BlockSpec(memory_space=pltpu.SMEM),
            *([pl.BlockSpec(memory_space=pltpu.HBM)] * in_hbm),
            *([whole] * (len(args) - in_hbm)),
        ],
        out_specs=[whole] * len(shapes),
        scratch_shapes=scratch,
        compiler_params=pltpu.CompilerParams(vmem_limit_bytes=limit << 20),
        cost_estimate=pl.CostEstimate(flops=flops, bytes_accessed=size, transcendentals=0),
    )(scalar, *far, *args[in_hbm:])


def load_call(*args):
    held = [pltpu.with_memory_space_constraint(a, pltpu.HBM) for a in args]
    shapes = [jax.ShapeDtypeStruct((EDGE, WIDTH), NARROW)]
    shapes += [jax.ShapeDtypeStruct(a.shape, a.dtype) for a in args]
    return pl.pallas_call(
        load,
        out_shape=shapes,
        in_specs=[pl.BlockSpec(memory_space=pltpu.HBM)] * len(args),
        out_specs=[pl.BlockSpec(memory_space=pltpu.VMEM)] * len(shapes),
        scratch_shapes=[pltpu.SemaphoreType.DMA((len(args),))],
        compiler_params=pltpu.CompilerParams(vmem_limit_bytes=6 << 20),
        cost_estimate=pl.CostEstimate(flops=1 << 16, bytes_accessed=1 << 19, transcendentals=0),
        name="load",
    )(*held)


def last_call(outs, *args):
    edge = pltpu.VMEM((EDGE, WIDTH), NARROW)
    return pl.pallas_call(
        finish,
        out_shape=[pltpu.HBM(*out) for out in outs],
        in_specs=[pl.BlockSpec(memory_space=pltpu.VMEM)] * len(args),
        out_specs=[pl.BlockSpec(memory_space=pltpu.HBM)] * len(outs),
        scratch_shapes=[
            edge, edge, pltpu.VMEM(*outs[3]), pltpu.VMEM(*outs[4]), pltpu.SemaphoreType.DMA((7,)),
        ],
        compiler_params=pltpu.CompilerParams(vmem_limit_bytes=6 << 20),
        cost_estimate=pl.CostEstimate(flops=1 << 16, bytes_accessed=1 << 19, transcendentals=0),
        name="finish",
    )(*args)


def solution(mesh):
    sizes = [size for _, size in AXES]
    split = Mesh(mesh.devices.reshape(*sizes, mesh.shape["tp"]), (*SP, "tp"))
    placed = (
        P(SP, "tp"),
        P(SP, "tp"),
        P(SP, None),
        P("tp", None),
        P(None, "tp"),
        P("tp"),
        P(SP),
        P(SP),
    )
    return jax.shard_map(
        shards,
        mesh=split,
        in_specs=placed,
        out_specs=(P(SP, "tp"), P(SP, "tp"), P(SP, "tp"), P(None, "tp"), P("tp")),
        check_vma=False,
    )
```

```python
import jax
import jax.numpy as jnp
from jax import lax
from jax.experimental import pallas as pl
from jax.experimental.pallas import tpu as pltpu
from jax.sharding import Mesh
from jax.sharding import PartitionSpec as P


SP = ("zh", "zl", "x", "c")
NEAR = ("zl", "x")
FAR = 16
CLOSE = 8
AXES = (("zh", FAR), ("zl", 2), ("x", 4), ("c", 2))
TP = 4
SUMS_ORDER = [2, 3, 0, 1]
OFFSETS = ((0, -1, -2, -3, 3, 2, 1, -4), (6, 7, 8, 5, -7, -6, -5, 4))
BLOCK = CLOSE * 2 * 8
NEAR_ORDER = [(place + 4) % CLOSE for place in range(CLOSE)]
GATHER_ORDER = [(place + 5) % (2 * CLOSE) for place in range(2 * CLOSE)]
TAPS = 31
SMALL = TAPS + 1
ROWS = 384
EDGE = 32
LANES = 128
HALVES = 2
WIDTH = HALVES * LANES
MODEL = 2048
OWN = 8
CHUNK = 64
WIDE = jnp.float32
NARROW = jnp.bfloat16


def shifted(value, axis, steps):
    count = lax.axis_size(axis)
    first, last = (max(0, -steps), min(count, count - steps))
    return lax.ppermute(value, axis, [(source, source + steps) for source in range(first, last)])


def exchange(pieces, axes, order=None):
    groups = order and [order]
    return lax.all_to_all(pieces, axes, 0, 0, tiled=True, axis_index_groups=groups)


def lanes(half):
    return slice(half * LANES, (half + 1) * LANES)


def column(row):
    return jnp.transpose(jnp.broadcast_to(row, (LANES, LANES)))


def call(body, outs, *args, flops=0, limit=6):
    shapes = [jax.ShapeDtypeStruct(shape, dtype) for shape, dtype in outs]
    size = sum(a.size * a.dtype.itemsize for a in (*args, *shapes))
    return pl.pallas_call(
        body,
        out_shape=shapes,
        compiler_params=pltpu.CompilerParams(vmem_limit_bytes=limit << 20),
        cost_estimate=pl.CostEstimate(flops=flops, bytes_accessed=size, transcendentals=0),
    )(*args)


def norm_backward(normed, factor, gain_row, upstream):
    active = normed * gain_row
    sig = jax.nn.sigmoid(active)
    hidden = (active * sig).astype(NARROW)
    d_active = upstream * sig * (1.0 + active * (1.0 - sig))
    d_normed = d_active * gain_row
    gain_part = jnp.sum((d_active * normed).reshape(normed.shape[0] // 8, 8, LANES), 0)
    return hidden, factor * d_normed, factor * normed, d_normed, d_normed * normed, gain_part


def convolve(source, half, taps_wide, start, size):
    conv = jnp.zeros((size, LANES), WIDE)
    for tap in range(TAPS):
        begin = start + tap + EDGE - TAPS + 1
        conv = conv + taps_wide[tap : tap + 1, lanes(half)] * source[half, begin : begin + size]
    return conv


def column_sums(source):
    return jnp.sum(jnp.transpose(source), 0, keepdims=True)


def both_blocks(cotangent, place, near):
    far, core = place[0] // (2 * CLOSE), place[0] % 2
    low, high = OFFSETS[0][near], OFFSETS[1][near]
    own = lax.rem(far + jnp.where(core == 0, low, high) + FAR, FAR)
    theirs = lax.rem(far + jnp.where(core == 0, high, low) + FAR, FAR)
    columns = [pl.ds(pl.multiple_of(block * BLOCK, BLOCK), BLOCK) for block in (own, theirs)]
    return jnp.concatenate([cotangent[:, columns[0]], cotangent[:, columns[1]]], 1)


def forward(
    place, value, gate, cotangent, weight, far_taps, far_gain, far_mean, far_scale,
    gated, scaled, spread, sums, gain_part, first_upstream, first_cotangent, product,
    held_value, held_gate, held, held_weight, taps, gain, mean, scale, arrivals,
    padded, taps_wide, mean_columns, scale_columns, sum_first, sum_second,
    hidden, normed, upstream,
):
    copies = [
        pltpu.make_async_copy(source, target, arrivals.at[i])
        for i, (source, target) in enumerate(
            (
                (value, held_value), (gate, held_gate), (far_taps, taps), (far_mean, mean),
                (far_scale, scale), (far_gain, gain), (weight, held_weight), (cotangent, held),
            )
        )
    ]
    for copy in copies:
        copy.start()
    sum_first[0:EDGE] = jnp.zeros((EDGE, LANES), WIDE)
    sum_second[0:EDGE] = jnp.zeros((EDGE, LANES), WIDE)
    hidden[0:EDGE] = jnp.zeros((EDGE, WIDTH), WIDE)
    for copy in copies[:6]:
        copy.wait()
    taps_wide[0:TAPS] = taps[...].astype(WIDE)
    for block in range(ROWS // LANES):
        rows = slice(block * LANES, (block + 1) * LANES)
        mean_columns[rows] = column(mean[rows].reshape(1, LANES))
        scale_columns[rows] = column(scale[rows].reshape(1, LANES))
    for half in range(HALVES):
        for start in range(0, ROWS, CHUNK):
            rows = slice(start, start + CHUNK)
            sig = jax.nn.sigmoid(held_gate[rows, lanes(half)].astype(WIDE))
            narrow = (held_value[rows, lanes(half)].astype(WIDE) * sig).astype(NARROW)
            gated[rows, lanes(half)] = narrow
            padded[half, EDGE + start : EDGE + start + CHUNK] = narrow.astype(WIDE)
        for start in range(EDGE, ROWS, EDGE):
            rows = slice(start, start + EDGE)
            conv = convolve(padded, half, taps_wide, start, EDGE)
            normed[half, rows] = (conv - mean_columns[rows]) * scale_columns[rows]
    copies[6].wait()
    copies[7].wait()
    upstream[...] = lax.dot_general(
        held[...], held_weight[...], (((1,), (1,)), ((), ())), preferred_element_type=WIDE
    )
    first_upstream[...] = upstream[0:EDGE]
    first_cotangent[...] = held[0:EDGE]
    for half in range(HALVES):
        gain_row = gain[0:1, lanes(half)]
        gain_sum = jnp.zeros((8, LANES), WIDE)
        for start in range(EDGE, ROWS, EDGE):
            rows = slice(start, start + EDGE)
            narrow, own_scaled, own_spread, first, second, part = norm_backward(
                normed[half, rows], scale_columns[rows], gain_row, upstream[rows, lanes(half)]
            )
            hidden[rows, lanes(half)] = narrow.astype(WIDE)
            scaled[half, start - EDGE : start] = own_scaled
            spread[half, start - EDGE : start] = own_spread
            gain_sum = gain_sum + part
            if half == 0:
                sum_first[rows] = first
                sum_second[rows] = second
            else:
                sum_first[rows] = sum_first[rows] + first
                sum_second[rows] = sum_second[rows] + second
        gain_part[half] = gain_sum
    found = [
        column_sums(source[block * LANES : (block + 1) * LANES])
        for source in (sum_first, sum_second)
        for block in range(ROWS // LANES)
    ]
    sums[...] = jnp.concatenate([*found, jnp.zeros((2, LANES), WIDE)], 0)
    turned = jnp.transpose(hidden[...]).astype(NARROW)
    for near in range(CLOSE):
        product[near] = jnp.dot(
            turned, both_blocks(held, place, near), preferred_element_type=WIDE
        )


def head(
    halo, gated, upstream, taps, gain, mean, scale, sums, gain_part,
    scaled, spread, hidden, message, gain_total,
    padded, taps_wide, turned,
):
    taps_wide[0:TAPS] = taps[...].astype(WIDE)
    rows = slice(0, EDGE)
    mean_columns = column(mean[0:LANES].reshape(1, LANES))[rows]
    scale_columns = column(scale[0:LANES].reshape(1, LANES))[rows]
    turned[...] = jnp.zeros((2, LANES, LANES), WIDE)
    for half in range(HALVES):
        padded[half, rows] = halo[:, lanes(half)].astype(WIDE)
        padded[half, EDGE:] = gated[rows, lanes(half)].astype(WIDE)
    for half in range(HALVES):
        conv = convolve(padded, half, taps_wide, 0, EDGE)
        normed = (conv - mean_columns) * scale_columns
        narrow, own_scaled, own_spread, first, second, part = norm_backward(
            normed, scale_columns, gain[0:1, lanes(half)], upstream[rows, lanes(half)]
        )
        hidden[:, lanes(half)] = narrow
        scaled[half] = own_scaled
        spread[half] = own_spread
        gain_total[half] = gain_part[half] + part
        turned[0, rows] = turned[0, rows] + first
        turned[1, rows] = turned[1, rows] + second
    blocks = ROWS // LANES
    total = sums[...]
    extra = [column_sums(turned[0]), column_sums(turned[1])]
    none = jnp.zeros((blocks - 1, LANES), WIDE)
    last = jnp.zeros((2, LANES), WIDE)
    total = total + jnp.concatenate([extra[0], none, extra[1], none, last], 0)
    for peer in range(TP):
        message[peer] = total


def head_product(cotangent, hidden, place, near, side):
    columns = both_blocks(cotangent, place, near)[:, side * BLOCK : (side + 1) * BLOCK]
    return lax.dot_general(
        hidden[...], columns, (((0,), (0,)), ((), ())), preferred_element_type=WIDE
    )


def backward(
    place, sums, scaled, spread, first_scaled, first_spread, halo, gated, scale, gain_part,
    first_cotangent, first_hidden, product,
    other, small, extended,
    padded,
):
    for half in range(HALVES):
        padded[half, 0:EDGE] = halo[:, lanes(half)].astype(WIDE)
        padded[half, EDGE:] = gated[:, lanes(half)].astype(WIDE)
    total = (sums[0] + sums[1]) + (sums[2] + sums[3])
    total = total * (1.0 / (TP * WIDTH))
    blocks = ROWS // LANES
    for half in range(HALVES):
        extended[half, 0:EDGE] = jnp.zeros((EDGE, LANES), WIDE)
        extended[half, EDGE + ROWS :] = jnp.zeros((EDGE, LANES), WIDE)
    for block in range(blocks):
        rows = slice(block * LANES, (block + 1) * LANES)
        first = column(total[block : block + 1] * scale[rows].reshape(1, LANES))
        second = column(total[blocks + block : blocks + block + 1])
        for half in range(HALVES):
            cut = 0
            if block == 0:
                cut = EDGE
                d_conv = first_scaled[half] - first[0:cut] - first_spread[half] * second[0:cut]
                extended[half, EDGE : EDGE + cut] = d_conv
            rows = slice(block * LANES + cut - EDGE, (block + 1) * LANES - EDGE)
            d_conv = scaled[half, rows] - first[cut:] - spread[half, rows] * second[cut:]
            extended[half, EDGE + block * LANES + cut : EDGE + (block + 1) * LANES] = d_conv
    lead = EDGE - TAPS + 1
    groups = ROWS // 8
    for offset in range(8):
        steps = [q for q in range(5) if 0 <= 8 * q + offset - lead < TAPS]
        found = {(half, q): jnp.zeros((8, LANES), WIDE) for half in range(HALVES) for q in steps}
        loaded = {}
        for m in range(groups + steps[-1]):
            for half in range(HALVES):
                if m < groups:
                    begin = EDGE + 8 * m
                    loaded[half, m] = extended[half, begin : begin + 8]
                moved = padded[half, 8 * m + offset : 8 * m + offset + 8]
                for q in steps:
                    if 0 <= m - q < groups:
                        found[half, q] = found[half, q] + loaded[half, m - q] * moved
        for half in range(HALVES):
            for q in steps:
                tap = 8 * q + offset - lead
                small[tap : tap + 1, lanes(half)] = jnp.sum(found[half, q], 0, keepdims=True)
        near = offset
        whole = product[near, :, BLOCK:] + head_product(
            first_cotangent, first_hidden, place, near, 1
        )
        other[near * WIDTH : (near + 1) * WIDTH] = whole.astype(NARROW)
    for half in range(HALVES):
        small[TAPS:SMALL, lanes(half)] = jnp.sum(gain_part[half], 0, keepdims=True)
    for half in range(HALVES):
        value = small[:, lanes(half)]
        top = value.astype(NARROW)
        begin = CLOSE * WIDTH + half * 2 * SMALL
        other[begin : begin + SMALL] = top
        other[begin + SMALL : begin + 2 * SMALL] = (value - top.astype(WIDE)).astype(NARROW)


def pack(mine, small, other, pieces):
    for half in range(HALVES):
        begin = CLOSE * WIDTH + half * 2 * SMALL
        top = other[begin : begin + SMALL].astype(WIDE)
        rest = other[begin + SMALL : begin + 2 * SMALL].astype(WIDE)
        both = (small[:, lanes(half)] + (top + rest)).astype(NARROW)
        for near in range(CLOSE):
            pieces[near, WIDTH + half * SMALL : WIDTH + (half + 1) * SMALL] = both
    for near in range(CLOSE):
        for start in range(0, WIDTH, 64):
            rows = slice(start, start + 64)
            there = other[near * WIDTH + start : near * WIDTH + start + 64].astype(WIDE)
            pieces[NEAR_ORDER.index(near), rows] = (mine[near, rows] + there).astype(NARROW)


def gated_gradient(
    place, extended, taps, value, gate, first_cotangent, first_hidden, product,
    value_grad, gate_grad, margin, last, mine,
    taps_wide,
):
    for near in range(CLOSE):
        mine[near] = product[near, :, 0:BLOCK] + head_product(
            first_cotangent, first_hidden, place, near, 0
        )
    taps_wide[0:TAPS] = taps[...].astype(WIDE)
    for half in range(HALVES):
        for start in range(0, EDGE + ROWS, EDGE):
            found = jnp.zeros((EDGE, LANES), WIDE)
            for tap in range(TAPS):
                begin = start + TAPS - 1 - tap
                found = found + taps_wide[tap : tap + 1, lanes(half)] * extended[half, begin : begin + EDGE]
            if start == 0:
                margin[half] = found
                continue
            rows = slice(start - EDGE, start)
            sig = jax.nn.sigmoid(gate[rows, lanes(half)].astype(WIDE))
            slope = value[rows, lanes(half)].astype(WIDE) * sig * (1.0 - sig)
            if start == ROWS:
                last[0, half], last[1, half], last[2, half] = found, sig, slope
            else:
                value_grad[rows, lanes(half)] = (found * sig).astype(NARROW)
                gate_grad[rows, lanes(half)] = (found * slope).astype(NARROW)


def fold_near(arrived, payload):
    for start in range(0, WIDTH + 2 * SMALL, 64):
        rows = slice(start, start + 64)
        total = arrived[0, rows].astype(WIDE)
        for near in range(1, CLOSE):
            total = total + arrived[near, rows].astype(WIDE)
        payload[rows] = total.astype(NARROW)


def hand_out(payload, message):
    weights = jnp.transpose(payload[0:WIDTH].astype(WIDE)).astype(NARROW)
    small = jnp.concatenate([payload[WIDTH : WIDTH + SMALL], payload[WIDTH + SMALL :]], 1)
    for position, member in enumerate(GATHER_ORDER):
        message[position, 0:OWN] = weights[member * OWN : (member + 1) * OWN]
        message[position, OWN:] = small


def totals(arrived, total):
    for start in range(0, OWN + SMALL, 8):
        rows = slice(start, start + 8)
        found = arrived[0, rows].astype(WIDE)
        for position in range(1, 2 * CLOSE):
            found = found + arrived[position, rows].astype(WIDE)
        total[rows] = found


def finish(
    total, value_part, gate_part, last, late,
    value_grad, gate_grad, weight_grad, taps_grad, gain_grad,
    value_end, gate_end, taps_held, gain_held, departures,
):
    main, end = pl.ds(0, ROWS - EDGE), pl.ds(ROWS - EDGE, EDGE)
    taps_held[...] = total[OWN : OWN + TAPS]
    gain_held[...] = total[OWN + TAPS :]
    for half in range(HALVES):
        grad = last[0, half] + late[half]
        value_end[:, lanes(half)] = (grad * last[1, half]).astype(NARROW)
        gate_end[:, lanes(half)] = (grad * last[2, half]).astype(NARROW)
    copies = [
        pltpu.make_async_copy(value_part, value_grad.at[main], departures.at[0]),
        pltpu.make_async_copy(gate_part, gate_grad.at[main], departures.at[1]),
        pltpu.make_async_copy(total.at[pl.ds(0, OWN)], weight_grad, departures.at[2]),
        pltpu.make_async_copy(taps_held, taps_grad, departures.at[3]),
        pltpu.make_async_copy(gain_held, gain_grad, departures.at[4]),
        pltpu.make_async_copy(value_end, value_grad.at[end], departures.at[5]),
        pltpu.make_async_copy(gate_end, gate_grad.at[end], departures.at[6]),
    ]
    for copy in copies:
        copy.start()
    for copy in copies:
        copy.wait()


def to_block(value):
    pairs = []
    for far in range(FAR):
        for near in range(CLOSE):
            for core in range(2):
                target = (far + OFFSETS[core][near]) % FAR
                pairs.append(((far * CLOSE + near) * 2 + core, (target * CLOSE + near) * 2 + core))
    return lax.ppermute(value, SP, pairs)


def shards(
    proj_value, proj_gate, out_cotangent, out_weight, conv_taps, norm_gain, row_mean, row_scale
):
    end_gate = jax.nn.sigmoid(proj_gate[ROWS - EDGE :].astype(WIDE))
    end = (proj_value[ROWS - EDGE :].astype(WIDE) * end_gate).astype(NARROW)
    halo = shifted(end, SP, 1)
    split = (HALVES, ROWS, LANES)
    rest = (HALVES, ROWS - EDGE, LANES)
    row_gain = norm_gain.reshape(1, WIDTH)
    sides = pltpu.VMEM((HALVES, EDGE + ROWS, LANES), WIDE)
    taps_scratch = pltpu.VMEM((TAPS + 1, WIDTH), WIDE)
    place = lax.axis_index(SP).reshape(1)
    narrow = ((ROWS, WIDTH), NARROW)
    gated, scaled, spread, sums, gain_part, first_upstream, first_cotangent, product = (
        scalar_call(
            forward,
            [
                narrow, (rest, WIDE), (rest, WIDE), ((8, LANES), WIDE),
                ((HALVES, 8, LANES), WIDE), ((EDGE, WIDTH), WIDE), ((EDGE, MODEL), NARROW),
                ((CLOSE, WIDTH, 2 * BLOCK), WIDE),
            ],
            place, proj_value, proj_gate, out_cotangent, out_weight,
            conv_taps, row_gain, row_mean, row_scale, in_hbm=8,
            scratch=[
                pltpu.VMEM(*narrow), pltpu.VMEM(*narrow), pltpu.VMEM((ROWS, MODEL), NARROW),
                pltpu.VMEM((WIDTH, MODEL), NARROW), pltpu.VMEM((TAPS, WIDTH), NARROW),
                pltpu.VMEM((1, WIDTH), WIDE), pltpu.VMEM((ROWS,), WIDE),
                pltpu.VMEM((ROWS,), WIDE), pltpu.SemaphoreType.DMA((8,)),
                sides, taps_scratch, *([pltpu.VMEM((ROWS, LANES), WIDE)] * 4),
                pltpu.VMEM((ROWS, WIDTH), WIDE), pltpu.VMEM(split, WIDE),
                pltpu.VMEM((ROWS, WIDTH), WIDE),
            ],
            flops=4 * ROWS * WIDTH * MODEL, limit=12,
        )
    )
    edge = (HALVES, EDGE, LANES)
    first_scaled, first_spread, first_hidden, message, gain_part = call_with(
        head,
        [
            (edge, WIDE), (edge, WIDE), ((EDGE, WIDTH), NARROW),
            ((TP, 8, LANES), WIDE), ((HALVES, 8, LANES), WIDE),
        ],
        [
            pltpu.VMEM((HALVES, 2 * EDGE, LANES), WIDE),
            taps_scratch,
            pltpu.VMEM((2, LANES, LANES), WIDE),
        ],
        halo, gated, first_upstream, conv_taps, row_gain, row_mean, row_scale, sums,
        gain_part, flops=10 * ROWS * WIDTH,
    )
    sums = exchange(message, "tp", SUMS_ORDER)
    rows = CLOSE * WIDTH + 4 * SMALL
    other, small, extended = scalar_call(
        backward,
        [
            ((rows, BLOCK), NARROW), ((SMALL, WIDTH), WIDE),
            ((HALVES, ROWS + 2 * EDGE, LANES), WIDE),
        ],
        place, sums, scaled, spread, first_scaled, first_spread, halo, gated, row_scale, gain_part,
        first_cotangent, first_hidden, product, scratch=[sides], flops=100 * ROWS * WIDTH,
    )
    other = lax.ppermute(other, "c", [(0, 1), (1, 0)])
    main = ((ROWS - EDGE, WIDTH), NARROW)
    value_part, gate_part, margin, last, mine = scalar_call(
        gated_gradient,
        [main, main, (edge, WIDE), ((3, *edge), WIDE), ((CLOSE, WIDTH, BLOCK), WIDE)],
        place, extended, conv_taps, proj_value, proj_gate, first_cotangent, first_hidden,
        product, scratch=[taps_scratch], flops=100 * ROWS * WIDTH,
    )
    (pieces,) = call(
        pack, [((CLOSE, WIDTH + 2 * SMALL, BLOCK), NARROW)], mine, small, other, flops=1 << 20
    )
    arrived = exchange(pieces, NEAR, NEAR_ORDER)
    (payload,) = call(
        fold_near, [((WIDTH + 2 * SMALL, BLOCK), NARROW)], arrived, flops=1 << 20
    )
    payload = to_block(payload)
    late = shifted(margin, SP, -1)
    (message,) = call(hand_out, [((2 * CLOSE, OWN + SMALL, WIDTH), NARROW)], payload, flops=1 << 16)
    arrived = exchange(message, (*NEAR, "c"), GATHER_ORDER)
    (total,) = call(totals, [((OWN + SMALL, WIDTH), WIDE)], arrived, flops=1 << 20)
    value_grad, gate_grad, weight_grad, taps_grad, gain_grad = last_call(
        [narrow, narrow, ((OWN, WIDTH), WIDE), ((TAPS, WIDTH), WIDE), ((1, WIDTH), WIDE)],
        total, value_part, gate_part, last, late,
    )
    return (value_grad, gate_grad, weight_grad, taps_grad, gain_grad.reshape(WIDTH))


def call_with(body, outs, scratch, *args, flops=0, limit=6):
    shapes = [jax.ShapeDtypeStruct(shape, dtype) for shape, dtype in outs]
    size = sum(a.size * a.dtype.itemsize for a in (*args, *shapes))
    return pl.pallas_call(
        body,
        out_shape=shapes,
        scratch_shapes=scratch,
        compiler_params=pltpu.CompilerParams(vmem_limit_bytes=limit << 20),
        cost_estimate=pl.CostEstimate(flops=flops, bytes_accessed=size, transcendentals=0),
    )(*args)


def scalar_call(
    body, outs, scalar, *args, scratch=(), flops=1 << 20, limit=6, in_hbm=0
):
    shapes = [jax.ShapeDtypeStruct(shape, dtype) for shape, dtype in outs]
    size = sum(a.size * a.dtype.itemsize for a in (*args, *shapes))
    whole = pl.BlockSpec(memory_space=pltpu.VMEM)
    far = [pltpu.with_memory_space_constraint(a, pltpu.HBM) for a in args[:in_hbm]]
    return pl.pallas_call(
        body,
        out_shape=shapes,
        in_specs=[
            pl.BlockSpec(memory_space=pltpu.SMEM),
            *([pl.BlockSpec(memory_space=pltpu.HBM)] * in_hbm),
            *([whole] * (len(args) - in_hbm)),
        ],
        out_specs=[whole] * len(shapes),
        scratch_shapes=scratch,
        compiler_params=pltpu.CompilerParams(vmem_limit_bytes=limit << 20),
        cost_estimate=pl.CostEstimate(flops=flops, bytes_accessed=size, transcendentals=0),
    )(scalar, *far, *args[in_hbm:])


def last_call(outs, *args):
    edge = pltpu.VMEM((EDGE, WIDTH), NARROW)
    return pl.pallas_call(
        finish,
        out_shape=[pltpu.HBM(*out) for out in outs],
        in_specs=[pl.BlockSpec(memory_space=pltpu.VMEM)] * len(args),
        out_specs=[pl.BlockSpec(memory_space=pltpu.HBM)] * len(outs),
        scratch_shapes=[
            edge, edge, pltpu.VMEM(*outs[3]), pltpu.VMEM(*outs[4]), pltpu.SemaphoreType.DMA((7,)),
        ],
        compiler_params=pltpu.CompilerParams(vmem_limit_bytes=6 << 20),
        cost_estimate=pl.CostEstimate(flops=1 << 16, bytes_accessed=1 << 19, transcendentals=0),
        name="finish",
    )(*args)


def solution(mesh):
    sizes = [size for _, size in AXES]
    split = Mesh(mesh.devices.reshape(*sizes, mesh.shape["tp"]), (*SP, "tp"))
    placed = (
        P(SP, "tp"),
        P(SP, "tp"),
        P(SP, None),
        P("tp", None),
        P(None, "tp"),
        P("tp"),
        P(SP),
        P(SP),
    )
    return jax.shard_map(
        shards,
        mesh=split,
        in_specs=placed,
        out_specs=(P(SP, "tp"), P(SP, "tp"), P(SP, "tp"), P(None, "tp"), P("tp")),
        check_vma=False,
    )
```
